512 devices in a mesh: sp: 128 (over z, y, core), tp: 4 (over x).
Axes of the slice: x: 4, y: 8, z: 8, core: 2. Of those that a mesh axis runs over, the one named last changes fastest.
Arguments:
- features: bfloat16 [16384, 2048], P('sp', 'tp'), may hold values from -16 to 16
- norm_gain: float32 [2048], replicated, may hold values from 0.1 to 1.9
- att_query: bfloat16 [2048, 1024], P('sp', 'tp'), may hold values from -1 to 1
- att_key: bfloat16 [2048, 512], P('sp', 'tp'), may hold values from -1 to 1
- att_value: bfloat16 [2048, 512], P('sp', 'tp'), may hold values from -0.125 to 0.125
- att_lambda: float32 [8], P('tp'), may hold values from 0.3 to 0.8
- att_gain: float32 [128], replicated, may hold values from 0.1 to 1.9
- ret_query: bfloat16 [2048, 512], P('sp', 'tp'), may hold values from -0.125 to 0.125
- ret_key: bfloat16 [2048, 512], P('sp', 'tp'), may hold values from -0.125 to 0.125
- ret_value: bfloat16 [2048, 1024], P('sp', 'tp'), may hold values from -0.125 to 0.125
- ret_gain: float32 [128], replicated, may hold values from 0.1 to 1.9
- out_weight: bfloat16 [2, 1024, 2048], P(None, 'tp'), may hold values from -0.125 to 0.125
Outputs:
- mixed: float32 [16384, 2048], P(('sp', 'tp'))
The draws below stay inside these ranges and needn't reach their ends.
All inputs are finite; a program needn't handle non-finite values.
Results may differ from the reference program's by a relative error of at most 0.0092.
Values may be sent and summed in bfloat16 or wider, within the bound.
No kernel may reach another device: no remote copies, remote signals or barrier semaphores. Data moves between devices by JAX's collectives and lax.ppermute only.
A program may use at most 64 MiB of HBM per device.

```python
import math
import jax
import jax.numpy as jnp
from jax import lax

D = 2048
HEADS = 8
KV_HEADS = 4
DH = 64
DV = 128
SEG = 64
TOKENS = 16384


def draw_features(key, part):
    base_key = jax.random.fold_in(key, 3)
    noise_seed = jax.random.fold_in(base_key, 0)
    noise = jax.random.normal(noise_seed, (TOKENS, D), jnp.float32)
    return jnp.clip(noise, -6.0, 6.0).astype(jnp.bfloat16)


def query_key_pair(key):
    base_key = jax.random.fold_in(key, 7)
    query_seed, other_seed = jax.random.split(base_key)
    query_matrix = jnp.clip(jax.random.normal(query_seed, (D, HEADS * 2 * DH), jnp.float32), -6.0, 6.0) * (2.0 / D) ** 0.5
    key_matrix = jnp.clip(jax.random.normal(other_seed, (D, KV_HEADS * 2 * DH), jnp.float32), -6.0, 6.0) * (2.0 / D) ** 0.5
    return (jnp.clip(query_matrix, -1.0, 1.0), jnp.clip(key_matrix, -1.0, 1.0))


def draw_att_query(key, part):
    return query_key_pair(key)[0].astype(jnp.bfloat16)


def draw_att_key(key, part):
    return query_key_pair(key)[1].astype(jnp.bfloat16)


def steps_of(key, shape, shards, smallest, high):
    level, own = 1.0, jax.random.fold_in(key, 6)
    for dim, blocks in shards:
        heights = jnp.exp(jax.random.uniform(jax.random.fold_in(own, dim), (blocks,), jnp.float32, smallest / len(shards), high / len(shards)))
        level = level * jnp.repeat(heights, shape[dim] // blocks).reshape([-1 if axis == dim else 1 for axis in range(len(shape))])
    return level


def centred(own_key, shape, spread, bound, cuts=(), kind=jnp.bfloat16):
    values = spread * jax.random.normal(own_key, shape, jnp.float32)
    if cuts:
        values = values * steps_of(own_key, shape, cuts, -0.22, 0.18)
    return jnp.clip(values, -bound, bound).astype(kind)


def setup_inputs(seed: int = 0) -> dict:
    key_list = jax.random.split(jax.random.key(seed), 13)
    return {
        "features": draw_features(jax.random.fold_in(key_list[12], 71), 0),
        "norm_gain": jnp.clip(1.0 + 0.18 * jax.random.normal(key_list[1], (D,), jnp.float32), 0.1, 1.9),
        "att_query": draw_att_query(jax.random.fold_in(key_list[12], 71), 0),
        "att_key": draw_att_key(jax.random.fold_in(key_list[12], 71), 0),
        "att_value": centred(key_list[4], (D, KV_HEADS * DV), D ** -0.5, 0.125, ((0, 128), (1, 4))),
        "att_lambda": jnp.clip(0.3 + 0.5 * jax.random.uniform(key_list[5], (HEADS,), jnp.float32) ** steps_of(key_list[5], (HEADS,), ((0, 4),), -0.2, 0.2), 0.3, 0.8),
        "att_gain": jnp.clip(1.0 + 0.18 * jax.random.normal(key_list[6], (DV,), jnp.float32), 0.1, 1.9),
        "ret_query": centred(key_list[7], (D, HEADS * DH), D ** -0.5, 0.125, ((0, 128), (1, 4))),
        "ret_key": centred(key_list[8], (D, HEADS * DH), D ** -0.5, 0.125, ((0, 128), (1, 4))),
        "ret_value": centred(key_list[9], (D, HEADS * DV), D ** -0.5, 0.125, ((0, 128), (1, 4))),
        "ret_gain": jnp.clip(1.0 + 0.18 * jax.random.normal(key_list[10], (DV,), jnp.float32), 0.1, 1.9),
        "out_weight": centred(key_list[11], (2, HEADS * DV, D), (2 * HEADS * DV) ** -0.5, 0.125, ((1, 4),)),
    }


EPSILON = 1e-06

def head_norm(vectors, gain):
    mean_sq = lax.optimization_barrier(jnp.mean(vectors * vectors, axis=-1, keepdims=True))
    return vectors * lax.rsqrt(mean_sq + EPSILON) * gain.astype(jnp.float32)

def rotate(vectors, positions):
    head_width = vectors.shape[-1]
    inverse = 10000.0 ** (-jnp.arange(0, head_width, 2).astype(jnp.float32) / head_width)
    angles = positions[:, None, None] * inverse[None, None, :]
    cosine = jnp.cos(angles)
    sine_part = jnp.sin(angles)
    first_half = vectors[..., :head_width // 2]
    second_half = vectors[..., head_width // 2:]
    return jnp.concatenate([first_half * cosine - second_half * sine_part, first_half * sine_part + second_half * cosine], axis=-1)

def decay_logs(head_index, length):
    pair_index = (head_index // 2).astype(jnp.float32)
    quick_logs = jnp.log1p(-jnp.exp2(-5.0 - pair_index / 4.0))
    slow_logs = jnp.log1p(-1.0 / (length * (1.0 + pair_index)))
    return jnp.where(head_index % 2 == 0, quick_logs, slow_logs)

def differential(query_att, keys_att, values_att, att_lambda):
    tokens = query_att.shape[0]
    group_size = HEADS // KV_HEADS
    query = query_att.reshape(tokens, KV_HEADS, group_size, 2, DH)
    key_rows = keys_att.reshape(tokens, KV_HEADS, 2, DH).astype(jnp.float32)
    values = values_att.reshape(tokens, KV_HEADS, DV).astype(jnp.float32)
    key_segment = jnp.arange(tokens) // SEG
    query_span = math.gcd(tokens, 128)
    blocks = tokens // query_span

    def one_block(block_index):
        query_block = lax.dynamic_slice_in_dim(query, block_index * query_span, query_span, 0).astype(jnp.float32)
        scores = jnp.einsum('qagmd,kamd->agmqk', query_block, key_rows) * DH ** (-0.5)
        query_segment = (block_index * query_span + jnp.arange(query_span)) // SEG
        allowed = key_segment[None, :] <= query_segment[:, None]
        scores = jnp.where(allowed, scores, -jnp.inf)
        running = lax.optimization_barrier(jnp.max(scores, axis=-1, keepdims=True))
        weights = jnp.exp(scores - running)
        summed = lax.optimization_barrier(jnp.sum(weights, axis=-1))
        rounded = lax.optimization_barrier(weights.astype(jnp.bfloat16)).astype(jnp.float32)
        weighted = jnp.einsum('agmqk,kae->agmqe', rounded, values)
        return weighted / summed[..., None]
    blocks_out = lax.map(one_block, jnp.arange(blocks))
    mixing = att_lambda.astype(jnp.float32).reshape(KV_HEADS, group_size)
    att_heads = blocks_out[:, :, :, 0] - mixing[None, :, :, None, None] * blocks_out[:, :, :, 1]
    return jnp.transpose(att_heads, (0, 3, 1, 2, 4)).reshape(tokens, HEADS, DV)

def retention(query_ret, keys_ret, values_ret):
    tokens = query_ret.shape[0]
    highest = lax.Precision.HIGHEST
    positions = jnp.arange(tokens).astype(jnp.float32)
    query = rotate(query_ret.reshape(tokens, HEADS, DH).astype(jnp.float32), positions)
    key_rows = rotate(keys_ret.reshape(tokens, HEADS, DH).astype(jnp.float32), positions) * DH ** (-0.5)
    values = values_ret.reshape(tokens, HEADS, DV).astype(jnp.float32)
    log_decay = decay_logs(jnp.arange(HEADS), float(tokens))
    offsets = jnp.arange(SEG).astype(jnp.float32)
    distance = offsets[:, None] - offsets[None, :]
    inside = jnp.exp(log_decay[:, None, None] * jnp.maximum(distance, 0.0)[None]) * (distance >= 0).astype(jnp.float32)[None]
    query_decay = jnp.exp(log_decay[None, :] * (offsets[:, None] + 1.0))
    key_decay = jnp.exp(log_decay[None, :] * (SEG - 1.0 - offsets[:, None]))
    state_decay = jnp.exp(log_decay * SEG)

    def advance(memory, block_inputs):
        query_block, key_block, value_block = block_inputs
        scores = jnp.einsum('ihd,jhd->hij', query_block, key_block, precision=highest) * inside
        within = jnp.einsum('hij,jhe->ihe', scores, value_block, precision=highest)
        carried_term = jnp.einsum('ihd,hde->ihe', query_block, memory, precision=highest) * query_decay[:, :, None]
        memory = memory * state_decay[:, None, None] + jnp.einsum('jhd,jhe->hde', key_block * key_decay[:, :, None], value_block, precision=highest)
        return (memory, within + carried_term)
    blocks = tokens // SEG

    def to_blocks(array):
        return array.reshape(blocks, SEG, HEADS, array.shape[-1])
    _, blocks_out = lax.scan(advance, jnp.zeros((HEADS, DH, DV), jnp.float32), (to_blocks(query), to_blocks(key_rows), to_blocks(values)))
    return blocks_out.reshape(tokens, HEADS, DV)

def reference(features, norm_gain, att_query, att_key, att_value, att_lambda, att_gain, ret_query, ret_key, ret_value, ret_gain, out_weight):
    tokens = features.shape[0]
    floats = features.astype(jnp.float32)
    mean_sq = lax.optimization_barrier(jnp.mean(floats * floats, axis=-1, keepdims=True))
    normed = (floats * lax.rsqrt(mean_sq + EPSILON) * norm_gain.astype(jnp.float32)).astype(jnp.bfloat16)

    def project(matrix):
        return jnp.dot(normed, matrix, preferred_element_type=jnp.float32).astype(jnp.bfloat16)
    att_heads = differential(project(att_query), project(att_key), project(att_value), att_lambda)
    att_out = head_norm(att_heads, att_gain).astype(jnp.bfloat16).reshape(tokens, HEADS * DV)
    ret_heads = retention(project(ret_query), project(ret_key), project(ret_value))
    ret_out = head_norm(ret_heads, ret_gain).astype(jnp.bfloat16).reshape(tokens, HEADS * DV)
    summed = jnp.dot(att_out, out_weight[0], preferred_element_type=jnp.float32)
    summed = summed + jnp.dot(ret_out, out_weight[1], preferred_element_type=jnp.float32)
    return summed
```

```python
import functools

import jax
import jax.numpy as jnp
from jax import lax
from jax.experimental import pallas as pl
from jax.experimental.pallas import tpu as pltpu
from jax.sharding import Mesh
from jax.sharding import PartitionSpec as P

DH = 64
DV = 128
SEG = 64
Z = ("zh", "zl")
SP = ("zh", "zl", "y", "c")
SP_TP = ("zh", "zl", "y", "c", "tp")
EPSILON = 1e-06
NEG = -1e30
LOG2E = 1.4426950408889634
KEYS = 512
INTERPRET = False


def to_all(value, axes):
    count = lax.axis_size(axes)
    return lax.all_to_all(
        jnp.broadcast_to(value[None], (count, *value.shape)), axes, 0, 0, tiled=True
    )


def shifted(value, step):
    count = lax.axis_size(Z)
    return lax.ppermute(value, Z, [(i, (i + step) % count) for i in range(count)])


def swapped(value):
    return lax.ppermute(value, "c", [(0, 1), (1, 0)])


def two_steps(own, half):
    before = shifted(own, 1)
    after = shifted(own, -1)
    low = shifted(before[:half], 1)
    high = shifted(after[half:], -1)
    return before, after, low, high


def attend_block(mine_ref, other_ref, qm_ref, qo_ref, m_ref, l_ref, o_ref, start, q0, masked):
    mine = mine_ref[0]
    other = other_ref[0]
    nt = (((1,), (1,)), ((), ()))
    s0 = lax.dot_general(mine, qm_ref[...], nt, preferred_element_type=jnp.float32)
    s1 = lax.dot_general(other, qo_ref[...], nt, preferred_element_type=jnp.float32)
    vt = jnp.concatenate([mine.T[DH:], other.T[DH:]], axis=0)
    tokens = s0.shape[1]
    for k, s in enumerate((s0, s1)):
        at = slice(k * tokens, (k + 1) * tokens)
        s = s * LOG2E
        if masked:
            rows = lax.broadcasted_iota(jnp.int32, s.shape, 0) + start
            cols = lax.broadcasted_iota(jnp.int32, s.shape, 1) + q0
            allowed = (rows // SEG) <= (cols // SEG)
            s = jnp.where(allowed, s, NEG)
        old = m_ref[:, at]
        top = jnp.maximum(old, jnp.max(s, axis=0, keepdims=True))
        w = jnp.exp2(s - top)
        if masked:
            w = jnp.where(allowed, w, 0.0)
        factor = jnp.exp2(old - top)
        m_ref[:, at] = top
        l_ref[:, at] = l_ref[:, at] * factor + jnp.sum(w, axis=0, keepdims=True)
        o_ref[:, at] = o_ref[:, at] * factor + jnp.dot(
            vt, w.astype(jnp.bfloat16), preferred_element_type=jnp.float32
        )


def attend_kernel(first, per_z, where_ref, mine_ref, other_ref, qm_ref, qo_ref, *refs):
    m_ref, l_ref, o_ref = refs[-3:]
    g = pl.program_id(0)
    start = where_ref[1 + g // per_z] + (g % per_z) * KEYS
    q0 = where_ref[0]

    @pl.when(g == 0)
    def _():
        if first:
            m_ref[...] = jnp.full(m_ref.shape, NEG, jnp.float32)
            l_ref[...] = jnp.zeros(l_ref.shape, jnp.float32)
            o_ref[...] = jnp.zeros(o_ref.shape, jnp.float32)
        else:
            m_ref[...] = refs[0][...]
            l_ref[...] = refs[1][...]
            o_ref[...] = refs[2][...]

    block = functools.partial(
        attend_block, mine_ref, other_ref, qm_ref, qo_ref, m_ref, l_ref, o_ref, start, q0
    )

    @pl.when(start + KEYS <= q0)
    def _():
        block(False)

    @pl.when((start + KEYS > q0) & (start <= q0))
    def _():
        block(True)


def attend(state, where, mine, other, qm, qo):
    blocks, span, _ = mine.shape
    tokens = qm.shape[0]
    per_z = span // KEYS
    first = state is None
    kv_spec = pl.BlockSpec((1, KEYS, 2 * DH), lambda g, w: (g // per_z, g % per_z, 0))

    def whole(shape):
        return pl.BlockSpec(shape, lambda g, w: (0, 0))

    shapes = [(1, 2 * tokens), (1, 2 * tokens), (DV, 2 * tokens)]
    q_shape = (tokens, 2 * DH)
    return pl.pallas_call(
        functools.partial(attend_kernel, first, per_z),
        grid_spec=pltpu.PrefetchScalarGridSpec(
            num_scalar_prefetch=1,
            grid=(blocks * per_z,),
            in_specs=[kv_spec, kv_spec, whole(q_shape), whole(q_shape)]
            + ([] if first else [whole(s) for s in shapes]),
            out_specs=[whole(s) for s in shapes],
        ),
        out_shape=[jax.ShapeDtypeStruct(s, jnp.float32) for s in shapes],
        compiler_params=pltpu.CompilerParams(dimension_semantics=("arbitrary",)),
        cost_estimate=pl.CostEstimate(
            flops=blocks * span * tokens * 4 * 256,
            bytes_accessed=blocks * span * 512,
            transcendentals=blocks * span * tokens * 2,
        ),
        name="attend",
        interpret=INTERPRET,
    )(where, mine, other, qm, qo, *(() if first else state))


def rotate(vectors, cosine, sine):
    half = vectors.shape[-1] // 2
    a = vectors[..., :half]
    b = vectors[..., half:]
    return jnp.concatenate([a * cosine - b * sine, a * sine + b * cosine], axis=-1)


def decay_log(head, length):
    pair = (head // 2).astype(jnp.float32)
    quick = jnp.log1p(-jnp.exp2(-5.0 - pair / 4.0))
    slow = jnp.log1p(-1.0 / (length * (1.0 + pair)))
    return jnp.where(head % 2 == 0, quick, slow)


def shards(
    features,
    norm_gain,
    att_query,
    att_key,
    att_value,
    att_lambda,
    att_gain,
    ret_query,
    ret_key,
    ret_value,
    ret_gain,
    out_weight,
):
    zh, zl, y, c = (lax.axis_index(a) for a in SP)
    ny = lax.axis_size("y")
    nz = lax.axis_size(Z)
    nl = lax.axis_size("zl")
    z = zh * nl + zl
    chip = z * ny + y
    residues = [(zl + k) % nl for k in (0, nl - 1, 1, 2)]

    def half(array, h):
        width = array.shape[1] // 2
        return array[:, h * width : (h + 1) * width]

    matrices = (att_query, att_key, att_value, ret_query, ret_key, ret_value)
    halves = jnp.stack(
        [jnp.concatenate([half(a, h) for a in matrices], axis=1) for h in range(2)]
    )
    rows, width = halves.shape[1:]
    sent = jnp.broadcast_to(halves[None], (2 * ny, 2, rows, width)).reshape(4 * ny, rows, width)
    w_own = lax.all_to_all(sent, ("zh", "y", "c"), 0, 0, tiled=True)
    w_own = w_own.reshape(4 * ny * rows, width)
    w_before, w_after, w_low, w_high = two_steps(w_own, 2 * ny * rows)

    gathered = to_all(features, "tp")
    tokens = features.shape[0]
    floats = gathered.astype(jnp.float32)
    mean_sq = jnp.sum(floats * floats, axis=(0, 2)) / norm_gain.shape[0]
    gain = norm_gain.reshape(gathered.shape[0], 1, -1)
    scaled = floats * lax.rsqrt(mean_sq + EPSILON)[None, :, None] * gain
    scaled = scaled.astype(jnp.bfloat16)
    per_tp = nz // gathered.shape[0]
    wide = scaled.shape[2] // per_tp
    by_z = jnp.stack([scaled[i // per_tp][:, (i % per_tp) * wide :][:, :wide] for i in range(nz)])
    both = to_all(by_z, "c")
    tokens = 2 * tokens

    def made_by(k, high, matrix):
        left = lax.dynamic_index_in_dim(both, high * nl + residues[k], 1, keepdims=False)
        left = left.reshape(tokens, wide)
        return jnp.dot(left, matrix, preferred_element_type=jnp.float32)

    made = made_by(0, 0, w_own[:wide]) + made_by(0, 1, w_own[wide:])
    made = made + made_by(1, 0, w_before[:wide]) + made_by(1, 1, w_before[wide:])
    made = made + made_by(2, 0, w_after[:wide]) + made_by(2, 1, w_after[wide:])
    made = made + made_by(3, 0, w_low) + made_by(3, 1, w_high)
    made = made.astype(jnp.bfloat16)
    q_att = made[:, :128]
    kv = made[:, 128:256]
    q_ret = made[:, 256:320].astype(jnp.float32)
    k_ret = made[:, 320:384].astype(jnp.float32)
    v_ret = made[:, 384:512].astype(jnp.float32)

    highest = lax.Precision.HIGHEST
    length = nz * ny * tokens
    log_decay = decay_log(lax.axis_index("tp") * 2 + c, float(length))
    offsets = jnp.arange(tokens).astype(jnp.float32)
    positions = (chip * tokens + jnp.arange(tokens)).astype(jnp.float32)
    inverse = 10000.0 ** (-jnp.arange(0, DH, 2).astype(jnp.float32) / DH)
    angles = positions[:, None] * inverse[None, :]
    cosine, sine = jnp.cos(angles), jnp.sin(angles)
    q_rot = rotate(q_ret, cosine, sine)
    k_rot = rotate(k_ret, cosine, sine) * DH ** (-0.5)
    key_weight = jnp.exp(log_decay * (tokens - 1.0 - offsets))
    own_state = jnp.einsum("jd,je->de", k_rot * key_weight[:, None], v_ret, precision=highest)

    payload = jnp.concatenate([kv, own_state.astype(jnp.bfloat16)], axis=0)
    spread = to_all(payload, ("zh", "y"))
    kv_own = spread[:, :tokens].reshape(2, ny * tokens, 2 * DH)
    kv_before, kv_after, kv_low, kv_high = two_steps(kv_own, 1)
    states = spread[:, tokens:].reshape(2, ny, DH, DV).astype(jnp.float32)

    ys = jnp.arange(ny)
    span = log_decay * tokens
    to_end = jnp.exp(span * (ny - 1 - ys).astype(jnp.float32))
    sums = jnp.sum(states * to_end[None, :, None, None], axis=1)
    others = to_all(sums.astype(jnp.bfloat16), "zl").astype(jnp.float32)
    in_z = lax.dynamic_index_in_dim(states, zh, 0, keepdims=False)
    y_weight = jnp.where(ys < y, jnp.exp(span * jnp.maximum(y - 1 - ys, 0).astype(jnp.float32)), 0.0)
    zs = jnp.arange(2)[None, :] * nl + jnp.arange(nl)[:, None]
    steps = jnp.maximum(ny * (z - 1 - zs) + y, 0).astype(jnp.float32)
    z_weight = jnp.where(zs < z, jnp.exp(span * steps), 0.0)
    carried = jnp.sum(in_z * y_weight[:, None, None], axis=0)
    carried = carried + jnp.sum(others * z_weight[:, :, None, None], axis=(0, 1))

    distance = offsets[:, None] - offsets[None, :]
    inside = jnp.where(distance >= 0, jnp.exp(log_decay * jnp.maximum(distance, 0.0)), 0.0)
    scores = jnp.einsum("id,jd->ij", q_rot, k_rot, precision=highest) * inside
    within = jnp.dot(scores, v_ret, precision=highest)
    query_weight = jnp.exp(log_decay * (offsets + 1.0))
    ret = within + jnp.dot(q_rot, carried, precision=highest) * query_weight[:, None]
    ret = ret * lax.rsqrt(jnp.mean(ret * ret, axis=-1, keepdims=True) + EPSILON) * ret_gain
    ret = ret.astype(jnp.bfloat16)

    scaled_q = q_att * jnp.bfloat16(DH ** (-0.5))
    q_mine = jnp.where(c == 0, scaled_q[:, :DH], scaled_q[:, DH:])
    q_other = jnp.where(c == 0, scaled_q[:, DH:], scaled_q[:, :DH])
    qm = jnp.pad(q_mine, ((0, 0), (0, DH)))
    qo = jnp.pad(q_other, ((0, 0), (0, DH)))
    q0 = chip * tokens

    def where(k, highs):
        return jnp.stack([q0] + [(h * nl + residues[k]) * ny * tokens for h in highs]).astype(jnp.int32)

    state = attend(None, where(0, (0, 1)), kv_own, swapped(kv_own), qm, qo)
    state = attend(state, where(1, (0, 1)), kv_before, swapped(kv_before), qm, qo)
    state = attend(state, where(2, (0, 1)), kv_after, swapped(kv_after), qm, qo)
    state = attend(state, where(3, (0,)), kv_low, swapped(kv_low), qm, qo)
    _, sums_l, weighted = attend(state, where(3, (1,)), kv_high, swapped(kv_high), qm, qo)
    maps = weighted / sums_l
    mixing = lax.dynamic_index_in_dim(att_lambda, c, 0, keepdims=False)
    att = jnp.where(c == 0, 1.0, -mixing) * maps[:, :tokens]
    att = att + jnp.where(c == 0, -mixing, 1.0) * maps[:, tokens:]
    att = att * lax.rsqrt(jnp.mean(att * att, axis=0, keepdims=True) + EPSILON)
    att = jnp.where(c == 0, att, jnp.concatenate([att[DH:], att[:DH]], axis=0))
    att = (att.T * att_gain).astype(jnp.bfloat16)

    heads = jnp.concatenate([att, ret], axis=1).reshape(2, tokens // 2, 2 * DV)
    heads = lax.all_to_all(heads, "c", 0, 0, tiled=True)
    joined = jnp.concatenate(
        [heads[0, :, :DV], heads[1, :, :DV], heads[0, :, DV:], heads[1, :, DV:]], axis=1
    )
    partial = jnp.dot(
        joined, out_weight.reshape(-1, out_weight.shape[2]), preferred_element_type=jnp.float32
    ).astype(jnp.bfloat16)
    groups = lax.axis_size("tp")
    partial = lax.all_to_all(
        partial.reshape(groups, -1, partial.shape[1]), "tp", 0, 0, tiled=True
    )
    return jnp.sum(partial.astype(jnp.float32), axis=0)


def solution(mesh):
    devices = mesh.devices
    torus = Mesh(devices.reshape(2, 4, -1, 2, devices.shape[-1]), SP_TP)
    return jax.shard_map(
        shards,
        mesh=torus,
        in_specs=(
            P(SP, "tp"),
            P(),
            P(SP, "tp"),
            P(SP, "tp"),
            P(SP, "tp"),
            P("tp"),
            P(),
            P(SP, "tp"),
            P(SP, "tp"),
            P(SP, "tp"),
            P(),
            P(None, "tp", None),
        ),
        out_specs=P(SP_TP, None),
        check_vma=False,
    )
```

```python
import functools

import jax
import jax.numpy as jnp
from jax import lax
from jax.experimental import pallas as pl
from jax.experimental.pallas import tpu as pltpu
from jax.sharding import Mesh
from jax.sharding import PartitionSpec as P

DH = 64
DV = 128
SEG = 64
Z = ("zh", "zl")
SP = ("zh", "zl", "y", "c")
SP_TP = ("zh", "zl", "y", "c", "tp")
EPSILON = 1e-06
NEG = -1e30
KEYS = 512
ROWS = 144
INTERPRET = False


def to_all(value, axes):
    count = lax.axis_size(axes)
    return lax.all_to_all(
        jnp.broadcast_to(value[None], (count, *value.shape)), axes, 0, 0, tiled=True
    )


def swapped(value):
    return lax.ppermute(value, "c", [(0, 1), (1, 0)])


def attend_kernel(where_ref, q_ref, k_ref, v_ref, out_ref, vt_ref, qt_ref, m_ref, l_ref, o_ref):
    step = pl.program_id(0)
    z = where_ref[0]
    y = where_ref[1]
    keys = k_ref.shape[0]
    tokens = q_ref.shape[1]

    @pl.when(step == 0)
    def _():
        vt_ref[...] = v_ref[...].T

    def visit(start, count, masked):
        s = jnp.dot(k_ref[pl.ds(start, count)], qt_ref[...], preferred_element_type=jnp.float32)
        if masked:
            rows = lax.broadcasted_iota(jnp.int32, s.shape, 0) + start
            cols = lax.broadcasted_iota(jnp.int32, s.shape, 1) % tokens + y * tokens
            allowed = (rows // SEG) <= (cols // SEG)
            s = jnp.where(allowed, s, NEG)
        old = m_ref[...]
        top = jnp.maximum(old, jnp.max(s, axis=0, keepdims=True))
        w = jnp.exp(s - top)
        factor = jnp.exp(old - top)
        m_ref[...] = top
        l_ref[...] = l_ref[...] * factor + jnp.sum(w, axis=0, keepdims=True)
        o_ref[...] = o_ref[...] * factor + jnp.dot(
            vt_ref[:, pl.ds(start, count)],
            w.astype(jnp.bfloat16),
            preferred_element_type=jnp.float32,
        )

    @pl.when(step >= z)
    def _():
        q = q_ref[0]
        lane = lax.broadcasted_iota(jnp.int32, q.shape, 1)
        zero = jnp.zeros_like(q)
        q = jnp.concatenate([jnp.where(lane < DH, q, zero), jnp.where(lane < DH, zero, q)], axis=0)
        qt_ref[...] = q.T
        m_ref[...] = jnp.full(m_ref.shape, NEG, jnp.float32)
        l_ref[...] = jnp.zeros(l_ref.shape, jnp.float32)
        o_ref[...] = jnp.zeros(o_ref.shape, jnp.float32)

    @pl.when(step == z)
    def _():
        def body(i, _):
            visit(pl.multiple_of(i * KEYS, KEYS), KEYS, True)
            return 0

        lax.fori_loop(0, (y * tokens) // KEYS + 1, body, 0)

    @pl.when(step > z)
    def _():
        for start in range(0, keys, KEYS):
            visit(start, KEYS, False)

    @pl.when(step >= z)
    def _():
        total = l_ref[...]
        out_ref[0, :DV] = (o_ref[...] / total).astype(jnp.bfloat16)
        weight = m_ref[...] + jnp.log(total)
        high = weight.astype(jnp.bfloat16)
        rest = weight - high.astype(jnp.float32)
        middle = rest.astype(jnp.bfloat16)
        low = (rest - middle.astype(jnp.float32)).astype(jnp.bfloat16)
        pad = jnp.zeros((ROWS - DV - 3, weight.shape[1]), jnp.bfloat16)
        out_ref[0, DV:] = jnp.concatenate([high, middle, low, pad], axis=0)

    @pl.when(step < z)
    def _():
        out_ref[0, :DV] = jnp.zeros((DV, 2 * tokens), jnp.bfloat16)
        row = lax.broadcasted_iota(jnp.int32, (ROWS - DV, 2 * tokens), 0)
        out_ref[0, DV:] = jnp.where(row == 0, NEG, 0.0).astype(jnp.bfloat16)


def attend(where, queries, keys, values):
    blocks, tokens, _ = queries.shape
    count = keys.shape[0]

    def whole(shape):
        return pl.BlockSpec(shape, lambda g, w: (0, 0))

    return pl.pallas_call(
        attend_kernel,
        grid_spec=pltpu.PrefetchScalarGridSpec(
            num_scalar_prefetch=1,
            grid=(blocks,),
            in_specs=[
                pl.BlockSpec((1, tokens, 2 * DH), lambda g, w: (g, 0, 0)),
                whole(keys.shape),
                whole(values.shape),
            ],
            out_specs=pl.BlockSpec((1, ROWS, 2 * tokens), lambda g, w: (g, 0, 0)),
            scratch_shapes=[
                pltpu.VMEM((DV, count), jnp.bfloat16),
                pltpu.VMEM((2 * DH, 2 * tokens), jnp.bfloat16),
                pltpu.VMEM((1, 2 * tokens), jnp.float32),
                pltpu.VMEM((1, 2 * tokens), jnp.float32),
                pltpu.VMEM((DV, 2 * tokens), jnp.float32),
            ],
        ),
        out_shape=jax.ShapeDtypeStruct((blocks, ROWS, 2 * tokens), jnp.bfloat16),
        compiler_params=pltpu.CompilerParams(dimension_semantics=("arbitrary",)),
        cost_estimate=pl.CostEstimate(
            flops=blocks * count * tokens * 4 * 256,
            bytes_accessed=blocks * tokens * 1024 + count * 512,
            transcendentals=blocks * count * tokens * 2,
        ),
        name="attend",
        interpret=INTERPRET,
    )(where, queries, keys, values)


def finish_kernel(parts_ref, mix_ref, gain_ref, out_ref):
    blocks = parts_ref.shape[0]
    tokens = out_ref.shape[0]
    logs = []
    for i in range(blocks):
        rows = parts_ref[i, DV:].astype(jnp.float32)
        logs.append(rows[0:1] + rows[1:2] + rows[2:3])
    top = functools.reduce(jnp.maximum, logs)
    shares = [jnp.exp(log - top) for log in logs]
    total = functools.reduce(jnp.add, shares)
    acc = jnp.zeros((DV, 2 * tokens), jnp.float32)
    for i in range(blocks):
        acc = acc + parts_ref[i, :DV].astype(jnp.float32) * (shares[i] / total)
    att = acc[:, :tokens] - mix_ref[...] * acc[:, tokens:]
    att = att * lax.rsqrt(jnp.mean(att * att, axis=0, keepdims=True) + EPSILON)
    out_ref[...] = (att.T * gain_ref[...]).astype(jnp.bfloat16)


def finish(parts, mixing, gain):
    tokens = parts.shape[2] // 2
    return pl.pallas_call(
        finish_kernel,
        out_shape=jax.ShapeDtypeStruct((tokens, DV), jnp.bfloat16),
        name="finish",
        interpret=INTERPRET,
    )(parts, jnp.broadcast_to(mixing.reshape(1, 1), (1, tokens)), gain.reshape(1, DV))


def rotate(vectors, cosine, sine):
    half = vectors.shape[-1] // 2
    a = vectors[..., :half]
    b = vectors[..., half:]
    return jnp.concatenate([a * cosine - b * sine, a * sine + b * cosine], axis=-1)


def decay_log(head, length):
    pair = (head // 2).astype(jnp.float32)
    quick = jnp.log1p(-jnp.exp2(-5.0 - pair / 4.0))
    slow = jnp.log1p(-1.0 / (length * (1.0 + pair)))
    return jnp.where(head % 2 == 0, quick, slow)


def layer(
    features,
    norm_gain,
    att_query,
    att_key,
    att_value,
    att_lambda,
    att_gain,
    ret_query,
    ret_key,
    ret_value,
    ret_gain,
    out_weight,
):
    z = lax.axis_index(Z)
    y = lax.axis_index("y")
    c = lax.axis_index("c")
    ny = lax.axis_size("y")
    nz = lax.axis_size(Z)
    chip = z * ny + y

    def half(array, h):
        width = array.shape[1] // 2
        return array[:, h * width : (h + 1) * width]

    per_head = (ret_query, ret_key, ret_value)
    halves = jnp.stack(
        [
            jnp.concatenate([half(att_query, h), whole] + [half(a, h) for a in per_head], axis=1)
            for h, whole in enumerate((att_key, att_value))
        ]
    )
    rows, width = halves.shape[1:]
    sent = jnp.broadcast_to(halves[None], (ny, 2, rows, width)).reshape(2 * ny, rows, width)
    w_z = lax.all_to_all(sent, ("y", "c"), 0, 0, tiled=True).reshape(2 * ny * rows, width)
    w_z, features = lax.optimization_barrier((w_z, features))
    w_all = to_all(w_z, Z).reshape(-1, width)

    groups = lax.axis_size("tp")
    x = lax.axis_index("tp")
    pieces = [features] + [
        lax.ppermute(features, "tp", [(i, (i + k) % groups) for i in range(groups)])
        for k in range(1, groups)
    ]
    tokens = features.shape[0]
    gathered = jnp.zeros((groups, *features.shape), features.dtype)
    for k, piece in enumerate(pieces):
        gathered = lax.dynamic_update_index_in_dim(gathered, piece, (x - k) % groups, 0)
    floats = gathered.astype(jnp.float32)
    mean_sq = jnp.sum(floats * floats, axis=(0, 2)) / norm_gain.shape[0]
    gain = norm_gain.reshape(groups, 1, -1)
    scaled = floats * lax.rsqrt(mean_sq + EPSILON)[None, :, None] * gain
    normed = jnp.concatenate(list(scaled.astype(jnp.bfloat16)), axis=1)
    across = swapped(normed)
    both = jnp.concatenate(
        [jnp.where(c == 0, normed, across), jnp.where(c == 0, across, normed)], axis=0
    )
    tokens = 2 * tokens
    made = jnp.dot(both, w_all, preferred_element_type=jnp.float32).astype(jnp.bfloat16)
    q_att = made[:, :128]
    kv = made[:, 128:256]
    q_ret = made[:, 256:320].astype(jnp.float32)
    k_ret = made[:, 320:384].astype(jnp.float32)
    v_ret = made[:, 384:512].astype(jnp.float32)

    highest = lax.Precision.HIGHEST
    length = nz * ny * tokens
    log_decay = decay_log(lax.axis_index("tp") * 2 + c, float(length))
    offsets = jnp.arange(tokens).astype(jnp.float32)
    positions = (chip * tokens + jnp.arange(tokens)).astype(jnp.float32)
    inverse = 10000.0 ** (-jnp.arange(0, DH, 2).astype(jnp.float32) / DH)
    angles = positions[:, None] * inverse[None, :]
    cosine, sine = jnp.cos(angles), jnp.sin(angles)
    q_rot = rotate(q_ret, cosine, sine)
    k_rot = rotate(k_ret, cosine, sine) * DH ** (-0.5)
    key_weight = jnp.exp(log_decay * (tokens - 1.0 - offsets))
    own_state = jnp.einsum("jd,je->de", k_rot * key_weight[:, None], v_ret, precision=highest)

    spread = to_all(jnp.concatenate([kv, own_state.astype(jnp.bfloat16)], axis=0), "y")
    kv_mine = spread[:, :tokens].reshape(ny * tokens, 2 * DH)
    kv_other = swapped(kv_mine)
    keys = jnp.where(c == 0, kv_mine, kv_other)
    values = jnp.where(c == 0, kv_other, kv_mine)
    states = spread[:, tokens:].astype(jnp.float32)
    ys = jnp.arange(ny)
    zs = jnp.arange(nz)
    span = log_decay * tokens
    to_end = jnp.exp(span * (ny - 1 - ys).astype(jnp.float32))
    sums = jnp.sum(states * to_end[:, None, None], axis=0)
    scaled_q = q_att * jnp.bfloat16(DH ** (-0.5))
    along = to_all(jnp.concatenate([scaled_q, sums.astype(jnp.bfloat16)], axis=0), Z)
    parts = attend(jnp.stack([z, y]).astype(jnp.int32), along[:, :tokens], keys, values)
    parts = lax.all_to_all(parts, Z, 0, 0, tiled=True)

    others = along[:, tokens:].astype(jnp.float32)
    y_weight = jnp.where(ys < y, jnp.exp(span * jnp.maximum(y - 1 - ys, 0).astype(jnp.float32)), 0.0)
    steps = jnp.maximum(ny * (z - 1 - zs) + y, 0).astype(jnp.float32)
    z_weight = jnp.where(zs < z, jnp.exp(span * steps), 0.0)
    carried = jnp.sum(states * y_weight[:, None, None], axis=0)
    carried = carried + jnp.sum(others * z_weight[:, None, None], axis=0)

    distance = offsets[:, None] - offsets[None, :]
    inside = jnp.where(distance >= 0, jnp.exp(log_decay * jnp.maximum(distance, 0.0)), 0.0)
    scores = jnp.einsum("id,jd->ij", q_rot, k_rot, precision=highest) * inside
    within = jnp.dot(scores, v_ret, precision=highest)
    query_weight = jnp.exp(log_decay * (offsets + 1.0))
    ret = within + jnp.dot(q_rot, carried, precision=highest) * query_weight[:, None]
    ret = ret * lax.rsqrt(jnp.mean(ret * ret, axis=-1, keepdims=True) + EPSILON) * ret_gain
    ret = ret.astype(jnp.bfloat16)

    mixing = lax.dynamic_index_in_dim(att_lambda, c, 0, keepdims=False)
    att = finish(parts, mixing, att_gain)

    heads = jnp.concatenate([att, ret], axis=1).reshape(2, tokens // 2, 2 * DV)
    heads = lax.all_to_all(heads, "c", 0, 0, tiled=True)
    joined = jnp.concatenate(
        [heads[0, :, :DV], heads[1, :, :DV], heads[0, :, DV:], heads[1, :, DV:]], axis=1
    )
    partial = jnp.dot(
        joined, out_weight.reshape(-1, out_weight.shape[2]), preferred_element_type=jnp.float32
    ).astype(jnp.bfloat16)
    partial = lax.all_to_all(
        partial.reshape(groups, -1, partial.shape[1]), "tp", 0, 0, tiled=True
    )
    return jnp.sum(partial.astype(jnp.float32), axis=0)


def solution(mesh):
    devices = mesh.devices
    torus = Mesh(devices.reshape(2, 4, -1, 2, devices.shape[-1]), SP_TP)
    return jax.shard_map(
        layer,
        mesh=torus,
        in_specs=(
            P(SP, "tp"),
            P(),
            P(SP, "tp"),
            P(SP, "tp"),
            P(SP, "tp"),
            P("tp"),
            P(),
            P(SP, "tp"),
            P(SP, "tp"),
            P(SP, "tp"),
            P(),
            P(None, "tp", None),
        ),
        out_specs=P(SP_TP, None),
        check_vma=False,
    )
```

```python
import functools

import jax
import jax.numpy as jnp
from jax import lax
from jax.experimental import pallas as pl
from jax.experimental.pallas import tpu as pltpu
from jax.sharding import Mesh
from jax.sharding import PartitionSpec as P

DH = 64
DV = 128
SEG = 64
Z = ("zh", "zl")
SP = ("zh", "zl", "y", "c")
SP_TP = ("zh", "zl", "y", "c", "tp")
EPSILON = 1e-06
NEG = -1e30
KEYS = 512
ROWS = 144
VMEM = pl.BlockSpec(memory_space=pltpu.VMEM)
SMEM = pl.BlockSpec(memory_space=pltpu.SMEM)
INTERPRET = False


def swapped(value):
    return lax.ppermute(value, "c", [(0, 1), (1, 0)])


def shifted(value, step):
    count = lax.axis_size(Z)
    return lax.ppermute(value, Z, [(i, (i + step) % count) for i in range(count)])


def two_steps(own, half):
    before = shifted(own, 1)
    after = shifted(own, -1)
    low = shifted(before[:half], 1)
    high = shifted(after[half:], -1)
    return before, after, low, high


def pack_kernel(query_ref, key_ref, value_ref, rq_ref, rk_ref, rv_ref, out_ref):
    for h, whole in enumerate((key_ref, value_ref)):
        parts = []
        for ref in (query_ref, None, rq_ref, rk_ref, rv_ref):
            if ref is None:
                parts.append(whole[...])
            else:
                width = ref.shape[1] // 2
                parts.append(ref[:, h * width : (h + 1) * width])
        row = jnp.concatenate(parts, axis=1)
        for i in range(out_ref.shape[0]):
            out_ref[i, h] = row


def pack(count, *matrices):
    rows = matrices[0].shape[0]
    return pl.pallas_call(
        pack_kernel,
        out_shape=jax.ShapeDtypeStruct((count, 2, rows, 512), jnp.bfloat16),
        name="pack",
        interpret=INTERPRET,
    )(*matrices)


def exact(a, b, dims):
    return lax.dot_general(
        a, b, (dims, ((), ())), precision=lax.Precision.HIGHEST, preferred_element_type=jnp.float32
    )


def retain_kernel(made_ref, turn_ref, decay_ref, send_ref, query_ref, within_ref):
    tokens = made_ref.shape[0]
    pair = made_ref[:, 256:384].astype(jnp.float32)
    lane = lax.broadcasted_iota(jnp.int32, pair.shape, 1)
    quarter = DH // 2
    ahead = pltpu.roll(pair, 2 * DH - quarter, 1)
    behind = pltpu.roll(pair, quarter, 1)
    crossed = jnp.where((lane & quarter) == 0, -ahead, behind)
    turned = pair * turn_ref[0] + crossed * turn_ref[1]
    query = turned[:, :DH]
    key = turned[:, DH:] * DH ** (-0.5)
    value = made_ref[:, 384:512].astype(jnp.float32)
    log_decay = decay_ref[0]
    offset = lax.broadcasted_iota(jnp.int32, (tokens, 1), 0).astype(jnp.float32)
    i = lax.broadcasted_iota(jnp.int32, (tokens, tokens), 0)
    j = lax.broadcasted_iota(jnp.int32, (tokens, tokens), 1)
    distance = (i - j).astype(jnp.float32)
    inside = jnp.where(i >= j, jnp.exp(log_decay * jnp.maximum(distance, 0.0)), 0.0)
    scores = exact(query, key, ((1,), (1,))) * inside
    within_ref[...] = exact(scores, value, ((1,), (0,)))
    query_ref[...] = query * jnp.exp(log_decay * (offset + 1.0))
    state = exact(key * jnp.exp(log_decay * (tokens - 1.0 - offset)), value, ((0,), (0,)))
    kv = made_ref[:, 128:256]
    for k in range(send_ref.shape[0]):
        send_ref[k, :tokens] = kv
        send_ref[k, tokens:] = state.astype(jnp.bfloat16)


def retain(made, turn, log_decay, count):
    tokens = made.shape[0]
    return pl.pallas_call(
        retain_kernel,
        in_specs=[VMEM, VMEM, SMEM],
        out_shape=[
            jax.ShapeDtypeStruct((count, tokens + DH, DV), jnp.bfloat16),
            jax.ShapeDtypeStruct((tokens, DH), jnp.float32),
            jax.ShapeDtypeStruct((tokens, DV), jnp.float32),
        ],
        name="retain",
        interpret=INTERPRET,
    )(made, turn, log_decay.reshape(1))


def pass_on_kernel(spread_ref, made_ref, weight_ref, send_ref):
    tokens = made_ref.shape[0]
    query = made_ref[:, : 2 * DH] * jnp.bfloat16(DH ** (-0.5))
    total = jnp.zeros((DH, DV), jnp.float32)
    for i in range(spread_ref.shape[0]):
        total = total + spread_ref[i, tokens:].astype(jnp.float32) * weight_ref[i]
    for k in range(send_ref.shape[0]):
        send_ref[k, :tokens] = query
        send_ref[k, tokens:] = total.astype(jnp.bfloat16)


def pass_on(spread, made, weight, count):
    return pl.pallas_call(
        pass_on_kernel,
        in_specs=[VMEM, VMEM, SMEM],
        out_shape=jax.ShapeDtypeStruct((count, *spread.shape[1:]), jnp.bfloat16),
        name="pass_on",
        interpret=INTERPRET,
    )(spread, made, weight)


def attend_kernel(
    where_ref, q_ref, mine_ref, other_ref, out_ref, k_ref, vt_ref, qt_ref, m_ref, l_ref, o_ref
):
    step = pl.program_id(0)
    z = where_ref[0]
    y = where_ref[1]
    keys = k_ref.shape[0]
    tokens = q_ref.shape[1]

    def prepare(key_ref, value_ref):
        for i in range(key_ref.shape[0]):
            at = slice(i * tokens, (i + 1) * tokens)
            k_ref[at] = key_ref[i, :tokens]
            vt_ref[:, at] = value_ref[i, :tokens].T

    @pl.when((step == 0) & (where_ref[2] == 0))
    def _():
        prepare(mine_ref, other_ref)

    @pl.when((step == 0) & (where_ref[2] != 0))
    def _():
        prepare(other_ref, mine_ref)

    def visit(start, count, masked):
        s = jnp.dot(k_ref[pl.ds(start, count)], qt_ref[...], preferred_element_type=jnp.float32)
        if masked:
            rows = lax.broadcasted_iota(jnp.int32, s.shape, 0) + start
            cols = lax.broadcasted_iota(jnp.int32, s.shape, 1) % tokens + y * tokens
            allowed = (rows // SEG) <= (cols // SEG)
            s = jnp.where(allowed, s, NEG)
        old = m_ref[...]
        top = jnp.maximum(old, jnp.max(s, axis=0, keepdims=True))
        w = jnp.exp(s - top)
        factor = jnp.exp(old - top)
        m_ref[...] = top
        l_ref[...] = l_ref[...] * factor + jnp.sum(w, axis=0, keepdims=True)
        o_ref[...] = o_ref[...] * factor + jnp.dot(
            vt_ref[:, pl.ds(start, count)],
            w.astype(jnp.bfloat16),
            preferred_element_type=jnp.float32,
        )

    @pl.when(step >= z)
    def _():
        q = q_ref[0]
        lane = lax.broadcasted_iota(jnp.int32, q.shape, 1)
        zero = jnp.zeros_like(q)
        q = jnp.concatenate([jnp.where(lane < DH, q, zero), jnp.where(lane < DH, zero, q)], axis=0)
        qt_ref[...] = q.T
        m_ref[...] = jnp.full(m_ref.shape, NEG, jnp.float32)
        l_ref[...] = jnp.zeros(l_ref.shape, jnp.float32)
        o_ref[...] = jnp.zeros(o_ref.shape, jnp.float32)

    @pl.when(step == z)
    def _():
        def body(i, _):
            visit(pl.multiple_of(i * KEYS, KEYS), KEYS, True)
            return 0

        lax.fori_loop(0, (y * tokens) // KEYS + 1, body, 0)

    @pl.when(step > z)
    def _():
        for start in range(0, keys, KEYS):
            visit(start, KEYS, False)

    @pl.when(step >= z)
    def _():
        total = l_ref[...]
        out_ref[0, :DV] = (o_ref[...] / total).astype(jnp.bfloat16)
        weight = m_ref[...] + jnp.log(total)
        high = weight.astype(jnp.bfloat16)
        rest = weight - high.astype(jnp.float32)
        middle = rest.astype(jnp.bfloat16)
        low = (rest - middle.astype(jnp.float32)).astype(jnp.bfloat16)
        pad = jnp.zeros((ROWS - DV - 3, weight.shape[1]), jnp.bfloat16)
        out_ref[0, DV:] = jnp.concatenate([high, middle, low, pad], axis=0)

    @pl.when(step < z)
    def _():
        out_ref[0, :DV] = jnp.zeros((DV, 2 * tokens), jnp.bfloat16)
        row = lax.broadcasted_iota(jnp.int32, (ROWS - DV, 2 * tokens), 0)
        out_ref[0, DV:] = jnp.where(row == 0, NEG, 0.0).astype(jnp.bfloat16)


def attend(where, along, mine, other, tokens):
    blocks = along.shape[0]
    count = mine.shape[0] * tokens

    def whole(shape):
        return pl.BlockSpec(shape, lambda g, w: (0,) * len(shape))

    return pl.pallas_call(
        attend_kernel,
        grid_spec=pltpu.PrefetchScalarGridSpec(
            num_scalar_prefetch=1,
            grid=(blocks,),
            in_specs=[
                pl.BlockSpec((1, tokens, 2 * DH), lambda g, w: (g, 0, 0)),
                whole(mine.shape),
                whole(other.shape),
            ],
            out_specs=pl.BlockSpec((1, ROWS, 2 * tokens), lambda g, w: (g, 0, 0)),
            scratch_shapes=[
                pltpu.VMEM((count, 2 * DH), jnp.bfloat16),
                pltpu.VMEM((DV, count), jnp.bfloat16),
                pltpu.VMEM((2 * DH, 2 * tokens), jnp.bfloat16),
                pltpu.VMEM((1, 2 * tokens), jnp.float32),
                pltpu.VMEM((1, 2 * tokens), jnp.float32),
                pltpu.VMEM((DV, 2 * tokens), jnp.float32),
            ],
        ),
        out_shape=jax.ShapeDtypeStruct((blocks, ROWS, 2 * tokens), jnp.bfloat16),
        compiler_params=pltpu.CompilerParams(dimension_semantics=("arbitrary",)),
        cost_estimate=pl.CostEstimate(
            flops=blocks * count * tokens * 4 * 256,
            bytes_accessed=blocks * tokens * 1024 + count * 512,
            transcendentals=blocks * count * tokens * 2,
        ),
        name="attend",
        interpret=INTERPRET,
    )(where, along, mine, other)


def finish_kernel(
    parts_ref, mix_ref, gain_ref, spread_ref, along_ref, weight_ref, query_ref, within_ref, out_ref
):
    blocks = parts_ref.shape[0]
    tokens = query_ref.shape[0]
    logs = []
    for i in range(blocks):
        rows = parts_ref[i, DV:].astype(jnp.float32)
        logs.append(rows[0:1] + rows[1:2] + rows[2:3])
    top = functools.reduce(jnp.maximum, logs)
    shares = [jnp.exp(log - top) for log in logs]
    total = functools.reduce(jnp.add, shares)
    acc = jnp.zeros((DV, 2 * tokens), jnp.float32)
    for i in range(blocks):
        acc = acc + parts_ref[i, :DV].astype(jnp.float32) * (shares[i] / total)
    att = acc[:, :tokens] - mix_ref[0] * acc[:, tokens:]
    att = att * lax.rsqrt(jnp.mean(att * att, axis=0, keepdims=True) + EPSILON)
    att = (att.T * gain_ref[0:1]).astype(jnp.bfloat16)
    carried = jnp.zeros((DH, DV), jnp.float32)
    chips = spread_ref.shape[0]
    for i in range(chips):
        carried = carried + spread_ref[i, tokens:].astype(jnp.float32) * weight_ref[i]
    for i in range(blocks):
        carried = carried + along_ref[i, tokens:].astype(jnp.float32) * weight_ref[chips + i]
    ret = within_ref[...] + exact(query_ref[...], carried, ((1,), (0,)))
    ret = ret * lax.rsqrt(jnp.mean(ret * ret, axis=1, keepdims=True) + EPSILON)
    ret = (ret * gain_ref[1:2]).astype(jnp.bfloat16)
    half = tokens // 2
    for i in range(2):
        out_ref[i, :, :DV] = att[i * half : (i + 1) * half]
        out_ref[i, :, DV:] = ret[i * half : (i + 1) * half]


def finish(parts, mixing, gains, spread, along, weights, query, within):
    tokens = query.shape[0]
    return pl.pallas_call(
        finish_kernel,
        in_specs=[VMEM, SMEM, VMEM, VMEM, VMEM, SMEM, VMEM, VMEM],
        out_shape=jax.ShapeDtypeStruct((2, tokens // 2, 2 * DV), jnp.bfloat16),
        name="finish",
        interpret=INTERPRET,
    )(parts, mixing.reshape(1), gains, spread, along, weights, query, within)


def decay_log(head, length):
    pair = (head // 2).astype(jnp.float32)
    quick = jnp.log1p(-jnp.exp2(-5.0 - pair / 4.0))
    slow = jnp.log1p(-1.0 / (length * (1.0 + pair)))
    return jnp.where(head % 2 == 0, quick, slow)


def layer(
    features,
    norm_gain,
    att_query,
    att_key,
    att_value,
    att_lambda,
    att_gain,
    ret_query,
    ret_key,
    ret_value,
    ret_gain,
    out_weight,
):
    z = lax.axis_index(Z)
    y = lax.axis_index("y")
    c = lax.axis_index("c")
    x = lax.axis_index("tp")
    ny = lax.axis_size("y")
    nz = lax.axis_size(Z)
    nl = lax.axis_size("zl")
    groups = lax.axis_size("tp")
    chip = z * ny + y
    tokens = 2 * features.shape[0]

    sent = pack(2 * ny, att_query, att_key, att_value, ret_query, ret_key, ret_value)
    rows, width = sent.shape[2:]
    sent = sent.reshape(4 * ny, rows, width)
    even = jnp.arange(0, DH, 2).astype(jnp.float32)
    small = (even, jnp.arange(ny), jnp.arange(nz), chip, z, y, c, x)
    sent, small = lax.optimization_barrier((sent, small))
    w_own = lax.all_to_all(sent, ("zh", "y", "c"), 0, 0, tiled=True)
    w_own = w_own.reshape(4 * ny * rows, width)
    inputs = (features, norm_gain, att_lambda, att_gain, ret_gain)
    w_own, inputs, small = lax.optimization_barrier((w_own, inputs, small))
    features, norm_gain, att_lambda, att_gain, ret_gain = inputs
    even, ys, zs, chip, z, y, c, x = small
    w_before, w_after, w_low, w_high = two_steps(w_own, 2 * ny * rows)

    residues = [(z + k) % nl for k in (0, nl - 1, 1, 2)]

    pieces = [features] + [
        lax.ppermute(features, "tp", [(i, (i + k) % groups) for i in range(groups)])
        for k in range(1, groups)
    ]
    gathered = jnp.zeros((groups, *features.shape), features.dtype)
    for k, piece in enumerate(pieces):
        gathered = lax.dynamic_update_index_in_dim(gathered, piece, (x - k) % groups, 0)
    floats = gathered.astype(jnp.float32)
    mean_sq = jnp.sum(floats * floats, axis=(0, 2)) / norm_gain.shape[0]
    gain = norm_gain.reshape(groups, 1, -1)
    scaled = floats * lax.rsqrt(mean_sq + EPSILON)[None, :, None] * gain
    scaled = scaled.astype(jnp.bfloat16)
    per_tp = nz // groups
    wide = scaled.shape[2] // per_tp
    by_z = jnp.stack([scaled[i // per_tp][:, (i % per_tp) * wide :][:, :wide] for i in range(nz)])
    across = swapped(by_z)
    both = jnp.stack([jnp.where(c == 0, by_z, across), jnp.where(c == 0, across, by_z)])

    log_decay = decay_log(x * 2 + c, float(nz * ny * tokens))
    positions = (chip * tokens + jnp.arange(tokens)).astype(jnp.float32)
    inverse = 10000.0 ** (-even / DH)
    angles = positions[:, None] * inverse[None, :]
    turn = jnp.stack([jnp.tile(jnp.cos(angles), (1, 4)), jnp.tile(jnp.sin(angles), (1, 4))])
    span = log_decay * tokens
    to_end = jnp.exp(span * (ny - 1 - ys).astype(jnp.float32))
    y_steps = jnp.maximum(y - 1 - ys, 0).astype(jnp.float32)
    z_steps = jnp.maximum(ny * (z - 1 - zs) + y, 0).astype(jnp.float32)
    before = jnp.concatenate(
        [
            jnp.where(ys < y, jnp.exp(span * y_steps), 0.0),
            jnp.where(zs < z, jnp.exp(span * z_steps), 0.0),
        ]
    )
    where = jnp.stack([z, y, c]).astype(jnp.int32)
    mixing = lax.dynamic_index_in_dim(att_lambda, c, 0, keepdims=False)
    gains = jnp.stack([att_gain, ret_gain])

    def made_by(k, high, matrix):
        left = lax.dynamic_index_in_dim(both, high * nl + residues[k], 1, keepdims=False)
        left = left.reshape(tokens, wide)
        return jnp.dot(left, matrix, preferred_element_type=jnp.float32)

    made = made_by(0, 0, w_own[:wide]) + made_by(0, 1, w_own[wide:])
    made = made + made_by(1, 0, w_before[:wide]) + made_by(1, 1, w_before[wide:])
    made = made + made_by(2, 0, w_after[:wide]) + made_by(2, 1, w_after[wide:])
    made = made + made_by(3, 0, w_low) + made_by(3, 1, w_high)
    made = made.astype(jnp.bfloat16)
    made, turn, log_decay, to_end, before, where, mixing, gains = lax.optimization_barrier(
        (made, turn, log_decay, to_end, before, where, mixing, gains)
    )

    send, query, within = retain(made, turn, log_decay, ny)
    spread = lax.all_to_all(send, "y", 0, 0, tiled=True)
    send = pass_on(spread, made, to_end, nz)
    along = lax.all_to_all(send, Z, 0, 0, tiled=True)
    spread, along = lax.optimization_barrier((spread, along))
    parts = attend(where, along, spread, swapped(spread), tokens)
    parts = lax.all_to_all(parts, Z, 0, 0, tiled=True)

    heads = finish(parts, mixing, gains, spread, along, before, query, within)
    heads = lax.all_to_all(heads, "c", 0, 0, tiled=True)
    joined = jnp.concatenate(
        [heads[0, :, :DV], heads[1, :, :DV], heads[0, :, DV:], heads[1, :, DV:]], axis=1
    )
    partial = jnp.dot(
        joined, out_weight.reshape(-1, out_weight.shape[2]), preferred_element_type=jnp.float32
    ).astype(jnp.bfloat16)
    partial = lax.all_to_all(
        partial.reshape(groups, -1, partial.shape[1]), "tp", 0, 0, tiled=True
    )
    return jnp.sum(partial.astype(jnp.float32), axis=0)


def solution(mesh):
    devices = mesh.devices
    torus = Mesh(devices.reshape(2, 4, -1, 2, devices.shape[-1]), SP_TP)
    return jax.shard_map(
        layer,
        mesh=torus,
        in_specs=(
            P(SP, "tp"),
            P(),
            P(SP, "tp"),
            P(SP, "tp"),
            P(SP, "tp"),
            P("tp"),
            P(),
            P(SP, "tp"),
            P(SP, "tp"),
            P(SP, "tp"),
            P(),
            P(None, "tp", None),
        ),
        out_specs=P(SP_TP, None),
        check_vma=False,
    )
```

```python
import functools

import jax
import jax.numpy as jnp
from jax import lax
from jax.experimental import pallas as pl
from jax.experimental.pallas import tpu as pltpu
from jax.sharding import Mesh
from jax.sharding import PartitionSpec as P

DH = 64
DV = 128
SEG = 64
Z = ("zh", "zl")
SP = ("zh", "zl", "y", "c")
SP_TP = ("zh", "zl", "y", "c", "tp")
EPSILON = 1e-06
NEG = -1e30
KEYS = 512
ROWS = 144
MIB = 1 << 20
VMEM = pl.BlockSpec(memory_space=pltpu.VMEM)
SMEM = pl.BlockSpec(memory_space=pltpu.SMEM)
INTERPRET = False


def swapped(value):
    return lax.ppermute(value, "c", [(0, 1), (1, 0)])


def shifted(value, step):
    count = lax.axis_size(Z)
    return lax.ppermute(value, Z, [(i, (i + step) % count) for i in range(count)])


def two_steps(own, half):
    before = shifted(own, 1)
    after = shifted(own, -1)
    low = shifted(before[:half], 1)
    high = shifted(after[half:], -1)
    return before, after, low, high


def pack_kernel(query_ref, key_ref, value_ref, rq_ref, rk_ref, rv_ref, out_ref):
    for h, whole in enumerate((key_ref, value_ref)):
        parts = []
        for ref in (query_ref, None, rq_ref, rk_ref, rv_ref):
            if ref is None:
                parts.append(whole[...])
            else:
                width = ref.shape[1] // 2
                parts.append(ref[:, h * width : (h + 1) * width])
        row = jnp.concatenate(parts, axis=1)
        for i in range(out_ref.shape[0]):
            out_ref[i, h] = row


def pack(count, *matrices):
    rows = matrices[0].shape[0]
    return pl.pallas_call(
        pack_kernel,
        out_shape=jax.ShapeDtypeStruct((count, 2, rows, 512), jnp.bfloat16),
        compiler_params=pltpu.CompilerParams(vmem_limit_bytes=4 * MIB),
        name="pack",
        interpret=INTERPRET,
    )(*matrices)


def rounded(a, b, dims):
    return lax.dot_general(
        a.astype(jnp.bfloat16),
        b.astype(jnp.bfloat16),
        (dims, ((), ())),
        preferred_element_type=jnp.float32,
    )


def norm_kernel(*refs):
    *piece_refs, place_ref, gain_ref, out_ref = refs
    groups = len(piece_refs)
    blocks, _, wide = out_ref.shape
    per_tp = blocks // groups
    total = 0.0
    for ref in piece_refs:
        floats = ref[...].astype(jnp.float32)
        total = total + jnp.sum(floats * floats, axis=1, keepdims=True)
    scale = lax.rsqrt(total / (blocks * wide) + EPSILON)
    for k, ref in enumerate(piece_refs):
        for i in range(per_tp):
            at = place_ref[k] * per_tp + i
            part = ref[:, i * wide : (i + 1) * wide].astype(jnp.float32)
            out_ref[at] = (part * scale * gain_ref[at]).astype(jnp.bfloat16)


def norm(pieces, place, gain, blocks):
    rows, width = pieces[0].shape
    wide = width * len(pieces) // blocks
    return pl.pallas_call(
        norm_kernel,
        in_specs=[VMEM] * len(pieces) + [SMEM, VMEM],
        out_shape=jax.ShapeDtypeStruct((blocks, rows, wide), jnp.bfloat16),
        compiler_params=pltpu.CompilerParams(vmem_limit_bytes=6 * MIB),
        name="norm",
        interpret=INTERPRET,
    )(*pieces, place, gain.reshape(blocks, 1, wide))


def project_kernel(
    own_ref,
    across_ref,
    w_own_ref,
    w_before_ref,
    w_after_ref,
    w_low_ref,
    w_high_ref,
    place_ref,
    turn_ref,
    decay_ref,
    send_ref,
    att_ref,
    query_ref,
    within_ref,
):
    half, wide = own_ref.shape[1:]
    tokens = 2 * half
    low, high = slice(0, wide), slice(wide, 2 * wide)
    weights = [(w_own_ref, low), (w_own_ref, high), (w_before_ref, low), (w_before_ref, high)]
    weights += [(w_after_ref, low), (w_after_ref, high), (w_low_ref, low), (w_high_ref, low)]
    made = jnp.zeros((tokens, w_own_ref.shape[1]), jnp.float32)
    for k, (ref, at) in enumerate(weights):
        block = place_ref[1 + k]
        left = jnp.concatenate([own_ref[block], across_ref[block]], axis=0)
        made = made + jnp.dot(left, ref[at], preferred_element_type=jnp.float32)
    first = place_ref[0] == 0
    made = jnp.concatenate(
        [jnp.where(first, made[:half], made[half:]), jnp.where(first, made[half:], made[:half])],
        axis=0,
    ).astype(jnp.bfloat16)
    att_ref[...] = made[:, : 2 * DH] * jnp.bfloat16(DH ** (-0.5))

    pair = made[:, 256:384].astype(jnp.float32)
    lane = lax.broadcasted_iota(jnp.int32, pair.shape, 1)
    quarter = DH // 2
    ahead = pltpu.roll(pair, 2 * DH - quarter, 1)
    behind = pltpu.roll(pair, quarter, 1)
    crossed = jnp.where((lane & quarter) == 0, -ahead, behind)
    turned = pair * turn_ref[0] + crossed * turn_ref[1]
    query = turned[:, :DH]
    key = turned[:, DH:] * DH ** (-0.5)
    value = made[:, 384:512]
    log_decay = decay_ref[0]
    offset = lax.broadcasted_iota(jnp.int32, (tokens, 1), 0).astype(jnp.float32)
    state = rounded(key * jnp.exp(log_decay * (tokens - 1.0 - offset)), value, ((0,), (0,)))
    state = state.astype(jnp.bfloat16)
    for k in range(send_ref.shape[0]):
        send_ref[k, :tokens] = made[:, 128:256]
        send_ref[k, tokens:] = state
    i = lax.broadcasted_iota(jnp.int32, (tokens, tokens), 0)
    j = lax.broadcasted_iota(jnp.int32, (tokens, tokens), 1)
    distance = (i - j).astype(jnp.float32)
    inside = jnp.where(i >= j, jnp.exp(log_decay * jnp.maximum(distance, 0.0)), 0.0)
    scores = rounded(query, key, ((1,), (1,))) * inside
    within_ref[...] = rounded(scores, value, ((1,), (0,)))
    query_ref[...] = query * jnp.exp(log_decay * (offset + 1.0))


def project(own, across, weights, place, turn, log_decay, count):
    tokens = 2 * own.shape[1]
    return pl.pallas_call(
        project_kernel,
        in_specs=[VMEM] * 7 + [SMEM, VMEM, SMEM],
        out_shape=[
            jax.ShapeDtypeStruct((count, tokens + DH, DV), jnp.bfloat16),
            jax.ShapeDtypeStruct((tokens, 2 * DH), jnp.bfloat16),
            jax.ShapeDtypeStruct((tokens, DH), jnp.float32),
            jax.ShapeDtypeStruct((tokens, DV), jnp.float32),
        ],
        compiler_params=pltpu.CompilerParams(vmem_limit_bytes=12 * MIB),
        name="project",
        interpret=INTERPRET,
    )(own, across, *weights, place, turn, log_decay.reshape(1))


def pass_on_kernel(spread_ref, att_ref, weight_ref, send_ref):
    tokens = att_ref.shape[0]
    total = jnp.zeros((DH, DV), jnp.float32)
    for i in range(spread_ref.shape[0]):
        total = total + spread_ref[i, tokens:].astype(jnp.float32) * weight_ref[i]
    for k in range(send_ref.shape[0]):
        send_ref[k, :tokens] = att_ref[...]
        send_ref[k, tokens:] = total.astype(jnp.bfloat16)


def pass_on(spread, att, weight, count):
    return pl.pallas_call(
        pass_on_kernel,
        in_specs=[VMEM, VMEM, SMEM],
        out_shape=jax.ShapeDtypeStruct((count, *spread.shape[1:]), jnp.bfloat16),
        compiler_params=pltpu.CompilerParams(vmem_limit_bytes=6 * MIB),
        name="pass_on",
        interpret=INTERPRET,
    )(spread, att, weight)


def attend_kernel(
    where_ref, q_ref, mine_ref, other_ref, out_ref, k_ref, vt_ref, qt_ref, m_ref, l_ref, o_ref
):
    step = pl.program_id(0)
    z = where_ref[0]
    y = where_ref[1]
    keys = k_ref.shape[0]
    tokens = q_ref.shape[1]

    def prepare(key_ref, value_ref):
        for i in range(key_ref.shape[0]):
            at = slice(i * tokens, (i + 1) * tokens)
            k_ref[at] = key_ref[i, :tokens]
            vt_ref[:, at] = value_ref[i, :tokens].T

    @pl.when((step == 0) & (where_ref[2] == 0))
    def _():
        prepare(mine_ref, other_ref)

    @pl.when((step == 0) & (where_ref[2] != 0))
    def _():
        prepare(other_ref, mine_ref)

    def visit(start, count, masked):
        s = jnp.dot(k_ref[pl.ds(start, count)], qt_ref[...], preferred_element_type=jnp.float32)
        if masked:
            rows = lax.broadcasted_iota(jnp.int32, s.shape, 0) + start
            cols = lax.broadcasted_iota(jnp.int32, s.shape, 1) % tokens + y * tokens
            allowed = (rows // SEG) <= (cols // SEG)
            s = jnp.where(allowed, s, NEG)
        old = m_ref[...]
        top = jnp.maximum(old, jnp.max(s, axis=0, keepdims=True))
        w = jnp.exp(s - top)
        factor = jnp.exp(old - top)
        m_ref[...] = top
        l_ref[...] = l_ref[...] * factor + jnp.sum(w, axis=0, keepdims=True)
        o_ref[...] = o_ref[...] * factor + jnp.dot(
            vt_ref[:, pl.ds(start, count)],
            w.astype(jnp.bfloat16),
            preferred_element_type=jnp.float32,
        )

    @pl.when(step >= z)
    def _():
        q = q_ref[0]
        lane = lax.broadcasted_iota(jnp.int32, q.shape, 1)
        zero = jnp.zeros_like(q)
        q = jnp.concatenate([jnp.where(lane < DH, q, zero), jnp.where(lane < DH, zero, q)], axis=0)
        qt_ref[...] = q.T
        m_ref[...] = jnp.full(m_ref.shape, NEG, jnp.float32)
        l_ref[...] = jnp.zeros(l_ref.shape, jnp.float32)
        o_ref[...] = jnp.zeros(o_ref.shape, jnp.float32)

    @pl.when(step == z)
    def _():
        def body(i, _):
            visit(pl.multiple_of(i * KEYS, KEYS), KEYS, True)
            return 0

        lax.fori_loop(0, (y * tokens) // KEYS + 1, body, 0)

    @pl.when(step > z)
    def _():
        for start in range(0, keys, KEYS):
            visit(start, KEYS, False)

    @pl.when(step >= z)
    def _():
        total = l_ref[...]
        out_ref[0, :DV] = (o_ref[...] / total).astype(jnp.bfloat16)
        weight = m_ref[...] + jnp.log(total)
        high = weight.astype(jnp.bfloat16)
        rest = weight - high.astype(jnp.float32)
        middle = rest.astype(jnp.bfloat16)
        low = (rest - middle.astype(jnp.float32)).astype(jnp.bfloat16)
        pad = jnp.zeros((ROWS - DV - 3, weight.shape[1]), jnp.bfloat16)
        out_ref[0, DV:] = jnp.concatenate([high, middle, low, pad], axis=0)

    @pl.when(step < z)
    def _():
        out_ref[0, :DV] = jnp.zeros((DV, 2 * tokens), jnp.bfloat16)
        row = lax.broadcasted_iota(jnp.int32, (ROWS - DV, 2 * tokens), 0)
        out_ref[0, DV:] = jnp.where(row == 0, NEG, 0.0).astype(jnp.bfloat16)


def attend(where, along, mine, other, tokens):
    blocks = along.shape[0]
    count = mine.shape[0] * tokens

    def whole(shape):
        return pl.BlockSpec(shape, lambda g, w: (0,) * len(shape))

    return pl.pallas_call(
        attend_kernel,
        grid_spec=pltpu.PrefetchScalarGridSpec(
            num_scalar_prefetch=1,
            grid=(blocks,),
            in_specs=[
                pl.BlockSpec((1, tokens, 2 * DH), lambda g, w: (g, 0, 0)),
                whole(mine.shape),
                whole(other.shape),
            ],
            out_specs=pl.BlockSpec((1, ROWS, 2 * tokens), lambda g, w: (g, 0, 0)),
            scratch_shapes=[
                pltpu.VMEM((count, 2 * DH), jnp.bfloat16),
                pltpu.VMEM((DV, count), jnp.bfloat16),
                pltpu.VMEM((2 * DH, 2 * tokens), jnp.bfloat16),
                pltpu.VMEM((1, 2 * tokens), jnp.float32),
                pltpu.VMEM((1, 2 * tokens), jnp.float32),
                pltpu.VMEM((DV, 2 * tokens), jnp.float32),
            ],
        ),
        out_shape=jax.ShapeDtypeStruct((blocks, ROWS, 2 * tokens), jnp.bfloat16),
        compiler_params=pltpu.CompilerParams(
            dimension_semantics=("arbitrary",), vmem_limit_bytes=24 * MIB
        ),
        cost_estimate=pl.CostEstimate(
            flops=blocks * count * tokens * 4 * 256,
            bytes_accessed=blocks * tokens * 1024 + count * 512,
            transcendentals=blocks * count * tokens * 2,
        ),
        name="attend",
        interpret=INTERPRET,
    )(where, along, mine, other)


def finish_kernel(
    parts_ref, mix_ref, gain_ref, spread_ref, along_ref, weight_ref, query_ref, within_ref, out_ref
):
    blocks = parts_ref.shape[0]
    tokens = query_ref.shape[0]
    logs = []
    for i in range(blocks):
        rows = parts_ref[i, DV:].astype(jnp.float32)
        logs.append(rows[0:1] + rows[1:2] + rows[2:3])
    top = functools.reduce(jnp.maximum, logs)
    shares = [jnp.exp(log - top) for log in logs]
    total = functools.reduce(jnp.add, shares)
    acc = jnp.zeros((DV, 2 * tokens), jnp.float32)
    for i in range(blocks):
        acc = acc + parts_ref[i, :DV].astype(jnp.float32) * (shares[i] / total)
    att = acc[:, :tokens] - mix_ref[0] * acc[:, tokens:]
    att = att * lax.rsqrt(jnp.mean(att * att, axis=0, keepdims=True) + EPSILON)
    att = (att.T * gain_ref[0:1]).astype(jnp.bfloat16)
    carried = jnp.zeros((DH, DV), jnp.float32)
    chips = spread_ref.shape[0]
    for i in range(chips):
        carried = carried + spread_ref[i, tokens:].astype(jnp.float32) * weight_ref[i]
    for i in range(blocks):
        carried = carried + along_ref[i, tokens:].astype(jnp.float32) * weight_ref[chips + i]
    ret = within_ref[...] + rounded(query_ref[...], carried, ((1,), (0,)))
    ret = ret * lax.rsqrt(jnp.mean(ret * ret, axis=1, keepdims=True) + EPSILON)
    ret = (ret * gain_ref[1:2]).astype(jnp.bfloat16)
    half = tokens // 2
    for i in range(2):
        out_ref[i, :, :DV] = att[i * half : (i + 1) * half]
        out_ref[i, :, DV:] = ret[i * half : (i + 1) * half]


def finish(parts, mixing, gains, spread, along, weights, query, within):
    tokens = query.shape[0]
    return pl.pallas_call(
        finish_kernel,
        in_specs=[VMEM, SMEM, VMEM, VMEM, VMEM, SMEM, VMEM, VMEM],
        out_shape=jax.ShapeDtypeStruct((2, tokens // 2, 2 * DV), jnp.bfloat16),
        compiler_params=pltpu.CompilerParams(vmem_limit_bytes=8 * MIB),
        name="finish",
        interpret=INTERPRET,
    )(parts, mixing.reshape(1), gains, spread, along, weights, query, within)


def decay_log(head, length):
    pair = (head // 2).astype(jnp.float32)
    quick = jnp.log1p(-jnp.exp2(-5.0 - pair / 4.0))
    slow = jnp.log1p(-1.0 / (length * (1.0 + pair)))
    return jnp.where(head % 2 == 0, quick, slow)


def layer(
    features,
    norm_gain,
    att_query,
    att_key,
    att_value,
    att_lambda,
    att_gain,
    ret_query,
    ret_key,
    ret_value,
    ret_gain,
    out_weight,
):
    z = lax.axis_index(Z)
    y = lax.axis_index("y")
    c = lax.axis_index("c")
    x = lax.axis_index("tp")
    ny = lax.axis_size("y")
    nz = lax.axis_size(Z)
    nl = lax.axis_size("zl")
    groups = lax.axis_size("tp")
    chip = z * ny + y
    tokens = 2 * features.shape[0]

    sent = pack(2 * ny, att_query, att_key, att_value, ret_query, ret_key, ret_value)
    rows, width = sent.shape[2:]
    sent = sent.reshape(4 * ny, rows, width)
    even = jnp.arange(0, DH, 2).astype(jnp.float32)
    small = (even, jnp.arange(ny), jnp.arange(nz), chip, z, y, c, x)
    sent, small = lax.optimization_barrier((sent, small))
    w_own = lax.all_to_all(sent, ("zh", "y", "c"), 0, 0, tiled=True)
    w_own = w_own.reshape(4 * ny * rows, width)
    inputs = (features, norm_gain, att_lambda, att_gain, ret_gain)
    w_own, inputs, small = lax.optimization_barrier((w_own, inputs, small))
    features, norm_gain, att_lambda, att_gain, ret_gain = inputs
    even, ys, zs, chip, z, y, c, x = small
    weights = (w_own, *two_steps(w_own, 2 * ny * rows))
    blocks = [high * nl + (z + k) % nl for k in (0, nl - 1, 1, 2) for high in range(2)]

    pieces = [features] + [
        lax.ppermute(features, "tp", [(i, (i + k) % groups) for i in range(groups)])
        for k in range(1, groups)
    ]
    origin = jnp.stack([(x - k) % groups for k in range(groups)]).astype(jnp.int32)
    normed = norm(pieces, origin, norm_gain, nz)
    across = swapped(normed)

    log_decay = decay_log(x * 2 + c, float(nz * ny * tokens))
    positions = (chip * tokens + jnp.arange(tokens)).astype(jnp.float32)
    inverse = 10000.0 ** (-even / DH)
    angles = positions[:, None] * inverse[None, :]
    turn = jnp.stack([jnp.tile(jnp.cos(angles), (1, 4)), jnp.tile(jnp.sin(angles), (1, 4))])
    span = log_decay * tokens
    to_end = jnp.exp(span * (ny - 1 - ys).astype(jnp.float32))
    y_steps = jnp.maximum(y - 1 - ys, 0).astype(jnp.float32)
    z_steps = jnp.maximum(ny * (z - 1 - zs) + y, 0).astype(jnp.float32)
    before = jnp.concatenate(
        [
            jnp.where(ys < y, jnp.exp(span * y_steps), 0.0),
            jnp.where(zs < z, jnp.exp(span * z_steps), 0.0),
        ]
    )
    where = jnp.stack([z, y, c]).astype(jnp.int32)
    place = jnp.stack([c, *blocks]).astype(jnp.int32)
    mixing = lax.dynamic_index_in_dim(att_lambda, c, 0, keepdims=False)
    gains = jnp.stack([att_gain, ret_gain])

    normed, across, weights, turn, log_decay, to_end, before, where, place, mixing, gains = (
        lax.optimization_barrier(
            (normed, across, weights, turn, log_decay, to_end, before, where, place, mixing, gains)
        )
    )

    send, att, query, within = project(normed, across, weights, place, turn, log_decay, ny)
    spread = lax.all_to_all(send, "y", 0, 0, tiled=True)
    send = pass_on(spread, att, to_end, nz)
    along = lax.all_to_all(send, Z, 0, 0, tiled=True)
    spread, along = lax.optimization_barrier((spread, along))
    parts = attend(where, along, spread, swapped(spread), tokens)
    parts = lax.all_to_all(parts, Z, 0, 0, tiled=True)

    heads = finish(parts, mixing, gains, spread, along, before, query, within)
    heads = lax.all_to_all(heads, "c", 0, 0, tiled=True)
    joined = jnp.concatenate(
        [heads[0, :, :DV], heads[1, :, :DV], heads[0, :, DV:], heads[1, :, DV:]], axis=1
    )
    partial = jnp.dot(
        joined, out_weight.reshape(-1, out_weight.shape[2]), preferred_element_type=jnp.float32
    ).astype(jnp.bfloat16)
    partial = lax.all_to_all(
        partial.reshape(groups, -1, partial.shape[1]), "tp", 0, 0, tiled=True
    )
    return jnp.sum(partial.astype(jnp.float32), axis=0)


def solution(mesh):
    devices = mesh.devices
    torus = Mesh(devices.reshape(2, 4, -1, 2, devices.shape[-1]), SP_TP)
    return jax.shard_map(
        layer,
        mesh=torus,
        in_specs=(
            P(SP, "tp"),
            P(),
            P(SP, "tp"),
            P(SP, "tp"),
            P(SP, "tp"),
            P("tp"),
            P(),
            P(SP, "tp"),
            P(SP, "tp"),
            P(SP, "tp"),
            P(),
            P(None, "tp", None),
        ),
        out_specs=P(SP_TP, None),
        check_vma=False,
    )
```

```python
import functools

import jax
import jax.numpy as jnp
from jax import lax
from jax.experimental import pallas as pl
from jax.experimental.pallas import tpu as pltpu
from jax.sharding import Mesh
from jax.sharding import PartitionSpec as P

DH = 64
DV = 128
SEG = 64
Z = ("zh", "zl")
SP = ("zh", "zl", "y", "c")
SP_TP = ("zh", "zl", "y", "c", "tp")
EPSILON = 1e-06
NEG = -1e30
KEYS = 512
ROWS = 144
MIB = 1 << 20
VMEM = pl.BlockSpec(memory_space=pltpu.VMEM)
SMEM = pl.BlockSpec(memory_space=pltpu.SMEM)
INTERPRET = False


def swapped(value):
    return lax.ppermute(value, "c", [(0, 1), (1, 0)])


def shifted(value, step):
    count = lax.axis_size(Z)
    return lax.ppermute(value, Z, [(i, (i + step) % count) for i in range(count)])


def two_steps(own, half):
    before = shifted(own, 1)
    after = shifted(own, -1)
    low = shifted(before[:half], 1)
    high = shifted(after[half:], -1)
    return before, after, low, high


def pack_kernel(*refs):
    count = len(refs) // 2
    sources, (out_ref, wide_ref), scratch, sems = (
        refs[: count - 1],
        refs[count - 1 : count + 1],
        refs[count + 1 : -1],
        refs[-1],
    )
    copies = [
        pltpu.make_async_copy(source, buffer, sems.at[i])
        for i, (source, buffer) in enumerate(zip(sources, scratch))
    ]
    for copy in copies:
        copy.start()
    for copy in copies:
        copy.wait()
    query, key, value, rq, rk, rv, features = (buffer[...] for buffer in scratch)
    for h, whole in enumerate((key, value)):
        parts = [query, whole, rq, rk, rv]
        for k in (0, 2, 3, 4):
            width = parts[k].shape[1] // 2
            parts[k] = parts[k][:, h * width : (h + 1) * width]
        row = jnp.concatenate(parts, axis=1)
        for i in range(out_ref.shape[0]):
            out_ref[i, h] = row
    for i in range(wide_ref.shape[0]):
        wide_ref[i] = features


def pack(count, groups, *arrays):
    rows = arrays[0].shape[0]
    return pl.pallas_call(
        pack_kernel,
        in_specs=[pl.BlockSpec(memory_space=pltpu.HBM)] * len(arrays),
        out_shape=[
            jax.ShapeDtypeStruct((count, 2, rows, 512), jnp.bfloat16),
            jax.ShapeDtypeStruct((groups, *arrays[-1].shape), jnp.bfloat16),
        ],
        scratch_shapes=[pltpu.VMEM(a.shape, a.dtype) for a in arrays]
        + [pltpu.SemaphoreType.DMA((len(arrays),))],
        compiler_params=pltpu.CompilerParams(vmem_limit_bytes=4 * MIB),
        name="pack",
        interpret=INTERPRET,
    )(*(pltpu.with_memory_space_constraint(a, pltpu.HBM) for a in arrays))


def rounded(a, b, dims):
    return lax.dot_general(
        a.astype(jnp.bfloat16),
        b.astype(jnp.bfloat16),
        (dims, ((), ())),
        preferred_element_type=jnp.float32,
    )


def norm_kernel(gathered_ref, gain_ref, out_ref):
    groups = gathered_ref.shape[0]
    blocks, _, wide = out_ref.shape
    per_tp = blocks // groups
    total = 0.0
    for g in range(groups):
        floats = gathered_ref[g].astype(jnp.float32)
        total = total + jnp.sum(floats * floats, axis=1, keepdims=True)
    scale = lax.rsqrt(total / (blocks * wide) + EPSILON)
    for at in range(blocks):
        i = at % per_tp
        part = gathered_ref[at // per_tp, :, i * wide : (i + 1) * wide].astype(jnp.float32)
        out_ref[at] = (part * scale * gain_ref[at]).astype(jnp.bfloat16)


def norm(gathered, gain, blocks):
    groups, rows, width = gathered.shape
    wide = width * groups // blocks
    return pl.pallas_call(
        norm_kernel,
        in_specs=[VMEM, VMEM],
        out_shape=jax.ShapeDtypeStruct((blocks, rows, wide), jnp.bfloat16),
        compiler_params=pltpu.CompilerParams(vmem_limit_bytes=6 * MIB),
        name="norm",
        interpret=INTERPRET,
    )(gathered, gain.reshape(blocks, 1, wide))


def project_kernel(
    own_ref,
    across_ref,
    w_own_ref,
    w_before_ref,
    w_after_ref,
    w_low_ref,
    w_high_ref,
    place_ref,
    cosine_ref,
    sine_ref,
    decay_ref,
    send_ref,
    att_ref,
    query_ref,
    within_ref,
):
    half, wide = own_ref.shape[1:]
    tokens = 2 * half
    low, high = slice(0, wide), slice(wide, 2 * wide)
    weights = [(w_own_ref, low), (w_own_ref, high), (w_before_ref, low), (w_before_ref, high)]
    weights += [(w_after_ref, low), (w_after_ref, high), (w_low_ref, low), (w_high_ref, low)]
    made = jnp.zeros((tokens, w_own_ref.shape[1]), jnp.float32)
    for k, (ref, at) in enumerate(weights):
        block = place_ref[1 + k]
        left = jnp.concatenate([own_ref[block], across_ref[block]], axis=0)
        made = made + jnp.dot(left, ref[at], preferred_element_type=jnp.float32)
    first = place_ref[0] == 0
    made = jnp.concatenate(
        [jnp.where(first, made[:half], made[half:]), jnp.where(first, made[half:], made[:half])],
        axis=0,
    ).astype(jnp.bfloat16)
    att_ref[...] = made[:, : 2 * DH] * jnp.bfloat16(DH ** (-0.5))

    pair = made[:, 256:384].astype(jnp.float32)
    lane = lax.broadcasted_iota(jnp.int32, pair.shape, 1)
    quarter = DH // 2
    ahead = pltpu.roll(pair, 2 * DH - quarter, 1)
    behind = pltpu.roll(pair, quarter, 1)
    crossed = jnp.where((lane & quarter) == 0, -ahead, behind)
    cosine = jnp.concatenate([cosine_ref[...]] * 4, axis=1)
    sine = jnp.concatenate([sine_ref[...]] * 4, axis=1)
    turned = pair * cosine + crossed * sine
    query = turned[:, :DH]
    key = turned[:, DH:] * DH ** (-0.5)
    value = made[:, 384:512]
    log_decay = decay_ref[0]
    offset = lax.broadcasted_iota(jnp.int32, (tokens, 1), 0).astype(jnp.float32)
    state = rounded(key * jnp.exp(log_decay * (tokens - 1.0 - offset)), value, ((0,), (0,)))
    state = state.astype(jnp.bfloat16)
    for k in range(send_ref.shape[0]):
        send_ref[k, :tokens] = made[:, 128:256]
        send_ref[k, tokens:] = state
    i = lax.broadcasted_iota(jnp.int32, (tokens, tokens), 0)
    j = lax.broadcasted_iota(jnp.int32, (tokens, tokens), 1)
    distance = (i - j).astype(jnp.float32)
    inside = jnp.where(i >= j, jnp.exp(log_decay * jnp.maximum(distance, 0.0)), 0.0)
    scores = rounded(query, key, ((1,), (1,))) * inside
    within_ref[...] = rounded(scores, value, ((1,), (0,)))
    query_ref[...] = query * jnp.exp(log_decay * (offset + 1.0))


def project(own, across, weights, place, cosine, sine, log_decay, count):
    tokens = 2 * own.shape[1]
    return pl.pallas_call(
        project_kernel,
        in_specs=[VMEM] * 7 + [SMEM, VMEM, VMEM, SMEM],
        out_shape=[
            jax.ShapeDtypeStruct((count, tokens + DH, DV), jnp.bfloat16),
            jax.ShapeDtypeStruct((tokens, 2 * DH), jnp.bfloat16),
            jax.ShapeDtypeStruct((tokens, DH), jnp.float32),
            jax.ShapeDtypeStruct((tokens, DV), jnp.float32),
        ],
        compiler_params=pltpu.CompilerParams(vmem_limit_bytes=12 * MIB),
        name="project",
        interpret=INTERPRET,
    )(own, across, *weights, place, cosine, sine, log_decay.reshape(1))


def pass_on_kernel(spread_ref, att_ref, weight_ref, send_ref):
    tokens = att_ref.shape[0]
    total = jnp.zeros((DH, DV), jnp.float32)
    for i in range(spread_ref.shape[0]):
        total = total + spread_ref[i, tokens:].astype(jnp.float32) * weight_ref[i]
    for k in range(send_ref.shape[0]):
        send_ref[k, :tokens] = att_ref[...]
        send_ref[k, tokens:] = total.astype(jnp.bfloat16)


def pass_on(spread, att, weight, count):
    return pl.pallas_call(
        pass_on_kernel,
        in_specs=[VMEM, VMEM, SMEM],
        out_shape=jax.ShapeDtypeStruct((count, *spread.shape[1:]), jnp.bfloat16),
        compiler_params=pltpu.CompilerParams(vmem_limit_bytes=6 * MIB),
        name="pass_on",
        interpret=INTERPRET,
    )(spread, att, weight)


def attend_kernel(
    where_ref, q_ref, mine_ref, other_ref, out_ref, k_ref, vt_ref, qt_ref, m_ref, l_ref, o_ref
):
    step = pl.program_id(0)
    z = where_ref[0]
    y = where_ref[1]
    keys = k_ref.shape[0]
    tokens = q_ref.shape[1]

    def prepare(key_ref, value_ref):
        for i in range(key_ref.shape[0]):
            at = slice(i * tokens, (i + 1) * tokens)
            k_ref[at] = key_ref[i, :tokens]
            vt_ref[:, at] = value_ref[i, :tokens].T

    @pl.when((step == 0) & (where_ref[2] == 0))
    def _():
        prepare(mine_ref, other_ref)

    @pl.when((step == 0) & (where_ref[2] != 0))
    def _():
        prepare(other_ref, mine_ref)

    def visit(start, count, masked):
        s = jnp.dot(k_ref[pl.ds(start, count)], qt_ref[...], preferred_element_type=jnp.float32)
        if masked:
            rows = lax.broadcasted_iota(jnp.int32, s.shape, 0) + start
            cols = lax.broadcasted_iota(jnp.int32, s.shape, 1) % tokens + y * tokens
            allowed = (rows // SEG) <= (cols // SEG)
            s = jnp.where(allowed, s, NEG)
        old = m_ref[...]
        top = jnp.maximum(old, jnp.max(s, axis=0, keepdims=True))
        w = jnp.exp(s - top)
        factor = jnp.exp(old - top)
        m_ref[...] = top
        l_ref[...] = l_ref[...] * factor + jnp.sum(w, axis=0, keepdims=True)
        o_ref[...] = o_ref[...] * factor + jnp.dot(
            vt_ref[:, pl.ds(start, count)],
            w.astype(jnp.bfloat16),
            preferred_element_type=jnp.float32,
        )

    @pl.when(step >= z)
    def _():
        q = q_ref[0]
        lane = lax.broadcasted_iota(jnp.int32, q.shape, 1)
        zero = jnp.zeros_like(q)
        q = jnp.concatenate([jnp.where(lane < DH, q, zero), jnp.where(lane < DH, zero, q)], axis=0)
        qt_ref[...] = q.T
        m_ref[...] = jnp.full(m_ref.shape, NEG, jnp.float32)
        l_ref[...] = jnp.zeros(l_ref.shape, jnp.float32)
        o_ref[...] = jnp.zeros(o_ref.shape, jnp.float32)

    @pl.when(step == z)
    def _():
        def body(i, _):
            visit(pl.multiple_of(i * KEYS, KEYS), KEYS, True)
            return 0

        lax.fori_loop(0, (y * tokens) // KEYS + 1, body, 0)

    @pl.when(step > z)
    def _():
        for start in range(0, keys, KEYS):
            visit(start, KEYS, False)

    @pl.when(step >= z)
    def _():
        total = l_ref[...]
        out_ref[0, :DV] = (o_ref[...] / total).astype(jnp.bfloat16)
        weight = m_ref[...] + jnp.log(total)
        high = weight.astype(jnp.bfloat16)
        rest = weight - high.astype(jnp.float32)
        middle = rest.astype(jnp.bfloat16)
        low = (rest - middle.astype(jnp.float32)).astype(jnp.bfloat16)
        pad = jnp.zeros((ROWS - DV - 3, weight.shape[1]), jnp.bfloat16)
        out_ref[0, DV:] = jnp.concatenate([high, middle, low, pad], axis=0)

    @pl.when(step < z)
    def _():
        out_ref[0, :DV] = jnp.zeros((DV, 2 * tokens), jnp.bfloat16)
        row = lax.broadcasted_iota(jnp.int32, (ROWS - DV, 2 * tokens), 0)
        out_ref[0, DV:] = jnp.where(row == 0, NEG, 0.0).astype(jnp.bfloat16)


def attend(where, along, mine, other, tokens):
    blocks = along.shape[0]
    count = mine.shape[0] * tokens

    def whole(shape):
        return pl.BlockSpec(shape, lambda g, w: (0,) * len(shape))

    return pl.pallas_call(
        attend_kernel,
        grid_spec=pltpu.PrefetchScalarGridSpec(
            num_scalar_prefetch=1,
            grid=(blocks,),
            in_specs=[
                pl.BlockSpec((1, tokens, 2 * DH), lambda g, w: (g, 0, 0)),
                whole(mine.shape),
                whole(other.shape),
            ],
            out_specs=pl.BlockSpec((1, ROWS, 2 * tokens), lambda g, w: (g, 0, 0)),
            scratch_shapes=[
                pltpu.VMEM((count, 2 * DH), jnp.bfloat16),
                pltpu.VMEM((DV, count), jnp.bfloat16),
                pltpu.VMEM((2 * DH, 2 * tokens), jnp.bfloat16),
                pltpu.VMEM((1, 2 * tokens), jnp.float32),
                pltpu.VMEM((1, 2 * tokens), jnp.float32),
                pltpu.VMEM((DV, 2 * tokens), jnp.float32),
            ],
        ),
        out_shape=jax.ShapeDtypeStruct((blocks, ROWS, 2 * tokens), jnp.bfloat16),
        compiler_params=pltpu.CompilerParams(
            dimension_semantics=("arbitrary",), vmem_limit_bytes=24 * MIB
        ),
        cost_estimate=pl.CostEstimate(
            flops=blocks * count * tokens * 4 * 256,
            bytes_accessed=blocks * tokens * 1024 + count * 512,
            transcendentals=blocks * count * tokens * 2,
        ),
        name="attend",
        interpret=INTERPRET,
    )(where, along, mine, other)


def finish_kernel(
    parts_ref, mix_ref, gain_ref, spread_ref, along_ref, weight_ref, query_ref, within_ref, out_ref
):
    blocks = parts_ref.shape[0]
    tokens = query_ref.shape[0]
    logs = []
    for i in range(blocks):
        rows = parts_ref[i, DV:].astype(jnp.float32)
        logs.append(rows[0:1] + rows[1:2] + rows[2:3])
    top = functools.reduce(jnp.maximum, logs)
    shares = [jnp.exp(log - top) for log in logs]
    total = functools.reduce(jnp.add, shares)
    acc = jnp.zeros((DV, 2 * tokens), jnp.float32)
    for i in range(blocks):
        acc = acc + parts_ref[i, :DV].astype(jnp.float32) * (shares[i] / total)
    att = acc[:, :tokens] - mix_ref[0] * acc[:, tokens:]
    att = att * lax.rsqrt(jnp.mean(att * att, axis=0, keepdims=True) + EPSILON)
    att = (att.T * gain_ref[0:1]).astype(jnp.bfloat16)
    carried = jnp.zeros((DH, DV), jnp.float32)
    chips = spread_ref.shape[0]
    for i in range(chips):
        carried = carried + spread_ref[i, tokens:].astype(jnp.float32) * weight_ref[i]
    for i in range(blocks):
        carried = carried + along_ref[i, tokens:].astype(jnp.float32) * weight_ref[chips + i]
    ret = within_ref[...] + rounded(query_ref[...], carried, ((1,), (0,)))
    ret = ret * lax.rsqrt(jnp.mean(ret * ret, axis=1, keepdims=True) + EPSILON)
    ret = (ret * gain_ref[1:2]).astype(jnp.bfloat16)
    half = tokens // 2
    for i in range(2):
        out_ref[i, :, :DV] = att[i * half : (i + 1) * half]
        out_ref[i, :, DV:] = ret[i * half : (i + 1) * half]


def finish(parts, mixing, gains, spread, along, weights, query, within):
    tokens = query.shape[0]
    return pl.pallas_call(
        finish_kernel,
        in_specs=[VMEM, SMEM, VMEM, VMEM, VMEM, SMEM, VMEM, VMEM],
        out_shape=jax.ShapeDtypeStruct((2, tokens // 2, 2 * DV), jnp.bfloat16),
        compiler_params=pltpu.CompilerParams(vmem_limit_bytes=8 * MIB),
        name="finish",
        interpret=INTERPRET,
    )(parts, mixing.reshape(1), gains, spread, along, weights, query, within)


def decay_log(head, length):
    pair = (head // 2).astype(jnp.float32)
    quick = jnp.log1p(-jnp.exp2(-5.0 - pair / 4.0))
    slow = jnp.log1p(-1.0 / (length * (1.0 + pair)))
    return jnp.where(head % 2 == 0, quick, slow)


def layer(
    features,
    norm_gain,
    att_query,
    att_key,
    att_value,
    att_lambda,
    att_gain,
    ret_query,
    ret_key,
    ret_value,
    ret_gain,
    out_weight,
):
    z = lax.axis_index(Z)
    y = lax.axis_index("y")
    c = lax.axis_index("c")
    x = lax.axis_index("tp")
    ny = lax.axis_size("y")
    nz = lax.axis_size(Z)
    nl = lax.axis_size("zl")
    groups = lax.axis_size("tp")
    chip = z * ny + y
    tokens = 2 * features.shape[0]

    matrices = (att_query, att_key, att_value, ret_query, ret_key, ret_value)
    sent, features = pack(2 * ny, groups, *matrices, features)
    rows, width = sent.shape[2:]
    sent = sent.reshape(4 * ny, rows, width)
    even = jnp.arange(0, DH, 2).astype(jnp.float32)
    small = (even, jnp.arange(ny), jnp.arange(nz), chip, z, y, c, x)
    sent, small = lax.optimization_barrier((sent, small))
    w_own = lax.all_to_all(sent, ("zh", "y", "c"), 0, 0, tiled=True)
    w_own = w_own.reshape(4 * ny * rows, width)
    inputs = (features, norm_gain, att_lambda, att_gain, ret_gain)
    w_own, inputs, small = lax.optimization_barrier((w_own, inputs, small))
    features, norm_gain, att_lambda, att_gain, ret_gain = inputs
    even, ys, zs, chip, z, y, c, x = small
    weights = (w_own, *two_steps(w_own, 2 * ny * rows))
    blocks = [high * nl + (z + k) % nl for k in (0, nl - 1, 1, 2) for high in range(2)]

    gathered = lax.all_to_all(features, "tp", 0, 0, tiled=True)
    normed = norm(gathered, norm_gain, nz)
    across = swapped(normed)

    log_decay = decay_log(x * 2 + c, float(nz * ny * tokens))
    positions = (chip * tokens + jnp.arange(tokens)).astype(jnp.float32)
    inverse = 10000.0 ** (-even / DH)
    angles = positions[:, None] * inverse[None, :]
    cosine, sine = jnp.cos(angles), jnp.sin(angles)
    span = log_decay * tokens
    to_end = jnp.exp(span * (ny - 1 - ys).astype(jnp.float32))
    y_steps = jnp.maximum(y - 1 - ys, 0).astype(jnp.float32)
    z_steps = jnp.maximum(ny * (z - 1 - zs) + y, 0).astype(jnp.float32)
    before = jnp.concatenate(
        [
            jnp.where(ys < y, jnp.exp(span * y_steps), 0.0),
            jnp.where(zs < z, jnp.exp(span * z_steps), 0.0),
        ]
    )
    where = jnp.stack([z, y, c]).astype(jnp.int32)
    place = jnp.stack([c, *blocks]).astype(jnp.int32)
    mixing = lax.dynamic_index_in_dim(att_lambda, c, 0, keepdims=False)
    gains = jnp.stack([att_gain, ret_gain])

    tables = (cosine, sine, log_decay, to_end, before, where, place, mixing, gains)
    normed, across, weights, tables = lax.optimization_barrier((normed, across, weights, tables))
    cosine, sine, log_decay, to_end, before, where, place, mixing, gains = tables

    send, att, query, within = project(
        normed, across, weights, place, cosine, sine, log_decay, ny
    )
    spread = lax.all_to_all(send, "y", 0, 0, tiled=True)
    send = pass_on(spread, att, to_end, nz)
    along = lax.all_to_all(send, Z, 0, 0, tiled=True)
    spread, along = lax.optimization_barrier((spread, along))
    parts = attend(where, along, spread, swapped(spread), tokens)
    parts = lax.all_to_all(parts, Z, 0, 0, tiled=True)

    heads = finish(parts, mixing, gains, spread, along, before, query, within)
    heads = lax.all_to_all(heads, "c", 0, 0, tiled=True)
    joined = jnp.concatenate(
        [heads[0, :, :DV], heads[1, :, :DV], heads[0, :, DV:], heads[1, :, DV:]], axis=1
    )
    partial = jnp.dot(
        joined, out_weight.reshape(-1, out_weight.shape[2]), preferred_element_type=jnp.float32
    ).astype(jnp.bfloat16)
    partial = lax.all_to_all(
        partial.reshape(groups, -1, partial.shape[1]), "tp", 0, 0, tiled=True
    )
    return jnp.sum(partial.astype(jnp.float32), axis=0)


def solution(mesh):
    devices = mesh.devices
    torus = Mesh(devices.reshape(2, 4, -1, 2, devices.shape[-1]), SP_TP)
    return jax.shard_map(
        layer,
        mesh=torus,
        in_specs=(
            P(SP, "tp"),
            P(),
            P(SP, "tp"),
            P(SP, "tp"),
            P(SP, "tp"),
            P("tp"),
            P(),
            P(SP, "tp"),
            P(SP, "tp"),
            P(SP, "tp"),
            P(),
            P(None, "tp", None),
        ),
        out_specs=P(SP_TP, None),
        check_vma=False,
    )
```

```python
import functools

import jax
import jax.numpy as jnp
from jax import lax
from jax.experimental import pallas as pl
from jax.experimental.pallas import tpu as pltpu
from jax.sharding import Mesh
from jax.sharding import PartitionSpec as P

DH = 64
DV = 128
SEG = 64
Z = ("zh", "zl")
SP = ("zh", "zl", "y", "c")
SP_TP = ("zh", "zl", "y", "c", "tp")
EPSILON = 1e-06
NEG = -1e30
KEYS = 512
ROWS = 144
MIB = 1 << 20
VMEM = pl.BlockSpec(memory_space=pltpu.VMEM)
SMEM = pl.BlockSpec(memory_space=pltpu.SMEM)
INTERPRET = False


def swapped(value):
    return lax.ppermute(value, "c", [(0, 1), (1, 0)])


def shifted(value, step):
    count = lax.axis_size(Z)
    return lax.ppermute(value, Z, [(i, (i + step) % count) for i in range(count)])


def around(own, half):
    before = shifted(own, 1)
    after = shifted(own, -1)
    low = shifted(own[:half], 2)
    high = shifted(own[half:], -2)
    return before, after, low, high


def pack_kernel(*refs):
    count = len(refs) // 2
    sources, (out_ref, wide_ref), scratch, sems = (
        refs[: count - 1],
        refs[count - 1 : count + 1],
        refs[count + 1 : -1],
        refs[-1],
    )
    copies = [
        pltpu.make_async_copy(source, buffer, sems.at[i])
        for i, (source, buffer) in enumerate(zip(sources, scratch))
    ]
    for copy in copies:
        copy.start()
    for copy in copies:
        copy.wait()
    query, key, value, rq, rk, rv, features = (buffer[...] for buffer in scratch)
    for h, whole in enumerate((key, value)):
        parts = [query, whole, rq, rk, rv]
        for k in (0, 2, 3, 4):
            width = parts[k].shape[1] // 2
            parts[k] = parts[k][:, h * width : (h + 1) * width]
        row = jnp.concatenate(parts, axis=1)
        for i in range(out_ref.shape[0]):
            out_ref[i, h] = row
    for i in range(wide_ref.shape[0]):
        wide_ref[i] = features


def pack(count, groups, *arrays):
    rows = arrays[0].shape[0]
    return pl.pallas_call(
        pack_kernel,
        in_specs=[pl.BlockSpec(memory_space=pltpu.HBM)] * len(arrays),
        out_shape=[
            jax.ShapeDtypeStruct((count, 2, rows, 512), jnp.bfloat16),
            jax.ShapeDtypeStruct((groups, *arrays[-1].shape), jnp.bfloat16),
        ],
        scratch_shapes=[pltpu.VMEM(a.shape, a.dtype) for a in arrays]
        + [pltpu.SemaphoreType.DMA((len(arrays),))],
        compiler_params=pltpu.CompilerParams(vmem_limit_bytes=4 * MIB),
        name="pack",
        interpret=INTERPRET,
    )(*(pltpu.with_memory_space_constraint(a, pltpu.HBM) for a in arrays))


def rounded(a, b, dims):
    return lax.dot_general(
        a.astype(jnp.bfloat16),
        b.astype(jnp.bfloat16),
        (dims, ((), ())),
        preferred_element_type=jnp.float32,
    )


def norm_kernel(gathered_ref, gain_ref, out_ref):
    groups = gathered_ref.shape[0]
    blocks, _, wide = out_ref.shape
    per_tp = blocks // groups
    total = 0.0
    for g in range(groups):
        floats = gathered_ref[g].astype(jnp.float32)
        total = total + jnp.sum(floats * floats, axis=1, keepdims=True)
    scale = lax.rsqrt(total / (blocks * wide) + EPSILON)
    for at in range(blocks):
        i = at % per_tp
        part = gathered_ref[at // per_tp, :, i * wide : (i + 1) * wide].astype(jnp.float32)
        out_ref[at] = (part * scale * gain_ref[at]).astype(jnp.bfloat16)


def norm(gathered, gain, blocks):
    groups, rows, width = gathered.shape
    wide = width * groups // blocks
    return pl.pallas_call(
        norm_kernel,
        in_specs=[VMEM, VMEM],
        out_shape=jax.ShapeDtypeStruct((blocks, rows, wide), jnp.bfloat16),
        compiler_params=pltpu.CompilerParams(vmem_limit_bytes=6 * MIB),
        name="norm",
        interpret=INTERPRET,
    )(gathered, gain.reshape(blocks, 1, wide))


def project_kernel(
    own_ref,
    across_ref,
    w_own_ref,
    w_before_ref,
    w_after_ref,
    w_low_ref,
    w_high_ref,
    place_ref,
    cosine_ref,
    sine_ref,
    decay_ref,
    send_ref,
    att_ref,
    query_ref,
    within_ref,
):
    half, wide = own_ref.shape[1:]
    tokens = 2 * half
    low, high = slice(0, wide), slice(wide, 2 * wide)
    weights = [(w_own_ref, low), (w_own_ref, high), (w_before_ref, low), (w_before_ref, high)]
    weights += [(w_after_ref, low), (w_after_ref, high), (w_low_ref, low), (w_high_ref, low)]
    made = jnp.zeros((tokens, w_own_ref.shape[1]), jnp.float32)
    for k, (ref, at) in enumerate(weights):
        block = place_ref[1 + k]
        left = jnp.concatenate([own_ref[block], across_ref[block]], axis=0)
        made = made + jnp.dot(left, ref[at], preferred_element_type=jnp.float32)
    first = place_ref[0] == 0
    made = jnp.concatenate(
        [jnp.where(first, made[:half], made[half:]), jnp.where(first, made[half:], made[:half])],
        axis=0,
    ).astype(jnp.bfloat16)
    att_ref[...] = made[:, : 2 * DH] * jnp.bfloat16(DH ** (-0.5))

    pair = made[:, 256:384].astype(jnp.float32)
    lane = lax.broadcasted_iota(jnp.int32, pair.shape, 1)
    quarter = DH // 2
    ahead = pltpu.roll(pair, 2 * DH - quarter, 1)
    behind = pltpu.roll(pair, quarter, 1)
    crossed = jnp.where((lane & quarter) == 0, -ahead, behind)
    cosine = jnp.concatenate([cosine_ref[...]] * 4, axis=1)
    sine = jnp.concatenate([sine_ref[...]] * 4, axis=1)
    turned = pair * cosine + crossed * sine
    query = turned[:, :DH]
    key = turned[:, DH:] * DH ** (-0.5)
    value = made[:, 384:512]
    log_decay = decay_ref[0]
    offset = lax.broadcasted_iota(jnp.int32, (tokens, 1), 0).astype(jnp.float32)
    state = rounded(key * jnp.exp(log_decay * (tokens - 1.0 - offset)), value, ((0,), (0,)))
    state = state.astype(jnp.bfloat16)
    for k in range(send_ref.shape[0]):
        send_ref[k, :tokens] = made[:, 128:256]
        send_ref[k, tokens:] = state
    i = lax.broadcasted_iota(jnp.int32, (tokens, tokens), 0)
    j = lax.broadcasted_iota(jnp.int32, (tokens, tokens), 1)
    distance = (i - j).astype(jnp.float32)
    inside = jnp.where(i >= j, jnp.exp(log_decay * jnp.maximum(distance, 0.0)), 0.0)
    scores = rounded(query, key, ((1,), (1,))) * inside
    within_ref[...] = rounded(scores, value, ((1,), (0,)))
    query_ref[...] = query * jnp.exp(log_decay * (offset + 1.0))


def project(own, across, weights, place, cosine, sine, log_decay, count):
    tokens = 2 * own.shape[1]
    return pl.pallas_call(
        project_kernel,
        in_specs=[VMEM] * 7 + [SMEM, VMEM, VMEM, SMEM],
        out_shape=[
            jax.ShapeDtypeStruct((count, tokens + DH, DV), jnp.bfloat16),
            jax.ShapeDtypeStruct((tokens, 2 * DH), jnp.bfloat16),
            jax.ShapeDtypeStruct((tokens, DH), jnp.float32),
            jax.ShapeDtypeStruct((tokens, DV), jnp.float32),
        ],
        compiler_params=pltpu.CompilerParams(vmem_limit_bytes=12 * MIB),
        name="project",
        interpret=INTERPRET,
    )(own, across, *weights, place, cosine, sine, log_decay.reshape(1))


def pass_on_kernel(spread_ref, att_ref, weight_ref, send_ref):
    tokens = att_ref.shape[0]
    total = jnp.zeros((DH, DV), jnp.float32)
    for i in range(spread_ref.shape[0]):
        total = total + spread_ref[i, tokens:].astype(jnp.float32) * weight_ref[i]
    for k in range(send_ref.shape[0]):
        send_ref[k, :tokens] = att_ref[...]
        send_ref[k, tokens:] = total.astype(jnp.bfloat16)


def pass_on(spread, att, weight, count):
    return pl.pallas_call(
        pass_on_kernel,
        in_specs=[VMEM, VMEM, SMEM],
        out_shape=jax.ShapeDtypeStruct((count, *spread.shape[1:]), jnp.bfloat16),
        compiler_params=pltpu.CompilerParams(vmem_limit_bytes=6 * MIB),
        name="pass_on",
        interpret=INTERPRET,
    )(spread, att, weight)


def attend_kernel(
    where_ref, q_ref, mine_ref, other_ref, out_ref, k_ref, vt_ref, qt_ref, m_ref, l_ref, o_ref
):
    step = pl.program_id(0)
    z = where_ref[0]
    y = where_ref[1]
    keys = k_ref.shape[0]
    tokens = q_ref.shape[1]

    def prepare(key_ref, value_ref):
        for i in range(key_ref.shape[0]):
            at = slice(i * tokens, (i + 1) * tokens)
            k_ref[at] = key_ref[i, :tokens]
            vt_ref[:, at] = value_ref[i, :tokens].T

    @pl.when((step == 0) & (where_ref[2] == 0))
    def _():
        prepare(mine_ref, other_ref)

    @pl.when((step == 0) & (where_ref[2] != 0))
    def _():
        prepare(other_ref, mine_ref)

    def visit(start, count, masked):
        s = jnp.dot(k_ref[pl.ds(start, count)], qt_ref[...], preferred_element_type=jnp.float32)
        if masked:
            rows = lax.broadcasted_iota(jnp.int32, s.shape, 0) + start
            cols = lax.broadcasted_iota(jnp.int32, s.shape, 1) % tokens + y * tokens
            allowed = (rows // SEG) <= (cols // SEG)
            s = jnp.where(allowed, s, NEG)
        old = m_ref[...]
        top = jnp.maximum(old, jnp.max(s, axis=0, keepdims=True))
        w = jnp.exp(s - top)
        factor = jnp.exp(old - top)
        m_ref[...] = top
        l_ref[...] = l_ref[...] * factor + jnp.sum(w, axis=0, keepdims=True)
        o_ref[...] = o_ref[...] * factor + jnp.dot(
            vt_ref[:, pl.ds(start, count)],
            w.astype(jnp.bfloat16),
            preferred_element_type=jnp.float32,
        )

    @pl.when(step >= 0)
    def _():
        q = q_ref[0]
        lane = lax.broadcasted_iota(jnp.int32, q.shape, 1)
        zero = jnp.zeros_like(q)
        q = jnp.concatenate([jnp.where(lane < DH, q, zero), jnp.where(lane < DH, zero, q)], axis=0)
        qt_ref[...] = q.T
        m_ref[...] = jnp.full(m_ref.shape, NEG, jnp.float32)
        l_ref[...] = jnp.zeros(l_ref.shape, jnp.float32)
        o_ref[...] = jnp.zeros(o_ref.shape, jnp.float32)

    @pl.when(step == z)
    def _():
        def body(i, _):
            visit(pl.multiple_of(i * KEYS, KEYS), KEYS, True)
            return 0

        lax.fori_loop(0, (y * tokens) // KEYS + 1, body, 0)

    @pl.when(step != z)
    def _():
        for start in range(0, keys, KEYS):
            visit(start, KEYS, False)

    @pl.when(step >= z)
    def _():
        total = l_ref[...]
        out_ref[0, :DV] = (o_ref[...] / total).astype(jnp.bfloat16)
        weight = m_ref[...] + jnp.log(total)
        high = weight.astype(jnp.bfloat16)
        rest = weight - high.astype(jnp.float32)
        middle = rest.astype(jnp.bfloat16)
        low = (rest - middle.astype(jnp.float32)).astype(jnp.bfloat16)
        pad = jnp.zeros((ROWS - DV - 3, weight.shape[1]), jnp.bfloat16)
        out_ref[0, DV:] = jnp.concatenate([high, middle, low, pad], axis=0)

    @pl.when(step < z)
    def _():
        out_ref[0, :DV] = jnp.zeros((DV, 2 * tokens), jnp.bfloat16)
        row = lax.broadcasted_iota(jnp.int32, (ROWS - DV, 2 * tokens), 0)
        out_ref[0, DV:] = jnp.where(row == 0, NEG, 0.0).astype(jnp.bfloat16)


def attend(where, along, mine, other, tokens):
    blocks = along.shape[0]
    count = mine.shape[0] * tokens

    def whole(shape):
        return pl.BlockSpec(shape, lambda g, w: (0,) * len(shape))

    return pl.pallas_call(
        attend_kernel,
        grid_spec=pltpu.PrefetchScalarGridSpec(
            num_scalar_prefetch=1,
            grid=(blocks,),
            in_specs=[
                pl.BlockSpec((1, tokens, 2 * DH), lambda g, w: (g, 0, 0)),
                whole(mine.shape),
                whole(other.shape),
            ],
            out_specs=pl.BlockSpec((1, ROWS, 2 * tokens), lambda g, w: (g, 0, 0)),
            scratch_shapes=[
                pltpu.VMEM((count, 2 * DH), jnp.bfloat16),
                pltpu.VMEM((DV, count), jnp.bfloat16),
                pltpu.VMEM((2 * DH, 2 * tokens), jnp.bfloat16),
                pltpu.VMEM((1, 2 * tokens), jnp.float32),
                pltpu.VMEM((1, 2 * tokens), jnp.float32),
                pltpu.VMEM((DV, 2 * tokens), jnp.float32),
            ],
        ),
        out_shape=jax.ShapeDtypeStruct((blocks, ROWS, 2 * tokens), jnp.bfloat16),
        compiler_params=pltpu.CompilerParams(
            dimension_semantics=("arbitrary",), vmem_limit_bytes=24 * MIB
        ),
        cost_estimate=pl.CostEstimate(
            flops=blocks * count * tokens * 4 * 256,
            bytes_accessed=blocks * tokens * 1024 + count * 512,
            transcendentals=blocks * count * tokens * 2,
        ),
        name="attend",
        interpret=INTERPRET,
    )(where, along, mine, other)


def finish_kernel(
    parts_ref, mix_ref, gain_ref, spread_ref, along_ref, weight_ref, query_ref, within_ref, out_ref
):
    blocks = parts_ref.shape[0]
    tokens = query_ref.shape[0]
    logs = []
    for i in range(blocks):
        rows = parts_ref[i, DV:].astype(jnp.float32)
        logs.append(rows[0:1] + rows[1:2] + rows[2:3])
    top = functools.reduce(jnp.maximum, logs)
    shares = [jnp.exp(log - top) for log in logs]
    total = functools.reduce(jnp.add, shares)
    acc = jnp.zeros((DV, 2 * tokens), jnp.float32)
    for i in range(blocks):
        acc = acc + parts_ref[i, :DV].astype(jnp.float32) * (shares[i] / total)
    att = acc[:, :tokens] - mix_ref[0] * acc[:, tokens:]
    att = att * lax.rsqrt(jnp.mean(att * att, axis=0, keepdims=True) + EPSILON)
    att = (att.T * gain_ref[0:1]).astype(jnp.bfloat16)
    carried = jnp.zeros((DH, DV), jnp.float32)
    chips = spread_ref.shape[0]
    for i in range(chips):
        carried = carried + spread_ref[i, tokens:].astype(jnp.float32) * weight_ref[i]
    for i in range(blocks):
        carried = carried + along_ref[i, tokens:].astype(jnp.float32) * weight_ref[chips + i]
    ret = within_ref[...] + rounded(query_ref[...], carried, ((1,), (0,)))
    ret = ret * lax.rsqrt(jnp.mean(ret * ret, axis=1, keepdims=True) + EPSILON)
    ret = (ret * gain_ref[1:2]).astype(jnp.bfloat16)
    half = tokens // 2
    for i in range(2):
        out_ref[i, :, :DV] = att[i * half : (i + 1) * half]
        out_ref[i, :, DV:] = ret[i * half : (i + 1) * half]


def finish(parts, mixing, gains, spread, along, weights, query, within):
    tokens = query.shape[0]
    return pl.pallas_call(
        finish_kernel,
        in_specs=[VMEM, SMEM, VMEM, VMEM, VMEM, SMEM, VMEM, VMEM],
        out_shape=jax.ShapeDtypeStruct((2, tokens // 2, 2 * DV), jnp.bfloat16),
        compiler_params=pltpu.CompilerParams(vmem_limit_bytes=8 * MIB),
        name="finish",
        interpret=INTERPRET,
    )(parts, mixing.reshape(1), gains, spread, along, weights, query, within)


def decay_log(head, length):
    pair = (head // 2).astype(jnp.float32)
    quick = jnp.log1p(-jnp.exp2(-5.0 - pair / 4.0))
    slow = jnp.log1p(-1.0 / (length * (1.0 + pair)))
    return jnp.where(head % 2 == 0, quick, slow)


def layer(
    features,
    norm_gain,
    att_query,
    att_key,
    att_value,
    att_lambda,
    att_gain,
    ret_query,
    ret_key,
    ret_value,
    ret_gain,
    out_weight,
):
    z = lax.axis_index(Z)
    y = lax.axis_index("y")
    c = lax.axis_index("c")
    x = lax.axis_index("tp")
    ny = lax.axis_size("y")
    nz = lax.axis_size(Z)
    nl = lax.axis_size("zl")
    groups = lax.axis_size("tp")
    chip = z * ny + y
    tokens = 2 * features.shape[0]

    matrices = (att_query, att_key, att_value, ret_query, ret_key, ret_value)
    sent, features = pack(2 * ny, groups, *matrices, features)
    rows, width = sent.shape[2:]
    sent = sent.reshape(4 * ny, rows, width)
    even = jnp.arange(0, DH, 2).astype(jnp.float32)
    small = (even, jnp.arange(ny), jnp.arange(nz), chip, z, y, c, x)
    sent, small = lax.optimization_barrier((sent, small))
    w_own = lax.all_to_all(sent, ("zh", "y", "c"), 0, 0, tiled=True)
    w_own = w_own.reshape(4 * ny * rows, width)
    inputs = (features, norm_gain, att_lambda, att_gain, ret_gain)
    w_own, inputs, small = lax.optimization_barrier((w_own, inputs, small))
    features, norm_gain, att_lambda, att_gain, ret_gain = inputs
    even, ys, zs, chip, z, y, c, x = small
    weights = (w_own, *around(w_own, 2 * ny * rows))
    blocks = [high * nl + (z + k) % nl for k in (0, nl - 1, 1, 2) for high in range(2)]

    gathered = lax.all_to_all(features, "tp", 0, 0, tiled=True)
    normed = norm(gathered, norm_gain, nz)
    across = swapped(normed)

    log_decay = decay_log(x * 2 + c, float(nz * ny * tokens))
    positions = (chip * tokens + jnp.arange(tokens)).astype(jnp.float32)
    inverse = 10000.0 ** (-even / DH)
    angles = positions[:, None] * inverse[None, :]
    cosine, sine = jnp.cos(angles), jnp.sin(angles)
    span = log_decay * tokens
    to_end = jnp.exp(span * (ny - 1 - ys).astype(jnp.float32))
    y_steps = jnp.maximum(y - 1 - ys, 0).astype(jnp.float32)
    z_steps = jnp.maximum(ny * (z - 1 - zs) + y, 0).astype(jnp.float32)
    before = jnp.concatenate(
        [
            jnp.where(ys < y, jnp.exp(span * y_steps), 0.0),
            jnp.where(zs < z, jnp.exp(span * z_steps), 0.0),
        ]
    )
    where = jnp.stack([z, y, c]).astype(jnp.int32)
    place = jnp.stack([c, *blocks]).astype(jnp.int32)
    mixing = lax.dynamic_index_in_dim(att_lambda, c, 0, keepdims=False)
    gains = jnp.stack([att_gain, ret_gain])

    tables = (cosine, sine, log_decay, to_end, before, where, place, mixing, gains)
    normed, across, weights, tables = lax.optimization_barrier((normed, across, weights, tables))
    cosine, sine, log_decay, to_end, before, where, place, mixing, gains = tables

    send, att, query, within = project(
        normed, across, weights, place, cosine, sine, log_decay, ny
    )
    spread = lax.all_to_all(send, "y", 0, 0, tiled=True)
    send = pass_on(spread, att, to_end, nz)
    along = lax.all_to_all(send, Z, 0, 0, tiled=True)
    spread, along = lax.optimization_barrier((spread, along))
    parts = attend(where, along, spread, swapped(spread), tokens)
    parts = lax.all_to_all(parts, Z, 0, 0, tiled=True)

    heads = finish(parts, mixing, gains, spread, along, before, query, within)
    heads = lax.all_to_all(heads, "c", 0, 0, tiled=True)
    joined = jnp.concatenate(
        [heads[0, :, :DV], heads[1, :, :DV], heads[0, :, DV:], heads[1, :, DV:]], axis=1
    )
    partial = jnp.dot(
        joined, out_weight.reshape(-1, out_weight.shape[2]), preferred_element_type=jnp.float32
    ).astype(jnp.bfloat16)
    partial = lax.all_to_all(
        partial.reshape(groups, -1, partial.shape[1]), "tp", 0, 0, tiled=True
    )
    return jnp.sum(partial.astype(jnp.float32), axis=0)


def solution(mesh):
    devices = mesh.devices
    torus = Mesh(devices.reshape(2, 4, -1, 2, devices.shape[-1]), SP_TP)
    return jax.shard_map(
        layer,
        mesh=torus,
        in_specs=(
            P(SP, "tp"),
            P(),
            P(SP, "tp"),
            P(SP, "tp"),
            P(SP, "tp"),
            P("tp"),
            P(),
            P(SP, "tp"),
            P(SP, "tp"),
            P(SP, "tp"),
            P(),
            P(None, "tp", None),
        ),
        out_specs=P(SP_TP, None),
        check_vma=False,
    )
```

```python
import functools

import jax
import jax.numpy as jnp
from jax import lax
from jax.experimental import pallas as pl
from jax.experimental.pallas import tpu as pltpu
from jax.sharding import Mesh
from jax.sharding import PartitionSpec as P

DH = 64
DV = 128
SEG = 64
Z = ("zh", "zl")
SP = ("zh", "zl", "y", "c")
SP_TP = ("zh", "zl", "y", "c", "tp")
EPSILON = 1e-06
NEG = -1e30
KEYS = 512
ROWS = 144
MIB = 1 << 20
VMEM = pl.BlockSpec(memory_space=pltpu.VMEM)
SMEM = pl.BlockSpec(memory_space=pltpu.SMEM)
INTERPRET = False


def swapped(value):
    return lax.ppermute(value, "c", [(0, 1), (1, 0)])


def shifted(value, step):
    count = lax.axis_size(Z)
    return lax.ppermute(value, Z, [(i, (i + step) % count) for i in range(count)])


def around(own, half):
    before = shifted(own, 1)
    after = shifted(own, -1)
    low = shifted(own[:half], 2)
    high = shifted(own[half:], -2)
    return before, after, low, high


def pack_kernel(*refs):
    count = len(refs) // 2
    sources, (out_ref, wide_ref), scratch, sems = (
        refs[: count - 1],
        refs[count - 1 : count + 1],
        refs[count + 1 : -1],
        refs[-1],
    )
    copies = [
        pltpu.make_async_copy(source, buffer, sems.at[i])
        for i, (source, buffer) in enumerate(zip(sources, scratch))
    ]
    for copy in copies:
        copy.start()
    for copy in copies:
        copy.wait()
    query, key, value, rq, rk, rv, features = (buffer[...] for buffer in scratch)
    for h, whole in enumerate((key, value)):
        parts = [query, whole, rq, rk, rv]
        for k in (0, 2, 3, 4):
            width = parts[k].shape[1] // 2
            parts[k] = parts[k][:, h * width : (h + 1) * width]
        row = jnp.concatenate(parts, axis=1)
        for i in range(out_ref.shape[0]):
            out_ref[i, h] = row
    for i in range(wide_ref.shape[0]):
        wide_ref[i] = features


def pack(count, groups, *arrays):
    rows = arrays[0].shape[0]
    return pl.pallas_call(
        pack_kernel,
        in_specs=[pl.BlockSpec(memory_space=pltpu.HBM)] * len(arrays),
        out_shape=[
            jax.ShapeDtypeStruct((count, 2, rows, 512), jnp.bfloat16),
            jax.ShapeDtypeStruct((groups, *arrays[-1].shape), jnp.bfloat16),
        ],
        scratch_shapes=[pltpu.VMEM(a.shape, a.dtype) for a in arrays]
        + [pltpu.SemaphoreType.DMA((len(arrays),))],
        compiler_params=pltpu.CompilerParams(vmem_limit_bytes=4 * MIB),
        name="pack",
        interpret=INTERPRET,
    )(*(pltpu.with_memory_space_constraint(a, pltpu.HBM) for a in arrays))


def rounded(a, b, dims):
    return lax.dot_general(
        a.astype(jnp.bfloat16),
        b.astype(jnp.bfloat16),
        (dims, ((), ())),
        preferred_element_type=jnp.float32,
    )


def norm_kernel(gathered_ref, gain_ref, out_ref):
    groups = gathered_ref.shape[0]
    blocks, _, wide = out_ref.shape
    per_tp = blocks // groups
    total = 0.0
    for g in range(groups):
        floats = gathered_ref[g].astype(jnp.float32)
        total = total + jnp.sum(floats * floats, axis=1, keepdims=True)
    scale = lax.rsqrt(total / (blocks * wide) + EPSILON)
    for at in range(blocks):
        i = at % per_tp
        part = gathered_ref[at // per_tp, :, i * wide : (i + 1) * wide].astype(jnp.float32)
        out_ref[at] = (part * scale * gain_ref[at]).astype(jnp.bfloat16)


def norm(gathered, gain, blocks):
    groups, rows, width = gathered.shape
    wide = width * groups // blocks
    return pl.pallas_call(
        norm_kernel,
        in_specs=[VMEM, VMEM],
        out_shape=jax.ShapeDtypeStruct((blocks, rows, wide), jnp.bfloat16),
        compiler_params=pltpu.CompilerParams(vmem_limit_bytes=6 * MIB),
        name="norm",
        interpret=INTERPRET,
    )(gathered, gain.reshape(blocks, 1, wide))


def project_kernel(
    own_ref,
    across_ref,
    w_own_ref,
    w_before_ref,
    w_after_ref,
    w_low_ref,
    w_high_ref,
    place_ref,
    cosine_ref,
    sine_ref,
    decay_ref,
    send_ref,
    att_ref,
    query_ref,
    within_ref,
):
    half, wide = own_ref.shape[1:]
    tokens = 2 * half
    low, high = slice(0, wide), slice(wide, 2 * wide)
    weights = [(w_own_ref, low), (w_own_ref, high), (w_before_ref, low), (w_before_ref, high)]
    weights += [(w_after_ref, low), (w_after_ref, high), (w_low_ref, low), (w_high_ref, low)]
    made = jnp.zeros((tokens, w_own_ref.shape[1]), jnp.float32)
    for k, (ref, at) in enumerate(weights):
        block = place_ref[1 + k]
        left = jnp.concatenate([own_ref[block], across_ref[block]], axis=0)
        made = made + jnp.dot(left, ref[at], preferred_element_type=jnp.float32)
    first = place_ref[0] == 0
    made = jnp.concatenate(
        [jnp.where(first, made[:half], made[half:]), jnp.where(first, made[half:], made[:half])],
        axis=0,
    ).astype(jnp.bfloat16)
    att_ref[...] = made[:, : 2 * DH] * jnp.bfloat16(DH ** (-0.5))

    pair = made[:, 256:384].astype(jnp.float32)
    lane = lax.broadcasted_iota(jnp.int32, pair.shape, 1)
    quarter = DH // 2
    ahead = pltpu.roll(pair, 2 * DH - quarter, 1)
    behind = pltpu.roll(pair, quarter, 1)
    crossed = jnp.where((lane & quarter) == 0, -ahead, behind)
    cosine = jnp.concatenate([cosine_ref[...]] * 4, axis=1)
    sine = jnp.concatenate([sine_ref[...]] * 4, axis=1)
    turned = pair * cosine + crossed * sine
    query = turned[:, :DH]
    key = turned[:, DH:] * DH ** (-0.5)
    value = made[:, 384:512]
    log_decay = decay_ref[0]
    offset = lax.broadcasted_iota(jnp.int32, (tokens, 1), 0).astype(jnp.float32)
    state = rounded(key * jnp.exp(log_decay * (tokens - 1.0 - offset)), value, ((0,), (0,)))
    state = state.astype(jnp.bfloat16)
    for k in range(send_ref.shape[0]):
        send_ref[k, :tokens] = made[:, 128:256]
        send_ref[k, tokens:] = state
    i = lax.broadcasted_iota(jnp.int32, (tokens, tokens), 0)
    j = lax.broadcasted_iota(jnp.int32, (tokens, tokens), 1)
    distance = (i - j).astype(jnp.float32)
    inside = jnp.where(i >= j, jnp.exp(log_decay * jnp.maximum(distance, 0.0)), 0.0)
    scores = rounded(query, key, ((1,), (1,))) * inside
    within_ref[...] = rounded(scores, value, ((1,), (0,)))
    query_ref[...] = query * jnp.exp(log_decay * (offset + 1.0))


def project(own, across, weights, place, cosine, sine, log_decay, count):
    tokens = 2 * own.shape[1]
    return pl.pallas_call(
        project_kernel,
        in_specs=[VMEM] * 7 + [SMEM, VMEM, VMEM, SMEM],
        out_shape=[
            jax.ShapeDtypeStruct((count, tokens + DH, DV), jnp.bfloat16),
            jax.ShapeDtypeStruct((tokens, 2 * DH), jnp.bfloat16),
            jax.ShapeDtypeStruct((tokens, DH), jnp.float32),
            jax.ShapeDtypeStruct((tokens, DV), jnp.float32),
        ],
        compiler_params=pltpu.CompilerParams(vmem_limit_bytes=12 * MIB),
        name="project",
        interpret=INTERPRET,
    )(own, across, *weights, place, cosine, sine, log_decay.reshape(1))


def pass_on_kernel(spread_ref, att_ref, weight_ref, send_ref):
    tokens = att_ref.shape[0]
    total = jnp.zeros((DH, DV), jnp.float32)
    for i in range(spread_ref.shape[0]):
        total = total + spread_ref[i, tokens:].astype(jnp.float32) * weight_ref[i]
    for k in range(send_ref.shape[0]):
        send_ref[k, :tokens] = att_ref[...]
        send_ref[k, tokens:] = total.astype(jnp.bfloat16)


def pass_on(spread, att, weight, count):
    return pl.pallas_call(
        pass_on_kernel,
        in_specs=[VMEM, VMEM, SMEM],
        out_shape=jax.ShapeDtypeStruct((count, *spread.shape[1:]), jnp.bfloat16),
        compiler_params=pltpu.CompilerParams(vmem_limit_bytes=6 * MIB),
        name="pass_on",
        interpret=INTERPRET,
    )(spread, att, weight)


def attend_kernel(
    where_ref, q_ref, mine_ref, other_ref, out_ref, k_ref, vt_ref, qt_ref, m_ref, l_ref, o_ref
):
    step = pl.program_id(0)
    z = where_ref[0]
    y = where_ref[1]
    keys = k_ref.shape[0]
    tokens = q_ref.shape[1]

    def prepare(key_ref, value_ref):
        for i in range(key_ref.shape[0]):
            at = slice(i * tokens, (i + 1) * tokens)
            k_ref[at] = key_ref[i, :tokens]
            vt_ref[:, at] = value_ref[i, :tokens].T

    @pl.when((step == 0) & (where_ref[2] == 0))
    def _():
        prepare(mine_ref, other_ref)

    @pl.when((step == 0) & (where_ref[2] != 0))
    def _():
        prepare(other_ref, mine_ref)

    def visit(start, count, masked):
        s = jnp.dot(k_ref[pl.ds(start, count)], qt_ref[...], preferred_element_type=jnp.float32)
        if masked:
            rows = lax.broadcasted_iota(jnp.int32, s.shape, 0) + start
            cols = lax.broadcasted_iota(jnp.int32, s.shape, 1) % tokens + y * tokens
            allowed = (rows // SEG) <= (cols // SEG)
            s = jnp.where(allowed, s, NEG)
        old = m_ref[...]
        top = jnp.maximum(old, jnp.max(s, axis=0, keepdims=True))
        w = jnp.exp(s - top)
        factor = jnp.exp(old - top)
        m_ref[...] = top
        l_ref[...] = l_ref[...] * factor + jnp.sum(w, axis=0, keepdims=True)
        o_ref[...] = o_ref[...] * factor + jnp.dot(
            vt_ref[:, pl.ds(start, count)],
            w.astype(jnp.bfloat16),
            preferred_element_type=jnp.float32,
        )

    @pl.when(step >= z)
    def _():
        q = q_ref[0]
        lane = lax.broadcasted_iota(jnp.int32, q.shape, 1)
        zero = jnp.zeros_like(q)
        q = jnp.concatenate([jnp.where(lane < DH, q, zero), jnp.where(lane < DH, zero, q)], axis=0)
        qt_ref[...] = q.T
        m_ref[...] = jnp.full(m_ref.shape, NEG, jnp.float32)
        l_ref[...] = jnp.zeros(l_ref.shape, jnp.float32)
        o_ref[...] = jnp.zeros(o_ref.shape, jnp.float32)

    @pl.when(step == z)
    def _():
        def body(i, _):
            visit(pl.multiple_of(i * KEYS, KEYS), KEYS, True)
            return 0

        lax.fori_loop(0, (y * tokens) // KEYS + 1, body, 0)

    @pl.when(step > z)
    def _():
        for start in range(0, keys, KEYS):
            visit(start, KEYS, False)

    @pl.when(step >= z)
    def _():
        total = l_ref[...]
        out_ref[0, :DV] = (o_ref[...] / total).astype(jnp.bfloat16)
        weight = m_ref[...] + jnp.log(total)
        high = weight.astype(jnp.bfloat16)
        rest = weight - high.astype(jnp.float32)
        middle = rest.astype(jnp.bfloat16)
        low = (rest - middle.astype(jnp.float32)).astype(jnp.bfloat16)
        pad = jnp.zeros((ROWS - DV - 3, weight.shape[1]), jnp.bfloat16)
        out_ref[0, DV:] = jnp.concatenate([high, middle, low, pad], axis=0)

    @pl.when(step < z)
    def _():
        out_ref[0, :DV] = jnp.zeros((DV, 2 * tokens), jnp.bfloat16)
        row = lax.broadcasted_iota(jnp.int32, (ROWS - DV, 2 * tokens), 0)
        out_ref[0, DV:] = jnp.where(row == 0, NEG, 0.0).astype(jnp.bfloat16)


def attend(where, along, mine, other, tokens):
    blocks = along.shape[0]
    count = mine.shape[0] * tokens

    def whole(shape):
        return pl.BlockSpec(shape, lambda g, w: (0,) * len(shape))

    return pl.pallas_call(
        attend_kernel,
        grid_spec=pltpu.PrefetchScalarGridSpec(
            num_scalar_prefetch=1,
            grid=(blocks,),
            in_specs=[
                pl.BlockSpec((1, tokens, 2 * DH), lambda g, w: (g, 0, 0)),
                whole(mine.shape),
                whole(other.shape),
            ],
            out_specs=pl.BlockSpec((1, ROWS, 2 * tokens), lambda g, w: (g, 0, 0)),
            scratch_shapes=[
                pltpu.VMEM((count, 2 * DH), jnp.bfloat16),
                pltpu.VMEM((DV, count), jnp.bfloat16),
                pltpu.VMEM((2 * DH, 2 * tokens), jnp.bfloat16),
                pltpu.VMEM((1, 2 * tokens), jnp.float32),
                pltpu.VMEM((1, 2 * tokens), jnp.float32),
                pltpu.VMEM((DV, 2 * tokens), jnp.float32),
            ],
        ),
        out_shape=jax.ShapeDtypeStruct((blocks, ROWS, 2 * tokens), jnp.bfloat16),
        compiler_params=pltpu.CompilerParams(
            dimension_semantics=("arbitrary",), vmem_limit_bytes=24 * MIB
        ),
        cost_estimate=pl.CostEstimate(
            flops=blocks * count * tokens * 4 * 256,
            bytes_accessed=blocks * tokens * 1024 + count * 512,
            transcendentals=blocks * count * tokens * 2,
        ),
        name="attend",
        interpret=INTERPRET,
    )(where, along, mine, other)


def finish_kernel(
    parts_ref, mix_ref, gain_ref, spread_ref, along_ref, weight_ref, query_ref, within_ref, out_ref
):
    blocks = parts_ref.shape[0]
    tokens = query_ref.shape[0]
    logs = []
    for i in range(blocks):
        rows = parts_ref[i, DV:].astype(jnp.float32)
        logs.append(rows[0:1] + rows[1:2] + rows[2:3])
    top = functools.reduce(jnp.maximum, logs)
    shares = [jnp.exp(log - top) for log in logs]
    total = functools.reduce(jnp.add, shares)
    acc = jnp.zeros((DV, 2 * tokens), jnp.float32)
    for i in range(blocks):
        acc = acc + parts_ref[i, :DV].astype(jnp.float32) * (shares[i] / total)
    att = acc[:, :tokens] - mix_ref[0] * acc[:, tokens:]
    att = att * lax.rsqrt(jnp.mean(att * att, axis=0, keepdims=True) + EPSILON)
    att = (att.T * gain_ref[0:1]).astype(jnp.bfloat16)
    carried = jnp.zeros((DH, DV), jnp.float32)
    chips = spread_ref.shape[0]
    for i in range(chips):
        carried = carried + spread_ref[i, tokens:].astype(jnp.float32) * weight_ref[i]
    for i in range(blocks):
        carried = carried + along_ref[i, tokens:].astype(jnp.float32) * weight_ref[chips + i]
    ret = within_ref[...] + rounded(query_ref[...], carried, ((1,), (0,)))
    ret = ret * lax.rsqrt(jnp.mean(ret * ret, axis=1, keepdims=True) + EPSILON)
    ret = (ret * gain_ref[1:2]).astype(jnp.bfloat16)
    half = tokens // 2
    for i in range(2):
        out_ref[i, :, :DV] = att[i * half : (i + 1) * half]
        out_ref[i, :, DV:] = ret[i * half : (i + 1) * half]


def finish(parts, mixing, gains, spread, along, weights, query, within):
    tokens = query.shape[0]
    return pl.pallas_call(
        finish_kernel,
        in_specs=[VMEM, SMEM, VMEM, VMEM, VMEM, SMEM, VMEM, VMEM],
        out_shape=jax.ShapeDtypeStruct((2, tokens // 2, 2 * DV), jnp.bfloat16),
        compiler_params=pltpu.CompilerParams(vmem_limit_bytes=8 * MIB),
        name="finish",
        interpret=INTERPRET,
    )(parts, mixing.reshape(1), gains, spread, along, weights, query, within)


def decay_log(head, length):
    pair = (head // 2).astype(jnp.float32)
    quick = jnp.log1p(-jnp.exp2(-5.0 - pair / 4.0))
    slow = jnp.log1p(-1.0 / (length * (1.0 + pair)))
    return jnp.where(head % 2 == 0, quick, slow)


def layer(
    features,
    norm_gain,
    att_query,
    att_key,
    att_value,
    att_lambda,
    att_gain,
    ret_query,
    ret_key,
    ret_value,
    ret_gain,
    out_weight,
):
    z = lax.axis_index(Z)
    y = lax.axis_index("y")
    c = lax.axis_index("c")
    x = lax.axis_index("tp")
    ny = lax.axis_size("y")
    nz = lax.axis_size(Z)
    nl = lax.axis_size("zl")
    groups = lax.axis_size("tp")
    chip = z * ny + y
    tokens = 2 * features.shape[0]

    matrices = (att_query, att_key, att_value, ret_query, ret_key, ret_value)
    sent, features = pack(2 * ny, groups, *matrices, features)
    rows, width = sent.shape[2:]
    sent = sent.reshape(4 * ny, rows, width)
    even = jnp.arange(0, DH, 2).astype(jnp.float32)
    small = (even, jnp.arange(ny), jnp.arange(nz), chip, z, y, c, x)
    sent, small = lax.optimization_barrier((sent, small))
    w_own = lax.all_to_all(sent, ("zh", "y", "c"), 0, 0, tiled=True)
    w_own = w_own.reshape(4 * ny * rows, width)
    inputs = (features, norm_gain, att_lambda, att_gain, ret_gain)
    w_own, inputs, small = lax.optimization_barrier((w_own, inputs, small))
    features, norm_gain, att_lambda, att_gain, ret_gain = inputs
    even, ys, zs, chip, z, y, c, x = small
    weights = (w_own, *around(w_own, 2 * ny * rows))
    blocks = [high * nl + (z + k) % nl for k in (0, nl - 1, 1, 2) for high in range(2)]

    gathered = lax.all_to_all(features, "tp", 0, 0, tiled=True)
    normed = norm(gathered, norm_gain, nz)
    across = swapped(normed)

    log_decay = decay_log(x * 2 + c, float(nz * ny * tokens))
    positions = (chip * tokens + jnp.arange(tokens)).astype(jnp.float32)
    inverse = 10000.0 ** (-even / DH)
    angles = positions[:, None] * inverse[None, :]
    cosine, sine = jnp.cos(angles), jnp.sin(angles)
    span = log_decay * tokens
    to_end = jnp.exp(span * (ny - 1 - ys).astype(jnp.float32))
    y_steps = jnp.maximum(y - 1 - ys, 0).astype(jnp.float32)
    z_steps = jnp.maximum(ny * (z - 1 - zs) + y, 0).astype(jnp.float32)
    before = jnp.concatenate(
        [
            jnp.where(ys < y, jnp.exp(span * y_steps), 0.0),
            jnp.where(zs < z, jnp.exp(span * z_steps), 0.0),
        ]
    )
    where = jnp.stack([z, y, c]).astype(jnp.int32)
    place = jnp.stack([c, *blocks]).astype(jnp.int32)
    mixing = lax.dynamic_index_in_dim(att_lambda, c, 0, keepdims=False)
    gains = jnp.stack([att_gain, ret_gain])

    tables = (cosine, sine, log_decay, to_end, before, where, place, mixing, gains)
    normed, across, weights, tables = lax.optimization_barrier((normed, across, weights, tables))
    cosine, sine, log_decay, to_end, before, where, place, mixing, gains = tables

    send, att, query, within = project(
        normed, across, weights, place, cosine, sine, log_decay, ny
    )
    spread = lax.all_to_all(send, "y", 0, 0, tiled=True)
    send = pass_on(spread, att, to_end, nz)
    along = lax.all_to_all(send, Z, 0, 0, tiled=True)
    other = swapped(spread)
    parts = attend(where, along, spread, other, tokens)
    parts = lax.all_to_all(parts, Z, 0, 0, tiled=True)

    heads = finish(parts, mixing, gains, spread, along, before, query, within)
    heads = lax.all_to_all(heads, "c", 0, 0, tiled=True)
    joined = jnp.concatenate(
        [heads[0, :, :DV], heads[1, :, :DV], heads[0, :, DV:], heads[1, :, DV:]], axis=1
    )
    partial = jnp.dot(
        joined, out_weight.reshape(-1, out_weight.shape[2]), preferred_element_type=jnp.float32
    ).astype(jnp.bfloat16)
    partial = lax.all_to_all(
        partial.reshape(groups, -1, partial.shape[1]), "tp", 0, 0, tiled=True
    )
    return jnp.sum(partial.astype(jnp.float32), axis=0)


def solution(mesh):
    devices = mesh.devices
    torus = Mesh(devices.reshape(2, 4, -1, 2, devices.shape[-1]), SP_TP)
    return jax.shard_map(
        layer,
        mesh=torus,
        in_specs=(
            P(SP, "tp"),
            P(),
            P(SP, "tp"),
            P(SP, "tp"),
            P(SP, "tp"),
            P("tp"),
            P(),
            P(SP, "tp"),
            P(SP, "tp"),
            P(SP, "tp"),
            P(),
            P(None, "tp", None),
        ),
        out_specs=P(SP_TP, None),
        check_vma=False,
    )
```

```python
import functools

import jax
import jax.numpy as jnp
from jax import lax
from jax.experimental import pallas as pl
from jax.experimental.pallas import tpu as pltpu
from jax.sharding import Mesh
from jax.sharding import PartitionSpec as P

DH = 64
DV = 128
SEG = 64
Z = ("zh", "zl")
SP = ("zh", "zl", "y", "c")
SP_TP = ("zh", "zl", "y", "c", "tp")
EPSILON = 1e-06
NEG = -1e30
KEYS = 512
ROWS = 136
MIB = 1 << 20
VMEM = pl.BlockSpec(memory_space=pltpu.VMEM)
SMEM = pl.BlockSpec(memory_space=pltpu.SMEM)
HBM = pl.BlockSpec(memory_space=pltpu.HBM)
INTERPRET = False


def swapped(value):
    return lax.ppermute(value, "c", [(0, 1), (1, 0)])


def shifted(value, step):
    count = lax.axis_size(Z)
    return lax.ppermute(value, Z, [(i, (i + step) % count) for i in range(count)])


def around(own, half):
    before = shifted(own, 1)
    after = shifted(own, -1)
    low = shifted(own[:half], 2)
    high = shifted(own[half:], -2)
    return before, after, low, high


def pack_kernel(*refs):
    count = len(refs) // 2
    sources, (out_ref, wide_ref), scratch, sems = (
        refs[: count - 1],
        refs[count - 1 : count + 1],
        refs[count + 1 : -1],
        refs[-1],
    )
    copies = [
        pltpu.make_async_copy(source, buffer, sems.at[i])
        for i, (source, buffer) in enumerate(zip(sources, scratch))
    ]
    for copy in copies:
        copy.start()
    for copy in copies:
        copy.wait()
    query, key, value, rq, rk, rv, features = (buffer[...] for buffer in scratch)
    for h, whole in enumerate((key, value)):
        parts = [query, whole, rq, rk, rv]
        for k in (0, 2, 3, 4):
            width = parts[k].shape[1] // 2
            parts[k] = parts[k][:, h * width : (h + 1) * width]
        row = jnp.concatenate(parts, axis=1)
        for i in range(out_ref.shape[0]):
            out_ref[i, h] = row
    for i in range(wide_ref.shape[0]):
        wide_ref[i] = features


def pack(count, groups, *arrays):
    rows = arrays[0].shape[0]
    return pl.pallas_call(
        pack_kernel,
        in_specs=[HBM] * len(arrays),
        out_shape=[
            jax.ShapeDtypeStruct((count, 2, rows, 512), jnp.bfloat16),
            jax.ShapeDtypeStruct((groups, *arrays[-1].shape), jnp.bfloat16),
        ],
        scratch_shapes=[pltpu.VMEM(a.shape, a.dtype) for a in arrays]
        + [pltpu.SemaphoreType.DMA((len(arrays),))],
        compiler_params=pltpu.CompilerParams(vmem_limit_bytes=4 * MIB),
        name="pack",
        interpret=INTERPRET,
    )(*(pltpu.with_memory_space_constraint(a, pltpu.HBM) for a in arrays))


def rounded(a, b, dims):
    return lax.dot_general(
        a.astype(jnp.bfloat16),
        b.astype(jnp.bfloat16),
        (dims, ((), ())),
        preferred_element_type=jnp.float32,
    )


def norm_kernel(far_ref, gain_ref, out_ref, gathered_ref, sems):
    groups = gathered_ref.shape[0]
    blocks, _, wide = out_ref.shape
    per_tp = blocks // groups
    copies = [
        pltpu.make_async_copy(far_ref.at[g], gathered_ref.at[g], sems.at[g]) for g in range(groups)
    ]
    for copy in copies:
        copy.start()
    total = 0.0
    for g in range(groups):
        copies[g].wait()
        floats = gathered_ref[g].astype(jnp.float32)
        total = total + jnp.sum(floats * floats, axis=1, keepdims=True)
    scale = lax.rsqrt(total / (blocks * wide) + EPSILON)
    for at in range(blocks):
        i = at % per_tp
        part = gathered_ref[at // per_tp, :, i * wide : (i + 1) * wide].astype(jnp.float32)
        out_ref[at] = (part * scale * gain_ref[at]).astype(jnp.bfloat16)


def norm(gathered, gain, blocks):
    groups, rows, width = gathered.shape
    wide = width * groups // blocks
    return pl.pallas_call(
        norm_kernel,
        in_specs=[HBM, VMEM],
        out_shape=jax.ShapeDtypeStruct((blocks, rows, wide), jnp.bfloat16),
        scratch_shapes=[
            pltpu.VMEM(gathered.shape, gathered.dtype),
            pltpu.SemaphoreType.DMA((groups,)),
        ],
        compiler_params=pltpu.CompilerParams(vmem_limit_bytes=6 * MIB),
        name="norm",
        interpret=INTERPRET,
    )(pltpu.with_memory_space_constraint(gathered, pltpu.HBM), gain.reshape(blocks, 1, wide))


def project_kernel(
    own_ref,
    across_ref,
    w_own_ref,
    w_before_ref,
    w_after_ref,
    w_low_ref,
    w_high_ref,
    place_ref,
    cosine_ref,
    sine_ref,
    decay_ref,
    send_ref,
    att_ref,
    query_ref,
    within_ref,
):
    half, wide = own_ref.shape[1:]
    tokens = 2 * half
    low, high = slice(0, wide), slice(wide, 2 * wide)
    weights = [(w_own_ref, low), (w_own_ref, high), (w_before_ref, low), (w_before_ref, high)]
    weights += [(w_after_ref, low), (w_after_ref, high), (w_low_ref, low), (w_high_ref, low)]
    made = jnp.zeros((tokens, w_own_ref.shape[1]), jnp.float32)
    for k, (ref, at) in enumerate(weights):
        block = place_ref[1 + k]
        left = jnp.concatenate([own_ref[block], across_ref[block]], axis=0)
        made = made + jnp.dot(left, ref[at], preferred_element_type=jnp.float32)
    first = place_ref[0] == 0
    made = jnp.concatenate(
        [jnp.where(first, made[:half], made[half:]), jnp.where(first, made[half:], made[:half])],
        axis=0,
    ).astype(jnp.bfloat16)
    att_ref[...] = made[:, : 2 * DH] * jnp.bfloat16(DH ** (-0.5))

    pair = made[:, 256:384].astype(jnp.float32)
    lane = lax.broadcasted_iota(jnp.int32, pair.shape, 1)
    quarter = DH // 2
    ahead = pltpu.roll(pair, 2 * DH - quarter, 1)
    behind = pltpu.roll(pair, quarter, 1)
    crossed = jnp.where((lane & quarter) == 0, -ahead, behind)
    cosine = jnp.concatenate([cosine_ref[...]] * 4, axis=1)
    sine = jnp.concatenate([sine_ref[...]] * 4, axis=1)
    turned = pair * cosine + crossed * sine
    query = turned[:, :DH]
    key = turned[:, DH:] * DH ** (-0.5)
    value = made[:, 384:512]
    log_decay = decay_ref[0]
    offset = lax.broadcasted_iota(jnp.int32, (tokens, 1), 0).astype(jnp.float32)
    state = rounded(key * jnp.exp(log_decay * (tokens - 1.0 - offset)), value, ((0,), (0,)))
    state = state.astype(jnp.bfloat16)
    for k in range(send_ref.shape[0]):
        send_ref[k, :tokens] = made[:, 128:256]
        send_ref[k, tokens:] = state
    i = lax.broadcasted_iota(jnp.int32, (tokens, tokens), 0)
    j = lax.broadcasted_iota(jnp.int32, (tokens, tokens), 1)
    distance = (i - j).astype(jnp.float32)
    inside = jnp.where(i >= j, jnp.exp(log_decay * jnp.maximum(distance, 0.0)), 0.0)
    scores = rounded(query, key, ((1,), (1,))) * inside
    within_ref[...] = rounded(scores, value, ((1,), (0,)))
    query_ref[...] = query * jnp.exp(log_decay * (offset + 1.0))


def project(own, across, weights, place, cosine, sine, log_decay, count):
    tokens = 2 * own.shape[1]
    return pl.pallas_call(
        project_kernel,
        in_specs=[VMEM] * 7 + [SMEM, VMEM, VMEM, SMEM],
        out_shape=[
            jax.ShapeDtypeStruct((count, tokens + DH, DV), jnp.bfloat16),
            jax.ShapeDtypeStruct((tokens, 2 * DH), jnp.bfloat16),
            jax.ShapeDtypeStruct((tokens, DH), jnp.float32),
            jax.ShapeDtypeStruct((tokens, DV), jnp.float32),
        ],
        compiler_params=pltpu.CompilerParams(vmem_limit_bytes=12 * MIB),
        name="project",
        interpret=INTERPRET,
    )(own, across, *weights, place, cosine, sine, log_decay.reshape(1))


def pass_on_kernel(spread_ref, att_ref, weight_ref, send_ref):
    tokens = att_ref.shape[0]
    total = jnp.zeros((DH, DV), jnp.float32)
    for i in range(spread_ref.shape[0]):
        total = total + spread_ref[i, tokens:].astype(jnp.float32) * weight_ref[i]
    for k in range(send_ref.shape[0]):
        send_ref[k, :tokens] = att_ref[...]
        send_ref[k, tokens:] = total.astype(jnp.bfloat16)


def pass_on(spread, att, weight, count):
    return pl.pallas_call(
        pass_on_kernel,
        in_specs=[VMEM, VMEM, SMEM],
        out_shape=jax.ShapeDtypeStruct((count, *spread.shape[1:]), jnp.bfloat16),
        compiler_params=pltpu.CompilerParams(vmem_limit_bytes=6 * MIB),
        name="pass_on",
        interpret=INTERPRET,
    )(spread, att, weight)


def attend_kernel(
    where_ref,
    q_ref,
    mine_ref,
    far_ref,
    out_ref,
    other_ref,
    k_ref,
    vt_ref,
    qt_ref,
    m_ref,
    l_ref,
    o_ref,
    sem,
):
    copy = pltpu.make_async_copy(far_ref, other_ref, sem)
    copy.start()
    z = where_ref[0]
    y = where_ref[1]
    keys = k_ref.shape[0]
    blocks = out_ref.shape[0]
    tokens = out_ref.shape[2] // 2

    first = where_ref[2] == 0

    def take_keys(ref):
        for i in range(ref.shape[0]):
            k_ref[i * tokens : (i + 1) * tokens] = ref[i, :tokens]

    def take_values(ref):
        for i in range(ref.shape[0]):
            vt_ref[:, i * tokens : (i + 1) * tokens] = ref[i, :tokens].T

    @pl.when(first)
    def _():
        take_keys(mine_ref)

    @pl.when(jnp.logical_not(first))
    def _():
        take_values(mine_ref)

    copy.wait()

    @pl.when(first)
    def _():
        take_values(other_ref)

    @pl.when(jnp.logical_not(first))
    def _():
        take_keys(other_ref)

    def visit(start, count, masked):
        s = jnp.dot(k_ref[pl.ds(start, count)], qt_ref[...], preferred_element_type=jnp.float32)
        if masked:
            rows = lax.broadcasted_iota(jnp.int32, s.shape, 0) + start
            cols = lax.broadcasted_iota(jnp.int32, s.shape, 1) % tokens + y * tokens
            allowed = (rows // SEG) <= (cols // SEG)
            s = jnp.where(allowed, s, NEG)
        old = m_ref[...]
        top = jnp.maximum(old, jnp.max(s, axis=0, keepdims=True))
        w = jnp.exp(s - top)
        factor = jnp.exp(old - top)
        m_ref[...] = top
        l_ref[...] = l_ref[...] * factor + jnp.sum(w, axis=0, keepdims=True)
        o_ref[...] = o_ref[...] * factor + jnp.dot(
            vt_ref[:, pl.ds(start, count)],
            w.astype(jnp.bfloat16),
            preferred_element_type=jnp.float32,
        )

    def empty(step, _):
        out_ref[step, :DV] = jnp.zeros((DV, 2 * tokens), jnp.bfloat16)
        row = lax.broadcasted_iota(jnp.int32, (ROWS - DV, 2 * tokens), 0)
        out_ref[step, DV:] = jnp.where(row == 0, NEG, 0.0).astype(jnp.bfloat16)
        return 0

    def begin(step):
        q = q_ref[step, :tokens]
        lane = lax.broadcasted_iota(jnp.int32, q.shape, 1)
        zero = jnp.zeros_like(q)
        q = jnp.concatenate([jnp.where(lane < DH, q, zero), jnp.where(lane < DH, zero, q)], axis=0)
        qt_ref[...] = q.T
        m_ref[...] = jnp.full(m_ref.shape, NEG, jnp.float32)
        l_ref[...] = jnp.zeros(l_ref.shape, jnp.float32)
        o_ref[...] = jnp.zeros(o_ref.shape, jnp.float32)

    def end(step):
        total = l_ref[...]
        out_ref[step, :DV] = (o_ref[...] / total).astype(jnp.bfloat16)
        weight = m_ref[...] + jnp.log(total)
        high = weight.astype(jnp.bfloat16)
        rest = weight - high.astype(jnp.float32)
        middle = rest.astype(jnp.bfloat16)
        low = (rest - middle.astype(jnp.float32)).astype(jnp.bfloat16)
        pad = jnp.zeros((ROWS - DV - 3, weight.shape[1]), jnp.bfloat16)
        out_ref[step, DV:] = jnp.concatenate([high, middle, low, pad], axis=0)

    def masked(i, _):
        visit(pl.multiple_of(i * KEYS, KEYS), KEYS, True)
        return 0

    def full(step, _):
        begin(step)
        for start in range(0, keys, KEYS):
            visit(start, KEYS, False)
        end(step)
        return 0

    lax.fori_loop(0, z, empty, 0)
    begin(z)
    lax.fori_loop(0, (y * tokens) // KEYS + 1, masked, 0)
    end(z)
    lax.fori_loop(z + 1, blocks, full, 0)


def attend(where, along, mine, other, tokens):
    blocks = along.shape[0]
    count = mine.shape[0] * tokens
    return pl.pallas_call(
        attend_kernel,
        in_specs=[SMEM, VMEM, VMEM, HBM],
        scratch_shapes=[
            pltpu.VMEM(other.shape, other.dtype),
            pltpu.VMEM((count, 2 * DH), jnp.bfloat16),
            pltpu.VMEM((DV, count), jnp.bfloat16),
            pltpu.VMEM((2 * DH, 2 * tokens), jnp.bfloat16),
            pltpu.VMEM((1, 2 * tokens), jnp.float32),
            pltpu.VMEM((1, 2 * tokens), jnp.float32),
            pltpu.VMEM((DV, 2 * tokens), jnp.float32),
            pltpu.SemaphoreType.DMA,
        ],
        out_shape=jax.ShapeDtypeStruct((blocks, ROWS, 2 * tokens), jnp.bfloat16),
        compiler_params=pltpu.CompilerParams(vmem_limit_bytes=16 * MIB),
        cost_estimate=pl.CostEstimate(
            flops=blocks * count * tokens * 4 * 256,
            bytes_accessed=blocks * tokens * 1024 + count * 512,
            transcendentals=blocks * count * tokens * 2,
        ),
        name="attend",
        interpret=INTERPRET,
    )(where, along, mine, pltpu.with_memory_space_constraint(other, pltpu.HBM))


def finish_kernel(
    parts_ref, mix_ref, gain_ref, spread_ref, along_ref, weight_ref, query_ref, within_ref, out_ref
):
    blocks = parts_ref.shape[0]
    tokens = query_ref.shape[0]
    logs = []
    for i in range(blocks):
        rows = parts_ref[i, DV:].astype(jnp.float32)
        logs.append(rows[0:1] + rows[1:2] + rows[2:3])
    top = functools.reduce(jnp.maximum, logs)
    shares = [jnp.exp(log - top) for log in logs]
    total = functools.reduce(jnp.add, shares)
    acc = jnp.zeros((DV, 2 * tokens), jnp.float32)
    for i in range(blocks):
        acc = acc + parts_ref[i, :DV].astype(jnp.float32) * (shares[i] / total)
    att = acc[:, :tokens] - mix_ref[0] * acc[:, tokens:]
    att = att * lax.rsqrt(jnp.mean(att * att, axis=0, keepdims=True) + EPSILON)
    att = (att.T * gain_ref[0:1]).astype(jnp.bfloat16)
    carried = jnp.zeros((DH, DV), jnp.float32)
    chips = spread_ref.shape[0]
    for i in range(chips):
        carried = carried + spread_ref[i, tokens:].astype(jnp.float32) * weight_ref[i]
    for i in range(blocks):
        carried = carried + along_ref[i, tokens:].astype(jnp.float32) * weight_ref[chips + i]
    ret = within_ref[...] + rounded(query_ref[...], carried, ((1,), (0,)))
    ret = ret * lax.rsqrt(jnp.mean(ret * ret, axis=1, keepdims=True) + EPSILON)
    ret = (ret * gain_ref[1:2]).astype(jnp.bfloat16)
    half = tokens // 2
    for i in range(2):
        out_ref[i, :, :DV] = att[i * half : (i + 1) * half]
        out_ref[i, :, DV:] = ret[i * half : (i + 1) * half]


def finish(parts, mixing, gains, spread, along, weights, query, within):
    tokens = query.shape[0]
    return pl.pallas_call(
        finish_kernel,
        in_specs=[VMEM, SMEM, VMEM, VMEM, VMEM, SMEM, VMEM, VMEM],
        out_shape=jax.ShapeDtypeStruct((2, tokens // 2, 2 * DV), jnp.bfloat16),
        compiler_params=pltpu.CompilerParams(vmem_limit_bytes=8 * MIB),
        name="finish",
        interpret=INTERPRET,
    )(parts, mixing.reshape(1), gains, spread, along, weights, query, within)


def decay_log(head, length):
    pair = (head // 2).astype(jnp.float32)
    quick = jnp.log1p(-jnp.exp2(-5.0 - pair / 4.0))
    slow = jnp.log1p(-1.0 / (length * (1.0 + pair)))
    return jnp.where(head % 2 == 0, quick, slow)


def layer(
    features,
    norm_gain,
    att_query,
    att_key,
    att_value,
    att_lambda,
    att_gain,
    ret_query,
    ret_key,
    ret_value,
    ret_gain,
    out_weight,
):
    z = lax.axis_index(Z)
    y = lax.axis_index("y")
    c = lax.axis_index("c")
    x = lax.axis_index("tp")
    ny = lax.axis_size("y")
    nz = lax.axis_size(Z)
    nl = lax.axis_size("zl")
    groups = lax.axis_size("tp")
    chip = z * ny + y
    tokens = 2 * features.shape[0]

    matrices = (att_query, att_key, att_value, ret_query, ret_key, ret_value)
    sent, features = pack(2 * ny, groups, *matrices, features)
    rows, width = sent.shape[2:]
    sent = sent.reshape(4 * ny, rows, width)
    even = jnp.arange(0, DH, 2).astype(jnp.float32)
    small = (even, jnp.arange(ny), jnp.arange(nz), chip, z, y, c, x)
    sent, small = lax.optimization_barrier((sent, small))
    w_own = lax.all_to_all(sent, ("zh", "y", "c"), 0, 0, tiled=True)
    w_own = w_own.reshape(4 * ny * rows, width)
    inputs = (features, norm_gain, att_lambda, att_gain, ret_gain)
    w_own, inputs, small = lax.optimization_barrier((w_own, inputs, small))
    features, norm_gain, att_lambda, att_gain, ret_gain = inputs
    even, ys, zs, chip, z, y, c, x = small
    weights = (w_own, *around(w_own, 2 * ny * rows))
    blocks = [high * nl + (z + k) % nl for k in (0, nl - 1, 1, 2) for high in range(2)]

    gathered = lax.all_to_all(features, "tp", 0, 0, tiled=True)
    normed = norm(gathered, norm_gain, nz)
    across = swapped(normed)

    log_decay = decay_log(x * 2 + c, float(nz * ny * tokens))
    positions = (chip * tokens + jnp.arange(tokens)).astype(jnp.float32)
    inverse = 10000.0 ** (-even / DH)
    angles = positions[:, None] * inverse[None, :]
    cosine, sine = jnp.cos(angles), jnp.sin(angles)
    span = log_decay * tokens
    to_end = jnp.exp(span * (ny - 1 - ys).astype(jnp.float32))
    y_steps = jnp.maximum(y - 1 - ys, 0).astype(jnp.float32)
    z_steps = jnp.maximum(ny * (z - 1 - zs) + y, 0).astype(jnp.float32)
    before = jnp.concatenate(
        [
            jnp.where(ys < y, jnp.exp(span * y_steps), 0.0),
            jnp.where(zs < z, jnp.exp(span * z_steps), 0.0),
        ]
    )
    where = jnp.stack([z, y, c]).astype(jnp.int32)
    place = jnp.stack([c, *blocks]).astype(jnp.int32)
    mixing = lax.dynamic_index_in_dim(att_lambda, c, 0, keepdims=False)
    gains = jnp.stack([att_gain, ret_gain])

    tables = (cosine, sine, log_decay, to_end, before, where, place, mixing, gains)
    normed, across, weights, tables = lax.optimization_barrier((normed, across, weights, tables))
    cosine, sine, log_decay, to_end, before, where, place, mixing, gains = tables

    send, att, query, within = project(
        normed, across, weights, place, cosine, sine, log_decay, ny
    )
    spread = lax.all_to_all(send, "y", 0, 0, tiled=True)
    send = pass_on(spread, att, to_end, nz)
    along = lax.all_to_all(send, Z, 0, 0, tiled=True)
    other = swapped(spread)
    parts = attend(where, along, spread, other, tokens)
    parts = lax.all_to_all(parts, Z, 0, 0, tiled=True)

    heads = finish(parts, mixing, gains, spread, along, before, query, within)
    heads = lax.all_to_all(heads, "c", 0, 0, tiled=True)
    joined = jnp.concatenate(
        [heads[0, :, :DV], heads[1, :, :DV], heads[0, :, DV:], heads[1, :, DV:]], axis=1
    )
    partial = jnp.dot(
        joined, out_weight.reshape(-1, out_weight.shape[2]), preferred_element_type=jnp.float32
    ).astype(jnp.bfloat16)
    partial = lax.all_to_all(
        partial.reshape(groups, -1, partial.shape[1]), "tp", 0, 0, tiled=True
    )
    return jnp.sum(partial.astype(jnp.float32), axis=0)


def solution(mesh):
    devices = mesh.devices
    torus = Mesh(devices.reshape(2, 4, -1, 2, devices.shape[-1]), SP_TP)
    return jax.shard_map(
        layer,
        mesh=torus,
        in_specs=(
            P(SP, "tp"),
            P(),
            P(SP, "tp"),
            P(SP, "tp"),
            P(SP, "tp"),
            P("tp"),
            P(),
            P(SP, "tp"),
            P(SP, "tp"),
            P(SP, "tp"),
            P(),
            P(None, "tp", None),
        ),
        out_specs=P(SP_TP, None),
        check_vma=False,
    )
```

```python
import functools

import jax
import jax.numpy as jnp
from jax import lax
from jax.experimental import pallas as pl
from jax.experimental.pallas import tpu as pltpu
from jax.sharding import Mesh
from jax.sharding import PartitionSpec as P

DH = 64
DV = 128
SEG = 64
Z = ("zh", "zl")
SP = ("zh", "zl", "y", "c")
SP_TP = ("zh", "zl", "y", "c", "tp")
EPSILON = 1e-06
NEG = -1e30
KEYS = 512
ROWS = 136
MIB = 1 << 20
VMEM = pl.BlockSpec(memory_space=pltpu.VMEM)
SMEM = pl.BlockSpec(memory_space=pltpu.SMEM)
HBM = pl.BlockSpec(memory_space=pltpu.HBM)
INTERPRET = False


def swapped(value):
    return lax.ppermute(value, "c", [(0, 1), (1, 0)])


def shifted(value, step):
    count = lax.axis_size(Z)
    return lax.ppermute(value, Z, [(i, (i + step) % count) for i in range(count)])


def around(own):
    before = shifted(own, 1)
    after = shifted(own, -1)
    count = lax.axis_size(Z)
    pairs = [(2 * i + k, 2 * ((i + (2, -2)[k]) % count) + k) for i in range(count) for k in range(2)]
    opposite = lax.ppermute(own, (*Z, "c"), pairs)
    return before, after, opposite


def pack_kernel(*refs):
    count = len(refs) // 2
    sources, (out_ref, wide_ref), scratch, sems = (
        refs[: count - 1],
        refs[count - 1 : count + 1],
        refs[count + 1 : -1],
        refs[-1],
    )
    copies = [
        pltpu.make_async_copy(source, buffer, sems.at[i])
        for i, (source, buffer) in enumerate(zip(sources, scratch))
    ]
    for copy in copies:
        copy.start()
    for copy in copies:
        copy.wait()
    query, key, value, rq, rk, rv, features = (buffer[...] for buffer in scratch)
    for h, whole in enumerate((key, value)):
        parts = [query, whole, rq, rk, rv]
        for k in (0, 2, 3, 4):
            width = parts[k].shape[1] // 2
            parts[k] = parts[k][:, h * width : (h + 1) * width]
        row = jnp.concatenate(parts, axis=1)
        for i in range(out_ref.shape[0]):
            out_ref[i, h] = row
    for i in range(wide_ref.shape[0]):
        wide_ref[i] = features


def pack(count, groups, *arrays):
    rows = arrays[0].shape[0]
    return pl.pallas_call(
        pack_kernel,
        in_specs=[HBM] * len(arrays),
        out_shape=[
            jax.ShapeDtypeStruct((count, 2, rows, 512), jnp.bfloat16),
            jax.ShapeDtypeStruct((groups, *arrays[-1].shape), jnp.bfloat16),
        ],
        scratch_shapes=[pltpu.VMEM(a.shape, a.dtype) for a in arrays]
        + [pltpu.SemaphoreType.DMA((len(arrays),))],
        compiler_params=pltpu.CompilerParams(vmem_limit_bytes=4 * MIB),
        name="pack",
        interpret=INTERPRET,
    )(*(pltpu.with_memory_space_constraint(a, pltpu.HBM) for a in arrays))


def rounded(a, b, dims):
    return lax.dot_general(
        a.astype(jnp.bfloat16),
        b.astype(jnp.bfloat16),
        (dims, ((), ())),
        preferred_element_type=jnp.float32,
    )


def norm_kernel(far_ref, gain_ref, out_ref, gathered_ref, sems):
    groups = gathered_ref.shape[0]
    blocks, _, wide = out_ref.shape
    per_tp = blocks // groups
    copies = [
        pltpu.make_async_copy(far_ref.at[g], gathered_ref.at[g], sems.at[g]) for g in range(groups)
    ]
    for copy in copies:
        copy.start()
    total = 0.0
    for g in range(groups):
        copies[g].wait()
        floats = gathered_ref[g].astype(jnp.float32)
        total = total + jnp.sum(floats * floats, axis=1, keepdims=True)
    scale = lax.rsqrt(total / (blocks * wide) + EPSILON)
    for at in range(blocks):
        i = at % per_tp
        part = gathered_ref[at // per_tp, :, i * wide : (i + 1) * wide].astype(jnp.float32)
        out_ref[at] = (part * scale * gain_ref[at]).astype(jnp.bfloat16)


def norm(gathered, gain, blocks):
    groups, rows, width = gathered.shape
    wide = width * groups // blocks
    return pl.pallas_call(
        norm_kernel,
        in_specs=[HBM, VMEM],
        out_shape=jax.ShapeDtypeStruct((blocks, rows, wide), jnp.bfloat16),
        scratch_shapes=[
            pltpu.VMEM(gathered.shape, gathered.dtype),
            pltpu.SemaphoreType.DMA((groups,)),
        ],
        compiler_params=pltpu.CompilerParams(vmem_limit_bytes=6 * MIB),
        name="norm",
        interpret=INTERPRET,
    )(pltpu.with_memory_space_constraint(gathered, pltpu.HBM), gain.reshape(blocks, 1, wide))


def project_kernel(
    own_ref,
    across_ref,
    w_own_ref,
    w_before_ref,
    w_after_ref,
    w_opposite_ref,
    place_ref,
    cosine_ref,
    sine_ref,
    decay_ref,
    send_ref,
    att_ref,
    query_ref,
    within_ref,
):
    half, wide = own_ref.shape[1:]
    tokens = 2 * half
    low, high = slice(0, wide), slice(wide, 2 * wide)
    weights = [(w_own_ref, low), (w_own_ref, high), (w_before_ref, low), (w_before_ref, high)]
    weights += [(w_after_ref, low), (w_after_ref, high)]
    weights += [(w_opposite_ref, low), (w_opposite_ref, high)]
    made = jnp.zeros((tokens, w_own_ref.shape[1]), jnp.float32)
    for k, (ref, at) in enumerate(weights):
        block = place_ref[1 + k]
        left = jnp.concatenate([own_ref[block], across_ref[block]], axis=0)
        made = made + jnp.dot(left, ref[at], preferred_element_type=jnp.float32)
    first = place_ref[0] == 0
    made = jnp.concatenate(
        [jnp.where(first, made[:half], made[half:]), jnp.where(first, made[half:], made[:half])],
        axis=0,
    ).astype(jnp.bfloat16)
    att_ref[...] = made[:, : 2 * DH] * jnp.bfloat16(DH ** (-0.5))

    pair = made[:, 256:384].astype(jnp.float32)
    lane = lax.broadcasted_iota(jnp.int32, pair.shape, 1)
    quarter = DH // 2
    ahead = pltpu.roll(pair, 2 * DH - quarter, 1)
    behind = pltpu.roll(pair, quarter, 1)
    crossed = jnp.where((lane & quarter) == 0, -ahead, behind)
    cosine = jnp.concatenate([cosine_ref[...]] * 4, axis=1)
    sine = jnp.concatenate([sine_ref[...]] * 4, axis=1)
    turned = pair * cosine + crossed * sine
    query = turned[:, :DH]
    key = turned[:, DH:] * DH ** (-0.5)
    value = made[:, 384:512]
    log_decay = decay_ref[0]
    offset = lax.broadcasted_iota(jnp.int32, (tokens, 1), 0).astype(jnp.float32)
    state = rounded(key * jnp.exp(log_decay * (tokens - 1.0 - offset)), value, ((0,), (0,)))
    state = state.astype(jnp.bfloat16)
    for k in range(send_ref.shape[0]):
        send_ref[k, :tokens] = made[:, 128:256]
        send_ref[k, tokens:] = state
    i = lax.broadcasted_iota(jnp.int32, (tokens, tokens), 0)
    j = lax.broadcasted_iota(jnp.int32, (tokens, tokens), 1)
    distance = (i - j).astype(jnp.float32)
    inside = jnp.where(i >= j, jnp.exp(log_decay * jnp.maximum(distance, 0.0)), 0.0)
    scores = rounded(query, key, ((1,), (1,))) * inside
    within_ref[...] = rounded(scores, value, ((1,), (0,)))
    query_ref[...] = query * jnp.exp(log_decay * (offset + 1.0))


def project(own, across, weights, place, cosine, sine, log_decay, count):
    tokens = 2 * own.shape[1]
    return pl.pallas_call(
        project_kernel,
        in_specs=[VMEM] * 6 + [SMEM, VMEM, VMEM, SMEM],
        out_shape=[
            jax.ShapeDtypeStruct((count, tokens + DH, DV), jnp.bfloat16),
            jax.ShapeDtypeStruct((tokens, 2 * DH), jnp.bfloat16),
            jax.ShapeDtypeStruct((tokens, DH), jnp.float32),
            jax.ShapeDtypeStruct((tokens, DV), jnp.float32),
        ],
        compiler_params=pltpu.CompilerParams(vmem_limit_bytes=12 * MIB),
        name="project",
        interpret=INTERPRET,
    )(own, across, *weights, place, cosine, sine, log_decay.reshape(1))


def pass_on_kernel(spread_ref, att_ref, weight_ref, send_ref):
    tokens = att_ref.shape[0]
    total = jnp.zeros((DH, DV), jnp.float32)
    for i in range(spread_ref.shape[0]):
        total = total + spread_ref[i, tokens:].astype(jnp.float32) * weight_ref[i]
    for k in range(send_ref.shape[0]):
        send_ref[k, :tokens] = att_ref[...]
        send_ref[k, tokens:] = total.astype(jnp.bfloat16)


def pass_on(spread, att, weight, count):
    return pl.pallas_call(
        pass_on_kernel,
        in_specs=[VMEM, VMEM, SMEM],
        out_shape=jax.ShapeDtypeStruct((count, *spread.shape[1:]), jnp.bfloat16),
        compiler_params=pltpu.CompilerParams(vmem_limit_bytes=6 * MIB),
        name="pass_on",
        interpret=INTERPRET,
    )(spread, att, weight)


def attend_kernel(
    where_ref,
    q_ref,
    mine_ref,
    far_ref,
    out_ref,
    other_ref,
    k_ref,
    vt_ref,
    qt_ref,
    m_ref,
    l_ref,
    o_ref,
    sem,
):
    copy = pltpu.make_async_copy(far_ref, other_ref, sem)
    copy.start()
    z = where_ref[0]
    y = where_ref[1]
    keys = k_ref.shape[0]
    blocks = out_ref.shape[0]
    tokens = out_ref.shape[2] // 2

    first = where_ref[2] == 0

    def take_keys(ref):
        for i in range(ref.shape[0]):
            k_ref[i * tokens : (i + 1) * tokens] = ref[i, :tokens]

    def take_values(ref):
        for i in range(ref.shape[0]):
            vt_ref[:, i * tokens : (i + 1) * tokens] = ref[i, :tokens].T

    @pl.when(first)
    def _():
        take_keys(mine_ref)

    @pl.when(jnp.logical_not(first))
    def _():
        take_values(mine_ref)

    copy.wait()

    @pl.when(first)
    def _():
        take_values(other_ref)

    @pl.when(jnp.logical_not(first))
    def _():
        take_keys(other_ref)

    def visit(start, count, masked):
        s = jnp.dot(k_ref[pl.ds(start, count)], qt_ref[...], preferred_element_type=jnp.float32)
        if masked:
            rows = lax.broadcasted_iota(jnp.int32, s.shape, 0) + start
            cols = lax.broadcasted_iota(jnp.int32, s.shape, 1) % tokens + y * tokens
            allowed = (rows // SEG) <= (cols // SEG)
            s = jnp.where(allowed, s, NEG)
        old = m_ref[...]
        top = jnp.maximum(old, jnp.max(s, axis=0, keepdims=True))
        w = jnp.exp(s - top)
        factor = jnp.exp(old - top)
        m_ref[...] = top
        l_ref[...] = l_ref[...] * factor + jnp.sum(w, axis=0, keepdims=True)
        o_ref[...] = o_ref[...] * factor + jnp.dot(
            vt_ref[:, pl.ds(start, count)],
            w.astype(jnp.bfloat16),
            preferred_element_type=jnp.float32,
        )

    def empty(step, _):
        out_ref[step, :DV] = jnp.zeros((DV, 2 * tokens), jnp.bfloat16)
        row = lax.broadcasted_iota(jnp.int32, (ROWS - DV, 2 * tokens), 0)
        out_ref[step, DV:] = jnp.where(row == 0, NEG, 0.0).astype(jnp.bfloat16)
        return 0

    def begin(step):
        q = q_ref[step, :tokens]
        lane = lax.broadcasted_iota(jnp.int32, q.shape, 1)
        zero = jnp.zeros_like(q)
        q = jnp.concatenate([jnp.where(lane < DH, q, zero), jnp.where(lane < DH, zero, q)], axis=0)
        qt_ref[...] = q.T
        m_ref[...] = jnp.full(m_ref.shape, NEG, jnp.float32)
        l_ref[...] = jnp.zeros(l_ref.shape, jnp.float32)
        o_ref[...] = jnp.zeros(o_ref.shape, jnp.float32)

    def end(step):
        total = l_ref[...]
        out_ref[step, :DV] = (o_ref[...] / total).astype(jnp.bfloat16)
        weight = m_ref[...] + jnp.log(total)
        high = weight.astype(jnp.bfloat16)
        rest = weight - high.astype(jnp.float32)
        middle = rest.astype(jnp.bfloat16)
        low = (rest - middle.astype(jnp.float32)).astype(jnp.bfloat16)
        pad = jnp.zeros((ROWS - DV - 3, weight.shape[1]), jnp.bfloat16)
        out_ref[step, DV:] = jnp.concatenate([high, middle, low, pad], axis=0)

    def masked(i, _):
        visit(pl.multiple_of(i * KEYS, KEYS), KEYS, True)
        return 0

    def full(step, _):
        begin(step)
        for start in range(0, keys, KEYS):
            visit(start, KEYS, False)
        end(step)
        return 0

    lax.fori_loop(0, z, empty, 0)
    begin(z)
    lax.fori_loop(0, (y * tokens) // KEYS + 1, masked, 0)
    end(z)
    lax.fori_loop(z + 1, blocks, full, 0)


def attend(where, along, mine, other, tokens):
    blocks = along.shape[0]
    count = mine.shape[0] * tokens
    return pl.pallas_call(
        attend_kernel,
        in_specs=[SMEM, VMEM, VMEM, HBM],
        scratch_shapes=[
            pltpu.VMEM(other.shape, other.dtype),
            pltpu.VMEM((count, 2 * DH), jnp.bfloat16),
            pltpu.VMEM((DV, count), jnp.bfloat16),
            pltpu.VMEM((2 * DH, 2 * tokens), jnp.bfloat16),
            pltpu.VMEM((1, 2 * tokens), jnp.float32),
            pltpu.VMEM((1, 2 * tokens), jnp.float32),
            pltpu.VMEM((DV, 2 * tokens), jnp.float32),
            pltpu.SemaphoreType.DMA,
        ],
        out_shape=jax.ShapeDtypeStruct((blocks, ROWS, 2 * tokens), jnp.bfloat16),
        compiler_params=pltpu.CompilerParams(vmem_limit_bytes=16 * MIB),
        cost_estimate=pl.CostEstimate(
            flops=blocks * count * tokens * 4 * 256,
            bytes_accessed=blocks * tokens * 1024 + count * 512,
            transcendentals=blocks * count * tokens * 2,
        ),
        name="attend",
        interpret=INTERPRET,
    )(where, along, mine, pltpu.with_memory_space_constraint(other, pltpu.HBM))


def finish_kernel(
    parts_ref, mix_ref, gain_ref, spread_ref, along_ref, weight_ref, query_ref, within_ref, out_ref
):
    blocks = parts_ref.shape[0]
    tokens = query_ref.shape[0]
    logs = []
    for i in range(blocks):
        rows = parts_ref[i, DV:].astype(jnp.float32)
        logs.append(rows[0:1] + rows[1:2] + rows[2:3])
    top = functools.reduce(jnp.maximum, logs)
    shares = [jnp.exp(log - top) for log in logs]
    total = functools.reduce(jnp.add, shares)
    acc = jnp.zeros((DV, 2 * tokens), jnp.float32)
    for i in range(blocks):
        acc = acc + parts_ref[i, :DV].astype(jnp.float32) * (shares[i] / total)
    att = acc[:, :tokens] - mix_ref[0] * acc[:, tokens:]
    att = att * lax.rsqrt(jnp.mean(att * att, axis=0, keepdims=True) + EPSILON)
    att = (att.T * gain_ref[0:1]).astype(jnp.bfloat16)
    carried = jnp.zeros((DH, DV), jnp.float32)
    chips = spread_ref.shape[0]
    for i in range(chips):
        carried = carried + spread_ref[i, tokens:].astype(jnp.float32) * weight_ref[i]
    for i in range(blocks):
        carried = carried + along_ref[i, tokens:].astype(jnp.float32) * weight_ref[chips + i]
    ret = within_ref[...] + rounded(query_ref[...], carried, ((1,), (0,)))
    ret = ret * lax.rsqrt(jnp.mean(ret * ret, axis=1, keepdims=True) + EPSILON)
    ret = (ret * gain_ref[1:2]).astype(jnp.bfloat16)
    half = tokens // 2
    for i in range(2):
        out_ref[i, :, :DV] = att[i * half : (i + 1) * half]
        out_ref[i, :, DV:] = ret[i * half : (i + 1) * half]


def finish(parts, mixing, gains, spread, along, weights, query, within):
    tokens = query.shape[0]
    return pl.pallas_call(
        finish_kernel,
        in_specs=[VMEM, SMEM, VMEM, VMEM, VMEM, SMEM, VMEM, VMEM],
        out_shape=jax.ShapeDtypeStruct((2, tokens // 2, 2 * DV), jnp.bfloat16),
        compiler_params=pltpu.CompilerParams(vmem_limit_bytes=8 * MIB),
        name="finish",
        interpret=INTERPRET,
    )(parts, mixing.reshape(1), gains, spread, along, weights, query, within)


def decay_log(head, length):
    pair = (head // 2).astype(jnp.float32)
    quick = jnp.log1p(-jnp.exp2(-5.0 - pair / 4.0))
    slow = jnp.log1p(-1.0 / (length * (1.0 + pair)))
    return jnp.where(head % 2 == 0, quick, slow)


def layer(
    features,
    norm_gain,
    att_query,
    att_key,
    att_value,
    att_lambda,
    att_gain,
    ret_query,
    ret_key,
    ret_value,
    ret_gain,
    out_weight,
):
    z = lax.axis_index(Z)
    y = lax.axis_index("y")
    c = lax.axis_index("c")
    x = lax.axis_index("tp")
    ny = lax.axis_size("y")
    nz = lax.axis_size(Z)
    nl = lax.axis_size("zl")
    groups = lax.axis_size("tp")
    chip = z * ny + y
    tokens = 2 * features.shape[0]

    matrices = (att_query, att_key, att_value, ret_query, ret_key, ret_value)
    sent, features = pack(2 * ny, groups, *matrices, features)
    rows, width = sent.shape[2:]
    sent = sent.reshape(4 * ny, rows, width)
    even = jnp.arange(0, DH, 2).astype(jnp.float32)
    small = (even, jnp.arange(ny), jnp.arange(nz), chip, z, y, c, x)
    sent, small = lax.optimization_barrier((sent, small))
    w_own = lax.all_to_all(sent, ("zh", "y", "c"), 0, 0, tiled=True)
    w_own = w_own.reshape(4 * ny * rows, width)
    inputs = (features, norm_gain, att_lambda, att_gain, ret_gain)
    w_own, inputs, small = lax.optimization_barrier((w_own, inputs, small))
    features, norm_gain, att_lambda, att_gain, ret_gain = inputs
    even, ys, zs, chip, z, y, c, x = small
    weights = (w_own, *around(w_own))
    blocks = [high * nl + (z + k) % nl for k in (0, nl - 1, 1, 2) for high in range(2)]

    gathered = lax.all_to_all(features, "tp", 0, 0, tiled=True)
    normed = norm(gathered, norm_gain, nz)
    across = swapped(normed)

    log_decay = decay_log(x * 2 + c, float(nz * ny * tokens))
    positions = (chip * tokens + jnp.arange(tokens)).astype(jnp.float32)
    inverse = 10000.0 ** (-even / DH)
    angles = positions[:, None] * inverse[None, :]
    cosine, sine = jnp.cos(angles), jnp.sin(angles)
    span = log_decay * tokens
    to_end = jnp.exp(span * (ny - 1 - ys).astype(jnp.float32))
    place = jnp.stack([c, *blocks]).astype(jnp.int32)
    tables = (cosine, sine, log_decay, to_end, place)
    normed, across, weights, tables = lax.optimization_barrier((normed, across, weights, tables))
    cosine, sine, log_decay, to_end, place = tables

    send, att, query, within = project(
        normed, across, weights, place, cosine, sine, log_decay, ny
    )
    spread = lax.all_to_all(send, "y", 0, 0, tiled=True)
    small = (ys, zs, span, z, y, c, att_lambda, att_gain, ret_gain)
    spread, small = lax.optimization_barrier((spread, small))
    ys, zs, span, z, y, c, att_lambda, att_gain, ret_gain = small
    y_steps = jnp.maximum(y - 1 - ys, 0).astype(jnp.float32)
    z_steps = jnp.maximum(ny * (z - 1 - zs) + y, 0).astype(jnp.float32)
    before = jnp.concatenate(
        [
            jnp.where(ys < y, jnp.exp(span * y_steps), 0.0),
            jnp.where(zs < z, jnp.exp(span * z_steps), 0.0),
        ]
    )
    where = jnp.stack([z, y, c]).astype(jnp.int32)
    mixing = lax.dynamic_index_in_dim(att_lambda, c, 0, keepdims=False)
    gains = jnp.stack([att_gain, ret_gain])
    send = pass_on(spread, att, to_end, nz)
    along = lax.all_to_all(send, Z, 0, 0, tiled=True)
    other = swapped(spread)
    tables = (before, where, mixing, gains)
    along, tables = lax.optimization_barrier((along, tables))
    before, where, mixing, gains = tables
    parts = attend(where, along, spread, other, tokens)
    parts = lax.all_to_all(parts, Z, 0, 0, tiled=True)

    heads = finish(parts, mixing, gains, spread, along, before, query, within)
    heads = lax.all_to_all(heads, "c", 0, 0, tiled=True)
    joined = jnp.concatenate(
        [heads[0, :, :DV], heads[1, :, :DV], heads[0, :, DV:], heads[1, :, DV:]], axis=1
    )
    partial = jnp.dot(
        joined, out_weight.reshape(-1, out_weight.shape[2]), preferred_element_type=jnp.float32
    ).astype(jnp.bfloat16)
    partial = lax.all_to_all(
        partial.reshape(groups, -1, partial.shape[1]), "tp", 0, 0, tiled=True
    )
    return jnp.sum(partial.astype(jnp.float32), axis=0)


def solution(mesh):
    devices = mesh.devices
    torus = Mesh(devices.reshape(2, 4, -1, 2, devices.shape[-1]), SP_TP)
    return jax.shard_map(
        layer,
        mesh=torus,
        in_specs=(
            P(SP, "tp"),
            P(),
            P(SP, "tp"),
            P(SP, "tp"),
            P(SP, "tp"),
            P("tp"),
            P(),
            P(SP, "tp"),
            P(SP, "tp"),
            P(SP, "tp"),
            P(),
            P(None, "tp", None),
        ),
        out_specs=P(SP_TP, None),
        check_vma=False,
    )
```

```python
import functools

import jax
import jax.numpy as jnp
from jax import lax
from jax.experimental import pallas as pl
from jax.experimental.pallas import tpu as pltpu
from jax.sharding import Mesh
from jax.sharding import PartitionSpec as P

DH = 64
DV = 128
SEG = 64
Z = ("zh", "zl")
SP = ("zh", "zl", "y", "c")
SP_TP = ("zh", "zl", "y", "c", "tp")
EPSILON = 1e-06
NEG = -1e30
KEYS = 512
ROWS = 136
MIB = 1 << 20
VMEM = pl.BlockSpec(memory_space=pltpu.VMEM)
SMEM = pl.BlockSpec(memory_space=pltpu.SMEM)
HBM = pl.BlockSpec(memory_space=pltpu.HBM)
INTERPRET = False


def swapped(value):
    return lax.ppermute(value, "c", [(0, 1), (1, 0)])


def shifted(value, step):
    count = lax.axis_size(Z)
    return lax.ppermute(value, Z, [(i, (i + step) % count) for i in range(count)])


def around(own):
    before = shifted(own, 1)
    after = shifted(own, -1)
    count = lax.axis_size(Z)
    pairs = [(2 * i + k, 2 * ((i + (2, -2)[k]) % count) + k) for i in range(count) for k in range(2)]
    opposite = lax.ppermute(own, (*Z, "c"), pairs)
    return before, after, opposite


def pack_kernel(*refs):
    count = len(refs) // 2
    sources, (out_ref, wide_ref), scratch, sems = (
        refs[: count - 1],
        refs[count - 1 : count + 1],
        refs[count + 1 : -1],
        refs[-1],
    )
    copies = [
        pltpu.make_async_copy(source, buffer, sems.at[i])
        for i, (source, buffer) in enumerate(zip(sources, scratch))
    ]
    for copy in copies:
        copy.start()
    for copy in copies:
        copy.wait()
    wide = [
        pltpu.make_async_copy(scratch[-1], wide_ref.at[i], sems.at[count - 1 + i])
        for i in range(wide_ref.shape[0])
    ]
    for copy in wide:
        copy.start()
    query, key, value, rq, rk, rv = (buffer[...] for buffer in scratch[:-1])
    for h, whole in enumerate((key, value)):
        parts = [query, whole, rq, rk, rv]
        for k in (0, 2, 3, 4):
            width = parts[k].shape[1] // 2
            parts[k] = parts[k][:, h * width : (h + 1) * width]
        row = jnp.concatenate(parts, axis=1)
        for i in range(out_ref.shape[0]):
            out_ref[i, h] = row
    for copy in wide:
        copy.wait()


def pack(count, groups, *arrays):
    rows = arrays[0].shape[0]
    return pl.pallas_call(
        pack_kernel,
        in_specs=[HBM] * len(arrays),
        out_specs=[VMEM, HBM],
        out_shape=[
            jax.ShapeDtypeStruct((count, 2, rows, 512), jnp.bfloat16),
            jax.ShapeDtypeStruct((groups, *arrays[-1].shape), jnp.bfloat16),
        ],
        scratch_shapes=[pltpu.VMEM(a.shape, a.dtype) for a in arrays]
        + [pltpu.SemaphoreType.DMA((len(arrays) + groups,))],
        compiler_params=pltpu.CompilerParams(vmem_limit_bytes=4 * MIB),
        name="pack",
        interpret=INTERPRET,
    )(*(pltpu.with_memory_space_constraint(a, pltpu.HBM) for a in arrays))


def rounded(a, b, dims):
    return lax.dot_general(
        a.astype(jnp.bfloat16),
        b.astype(jnp.bfloat16),
        (dims, ((), ())),
        preferred_element_type=jnp.float32,
    )


def norm_kernel(far_ref, gain_ref, out_ref, gathered_ref, sems):
    groups = gathered_ref.shape[0]
    blocks, _, wide = out_ref.shape
    per_tp = blocks // groups
    copies = [
        pltpu.make_async_copy(far_ref.at[g], gathered_ref.at[g], sems.at[g]) for g in range(groups)
    ]
    for copy in copies:
        copy.start()
    total = 0.0
    for g in range(groups):
        copies[g].wait()
        floats = gathered_ref[g].astype(jnp.float32)
        total = total + jnp.sum(floats * floats, axis=1, keepdims=True)
    scale = lax.rsqrt(total / (blocks * wide) + EPSILON)
    for at in range(blocks):
        i = at % per_tp
        part = gathered_ref[at // per_tp, :, i * wide : (i + 1) * wide].astype(jnp.float32)
        out_ref[at] = (part * scale * gain_ref[at]).astype(jnp.bfloat16)


def norm(gathered, gain, blocks):
    groups, rows, width = gathered.shape
    wide = width * groups // blocks
    return pl.pallas_call(
        norm_kernel,
        in_specs=[HBM, VMEM],
        out_shape=jax.ShapeDtypeStruct((blocks, rows, wide), jnp.bfloat16),
        scratch_shapes=[
            pltpu.VMEM(gathered.shape, gathered.dtype),
            pltpu.SemaphoreType.DMA((groups,)),
        ],
        compiler_params=pltpu.CompilerParams(vmem_limit_bytes=6 * MIB),
        name="norm",
        interpret=INTERPRET,
    )(pltpu.with_memory_space_constraint(gathered, pltpu.HBM), gain.reshape(blocks, 1, wide))


def project_kernel(
    own_ref,
    across_ref,
    w_own_ref,
    w_before_ref,
    w_after_ref,
    w_opposite_ref,
    place_ref,
    cosine_ref,
    sine_ref,
    decay_ref,
    send_ref,
    att_ref,
    turned_ref,
    value_ref,
):
    half, wide = own_ref.shape[1:]
    tokens = 2 * half
    low, high = slice(0, wide), slice(wide, 2 * wide)
    weights = [(w_own_ref, low), (w_own_ref, high), (w_before_ref, low), (w_before_ref, high)]
    weights += [(w_after_ref, low), (w_after_ref, high)]
    weights += [(w_opposite_ref, low), (w_opposite_ref, high)]
    made = jnp.zeros((tokens, w_own_ref.shape[1]), jnp.float32)
    for k, (ref, at) in enumerate(weights):
        block = place_ref[1 + k]
        left = jnp.concatenate([own_ref[block], across_ref[block]], axis=0)
        made = made + jnp.dot(left, ref[at], preferred_element_type=jnp.float32)
    first = place_ref[0] == 0
    made = jnp.concatenate(
        [jnp.where(first, made[:half], made[half:]), jnp.where(first, made[half:], made[:half])],
        axis=0,
    ).astype(jnp.bfloat16)
    att_ref[...] = made[:, : 2 * DH] * jnp.bfloat16(DH ** (-0.5))

    pair = made[:, 256:384].astype(jnp.float32)
    lane = lax.broadcasted_iota(jnp.int32, pair.shape, 1)
    quarter = DH // 2
    ahead = pltpu.roll(pair, 2 * DH - quarter, 1)
    behind = pltpu.roll(pair, quarter, 1)
    crossed = jnp.where((lane & quarter) == 0, -ahead, behind)
    cosine = jnp.concatenate([cosine_ref[...]] * 4, axis=1)
    sine = jnp.concatenate([sine_ref[...]] * 4, axis=1)
    turned = pair * cosine + crossed * sine
    key = turned[:, DH:] * DH ** (-0.5)
    value = made[:, 384:512]
    log_decay = decay_ref[0]
    offset = lax.broadcasted_iota(jnp.int32, (tokens, 1), 0).astype(jnp.float32)
    state = rounded(key * jnp.exp(log_decay * (tokens - 1.0 - offset)), value, ((0,), (0,)))
    state = state.astype(jnp.bfloat16)
    for k in range(send_ref.shape[0]):
        send_ref[k, :tokens] = made[:, 128:256]
        send_ref[k, tokens:] = state
    turned_ref[...] = turned
    value_ref[...] = value


def local_kernel(turned_ref, value_ref, decay_ref, query_ref, within_ref):
    tokens = turned_ref.shape[0]
    query = turned_ref[:, :DH]
    key = turned_ref[:, DH:] * DH ** (-0.5)
    value = value_ref[...]
    log_decay = decay_ref[0]
    offset = lax.broadcasted_iota(jnp.int32, (tokens, 1), 0).astype(jnp.float32)
    i = lax.broadcasted_iota(jnp.int32, (tokens, tokens), 0)
    j = lax.broadcasted_iota(jnp.int32, (tokens, tokens), 1)
    distance = (i - j).astype(jnp.float32)
    inside = jnp.where(i >= j, jnp.exp(log_decay * jnp.maximum(distance, 0.0)), 0.0)
    scores = rounded(query, key, ((1,), (1,))) * inside
    within_ref[...] = rounded(scores, value, ((1,), (0,)))
    query_ref[...] = query * jnp.exp(log_decay * (offset + 1.0))


def local(turned, value, log_decay):
    tokens = turned.shape[0]
    return pl.pallas_call(
        local_kernel,
        in_specs=[VMEM, VMEM, SMEM],
        out_shape=[
            jax.ShapeDtypeStruct((tokens, DH), jnp.float32),
            jax.ShapeDtypeStruct((tokens, DV), jnp.float32),
        ],
        compiler_params=pltpu.CompilerParams(vmem_limit_bytes=6 * MIB),
        name="local",
        interpret=INTERPRET,
    )(turned, value, log_decay.reshape(1))


def project(own, across, weights, place, cosine, sine, log_decay, count):
    tokens = 2 * own.shape[1]
    return pl.pallas_call(
        project_kernel,
        in_specs=[VMEM] * 6 + [SMEM, VMEM, VMEM, SMEM],
        out_shape=[
            jax.ShapeDtypeStruct((count, tokens + DH, DV), jnp.bfloat16),
            jax.ShapeDtypeStruct((tokens, 2 * DH), jnp.bfloat16),
            jax.ShapeDtypeStruct((tokens, 2 * DH), jnp.float32),
            jax.ShapeDtypeStruct((tokens, DV), jnp.bfloat16),
        ],
        compiler_params=pltpu.CompilerParams(vmem_limit_bytes=12 * MIB),
        name="project",
        interpret=INTERPRET,
    )(own, across, *weights, place, cosine, sine, log_decay.reshape(1))


def pass_on_kernel(spread_ref, att_ref, weight_ref, send_ref):
    tokens = att_ref.shape[0]
    total = jnp.zeros((DH, DV), jnp.float32)
    for i in range(spread_ref.shape[0]):
        total = total + spread_ref[i, tokens:].astype(jnp.float32) * weight_ref[i]
    for k in range(send_ref.shape[0]):
        send_ref[k, :tokens] = att_ref[...]
        send_ref[k, tokens:] = total.astype(jnp.bfloat16)


def pass_on(spread, att, weight, count):
    return pl.pallas_call(
        pass_on_kernel,
        in_specs=[VMEM, VMEM, SMEM],
        out_shape=jax.ShapeDtypeStruct((count, *spread.shape[1:]), jnp.bfloat16),
        compiler_params=pltpu.CompilerParams(vmem_limit_bytes=6 * MIB),
        name="pass_on",
        interpret=INTERPRET,
    )(spread, att, weight)


def attend_kernel(
    where_ref,
    q_ref,
    mine_ref,
    far_ref,
    out_ref,
    other_ref,
    k_ref,
    vt_ref,
    qt_ref,
    m_ref,
    l_ref,
    o_ref,
    sem,
):
    copy = pltpu.make_async_copy(far_ref, other_ref, sem)
    copy.start()
    z = where_ref[0]
    y = where_ref[1]
    keys = k_ref.shape[0]
    blocks = out_ref.shape[0]
    tokens = out_ref.shape[2] // 2

    first = where_ref[2] == 0

    def take_keys(ref):
        for i in range(ref.shape[0]):
            k_ref[i * tokens : (i + 1) * tokens] = ref[i, :tokens]

    def take_values(ref):
        for i in range(ref.shape[0]):
            vt_ref[:, i * tokens : (i + 1) * tokens] = ref[i, :tokens].T

    @pl.when(first)
    def _():
        take_keys(mine_ref)

    @pl.when(jnp.logical_not(first))
    def _():
        take_values(mine_ref)

    copy.wait()

    @pl.when(first)
    def _():
        take_values(other_ref)

    @pl.when(jnp.logical_not(first))
    def _():
        take_keys(other_ref)

    def visit(start, count, masked):
        s = jnp.dot(k_ref[pl.ds(start, count)], qt_ref[...], preferred_element_type=jnp.float32)
        if masked:
            rows = lax.broadcasted_iota(jnp.int32, s.shape, 0) + start
            cols = lax.broadcasted_iota(jnp.int32, s.shape, 1) % tokens + y * tokens
            allowed = (rows // SEG) <= (cols // SEG)
            s = jnp.where(allowed, s, NEG)
        old = m_ref[...]
        top = jnp.maximum(old, jnp.max(s, axis=0, keepdims=True))
        w = jnp.exp(s - top)
        factor = jnp.exp(old - top)
        m_ref[...] = top
        l_ref[...] = l_ref[...] * factor + jnp.sum(w, axis=0, keepdims=True)
        o_ref[...] = o_ref[...] * factor + jnp.dot(
            vt_ref[:, pl.ds(start, count)],
            w.astype(jnp.bfloat16),
            preferred_element_type=jnp.float32,
        )

    def empty(step, _):
        out_ref[step, :DV] = jnp.zeros((DV, 2 * tokens), jnp.bfloat16)
        row = lax.broadcasted_iota(jnp.int32, (ROWS - DV, 2 * tokens), 0)
        out_ref[step, DV:] = jnp.where(row == 0, NEG, 0.0).astype(jnp.bfloat16)
        return 0

    def begin(step):
        q = q_ref[step, :tokens]
        lane = lax.broadcasted_iota(jnp.int32, q.shape, 1)
        zero = jnp.zeros_like(q)
        q = jnp.concatenate([jnp.where(lane < DH, q, zero), jnp.where(lane < DH, zero, q)], axis=0)
        qt_ref[...] = q.T
        m_ref[...] = jnp.full(m_ref.shape, NEG, jnp.float32)
        l_ref[...] = jnp.zeros(l_ref.shape, jnp.float32)
        o_ref[...] = jnp.zeros(o_ref.shape, jnp.float32)

    def end(step):
        total = l_ref[...]
        out_ref[step, :DV] = (o_ref[...] / total).astype(jnp.bfloat16)
        weight = m_ref[...] + jnp.log(total)
        high = weight.astype(jnp.bfloat16)
        rest = weight - high.astype(jnp.float32)
        middle = rest.astype(jnp.bfloat16)
        low = (rest - middle.astype(jnp.float32)).astype(jnp.bfloat16)
        pad = jnp.zeros((ROWS - DV - 3, weight.shape[1]), jnp.bfloat16)
        out_ref[step, DV:] = jnp.concatenate([high, middle, low, pad], axis=0)

    def masked(i, _):
        visit(pl.multiple_of(i * KEYS, KEYS), KEYS, True)
        return 0

    def full(step, _):
        begin(step)
        for start in range(0, keys, KEYS):
            visit(start, KEYS, False)
        end(step)
        return 0

    lax.fori_loop(0, z, empty, 0)
    begin(z)
    lax.fori_loop(0, (y * tokens) // KEYS + 1, masked, 0)
    end(z)
    lax.fori_loop(z + 1, blocks, full, 0)


def attend(where, along, mine, other, tokens):
    blocks = along.shape[0]
    count = mine.shape[0] * tokens
    return pl.pallas_call(
        attend_kernel,
        in_specs=[SMEM, VMEM, VMEM, HBM],
        scratch_shapes=[
            pltpu.VMEM(other.shape, other.dtype),
            pltpu.VMEM((count, 2 * DH), jnp.bfloat16),
            pltpu.VMEM((DV, count), jnp.bfloat16),
            pltpu.VMEM((2 * DH, 2 * tokens), jnp.bfloat16),
            pltpu.VMEM((1, 2 * tokens), jnp.float32),
            pltpu.VMEM((1, 2 * tokens), jnp.float32),
            pltpu.VMEM((DV, 2 * tokens), jnp.float32),
            pltpu.SemaphoreType.DMA,
        ],
        out_shape=jax.ShapeDtypeStruct((blocks, ROWS, 2 * tokens), jnp.bfloat16),
        compiler_params=pltpu.CompilerParams(vmem_limit_bytes=16 * MIB),
        cost_estimate=pl.CostEstimate(
            flops=blocks * count * tokens * 4 * 256,
            bytes_accessed=blocks * tokens * 1024 + count * 512,
            transcendentals=blocks * count * tokens * 2,
        ),
        name="attend",
        interpret=INTERPRET,
    )(where, along, mine, pltpu.with_memory_space_constraint(other, pltpu.HBM))


def finish_kernel(
    parts_ref, mix_ref, gain_ref, spread_ref, along_ref, weight_ref, query_ref, within_ref, out_ref
):
    blocks = parts_ref.shape[0]
    tokens = query_ref.shape[0]
    logs = []
    for i in range(blocks):
        rows = parts_ref[i, DV:].astype(jnp.float32)
        logs.append(rows[0:1] + rows[1:2] + rows[2:3])
    top = functools.reduce(jnp.maximum, logs)
    shares = [jnp.exp(log - top) for log in logs]
    total = functools.reduce(jnp.add, shares)
    acc = jnp.zeros((DV, 2 * tokens), jnp.float32)
    for i in range(blocks):
        acc = acc + parts_ref[i, :DV].astype(jnp.float32) * (shares[i] / total)
    att = acc[:, :tokens] - mix_ref[0] * acc[:, tokens:]
    att = att * lax.rsqrt(jnp.mean(att * att, axis=0, keepdims=True) + EPSILON)
    att = (att.T * gain_ref[0:1]).astype(jnp.bfloat16)
    carried = jnp.zeros((DH, DV), jnp.float32)
    chips = spread_ref.shape[0]
    for i in range(chips):
        carried = carried + spread_ref[i, tokens:].astype(jnp.float32) * weight_ref[i]
    for i in range(blocks):
        carried = carried + along_ref[i, tokens:].astype(jnp.float32) * weight_ref[chips + i]
    ret = within_ref[...] + rounded(query_ref[...], carried, ((1,), (0,)))
    ret = ret * lax.rsqrt(jnp.mean(ret * ret, axis=1, keepdims=True) + EPSILON)
    ret = (ret * gain_ref[1:2]).astype(jnp.bfloat16)
    half = tokens // 2
    for i in range(2):
        out_ref[i, :, :DV] = att[i * half : (i + 1) * half]
        out_ref[i, :, DV:] = ret[i * half : (i + 1) * half]


def finish(parts, mixing, gains, spread, along, weights, query, within):
    tokens = query.shape[0]
    return pl.pallas_call(
        finish_kernel,
        in_specs=[VMEM, SMEM, VMEM, VMEM, VMEM, SMEM, VMEM, VMEM],
        out_shape=jax.ShapeDtypeStruct((2, tokens // 2, 2 * DV), jnp.bfloat16),
        compiler_params=pltpu.CompilerParams(vmem_limit_bytes=8 * MIB),
        name="finish",
        interpret=INTERPRET,
    )(parts, mixing.reshape(1), gains, spread, along, weights, query, within)


def decay_log(head, length):
    pair = (head // 2).astype(jnp.float32)
    quick = jnp.log1p(-jnp.exp2(-5.0 - pair / 4.0))
    slow = jnp.log1p(-1.0 / (length * (1.0 + pair)))
    return jnp.where(head % 2 == 0, quick, slow)


def layer(
    features,
    norm_gain,
    att_query,
    att_key,
    att_value,
    att_lambda,
    att_gain,
    ret_query,
    ret_key,
    ret_value,
    ret_gain,
    out_weight,
):
    z = lax.axis_index(Z)
    y = lax.axis_index("y")
    c = lax.axis_index("c")
    x = lax.axis_index("tp")
    ny = lax.axis_size("y")
    nz = lax.axis_size(Z)
    nl = lax.axis_size("zl")
    groups = lax.axis_size("tp")
    chip = z * ny + y
    tokens = 2 * features.shape[0]

    matrices = (att_query, att_key, att_value, ret_query, ret_key, ret_value)
    sent, features = pack(2 * ny, groups, *matrices, features)
    rows, width = sent.shape[2:]
    sent = sent.reshape(4 * ny, rows, width)
    even = jnp.arange(0, DH, 2).astype(jnp.float32)
    small = (even, jnp.arange(ny), jnp.arange(nz), chip, z, y, c, x)
    sent, small = lax.optimization_barrier((sent, small))
    w_own = lax.all_to_all(sent, ("zh", "y", "c"), 0, 0, tiled=True)
    w_own = w_own.reshape(4 * ny * rows, width)
    inputs = (features, norm_gain, att_lambda, att_gain, ret_gain)
    w_own, inputs, small = lax.optimization_barrier((w_own, inputs, small))
    features, norm_gain, att_lambda, att_gain, ret_gain = inputs
    even, ys, zs, chip, z, y, c, x = small
    weights = (w_own, *around(w_own))
    blocks = [high * nl + (z + k) % nl for k in (0, nl - 1, 1, 2) for high in range(2)]

    gathered = lax.all_to_all(features, "tp", 0, 0, tiled=True)
    normed = norm(gathered, norm_gain, nz)
    across = swapped(normed)

    log_decay = decay_log(x * 2 + c, float(nz * ny * tokens))
    positions = (chip * tokens + jnp.arange(tokens)).astype(jnp.float32)
    inverse = 10000.0 ** (-even / DH)
    angles = positions[:, None] * inverse[None, :]
    cosine, sine = jnp.cos(angles), jnp.sin(angles)
    span = log_decay * tokens
    to_end = jnp.exp(span * (ny - 1 - ys).astype(jnp.float32))
    place = jnp.stack([c, *blocks]).astype(jnp.int32)
    tables = (cosine, sine, log_decay, to_end, place)
    normed, across, weights, tables = lax.optimization_barrier((normed, across, weights, tables))
    cosine, sine, log_decay, to_end, place = tables

    send, att, turned, value = project(
        normed, across, weights, place, cosine, sine, log_decay, ny
    )
    spread = lax.all_to_all(send, "y", 0, 0, tiled=True)
    small = (ys, zs, span, z, y, c, att_lambda, att_gain, ret_gain, turned, value, log_decay)
    spread, small = lax.optimization_barrier((spread, small))
    ys, zs, span, z, y, c, att_lambda, att_gain, ret_gain, turned, value, log_decay = small
    query, within = local(turned, value, log_decay)
    y_steps = jnp.maximum(y - 1 - ys, 0).astype(jnp.float32)
    z_steps = jnp.maximum(ny * (z - 1 - zs) + y, 0).astype(jnp.float32)
    before = jnp.concatenate(
        [
            jnp.where(ys < y, jnp.exp(span * y_steps), 0.0),
            jnp.where(zs < z, jnp.exp(span * z_steps), 0.0),
        ]
    )
    where = jnp.stack([z, y, c]).astype(jnp.int32)
    mixing = lax.dynamic_index_in_dim(att_lambda, c, 0, keepdims=False)
    gains = jnp.stack([att_gain, ret_gain])
    send = pass_on(spread, att, to_end, nz)
    along = lax.all_to_all(send, Z, 0, 0, tiled=True)
    other = swapped(spread)
    tables = (before, where, mixing, gains, query, within)
    along, tables = lax.optimization_barrier((along, tables))
    before, where, mixing, gains, query, within = tables
    parts = attend(where, along, spread, other, tokens)
    parts = lax.all_to_all(parts, Z, 0, 0, tiled=True)

    heads = finish(parts, mixing, gains, spread, along, before, query, within)
    heads = lax.all_to_all(heads, "c", 0, 0, tiled=True)
    joined = jnp.concatenate(
        [heads[0, :, :DV], heads[1, :, :DV], heads[0, :, DV:], heads[1, :, DV:]], axis=1
    )
    partial = jnp.dot(
        joined, out_weight.reshape(-1, out_weight.shape[2]), preferred_element_type=jnp.float32
    ).astype(jnp.bfloat16)
    partial = lax.all_to_all(
        partial.reshape(groups, -1, partial.shape[1]), "tp", 0, 0, tiled=True
    )
    return jnp.sum(partial.astype(jnp.float32), axis=0)


def solution(mesh):
    devices = mesh.devices
    torus = Mesh(devices.reshape(2, 4, -1, 2, devices.shape[-1]), SP_TP)
    return jax.shard_map(
        layer,
        mesh=torus,
        in_specs=(
            P(SP, "tp"),
            P(),
            P(SP, "tp"),
            P(SP, "tp"),
            P(SP, "tp"),
            P("tp"),
            P(),
            P(SP, "tp"),
            P(SP, "tp"),
            P(SP, "tp"),
            P(),
            P(None, "tp", None),
        ),
        out_specs=P(SP_TP, None),
        check_vma=False,
    )
```
